256 devices in a mesh: sp: 32 (over z, x), tp: 8 (over y, core).
Axes of the slice: x: 4, y: 4, z: 8, core: 2. Of those that a mesh axis runs over, the one named last changes fastest.
Arguments:
- inputs: bfloat16 [32768, 2048], P('sp', 'tp'), may hold values from -6 to 6
- w_query: bfloat16 [2048, 2048], P(None, 'tp'), may hold values from -0.125 to 0.125
- w_value: bfloat16 [2048, 2048], P(None, 'tp'), may hold values from -0.125 to 0.125
- w_forget: bfloat16 [2, 2048, 2048], P(None, None, 'tp'), may hold values from -0.125 to 0.125
- w_gate: bfloat16 [2048, 2048], P(None, 'tp'), may hold values from -0.125 to 0.125
- gate_room: float32 [2, 2048], P(None, 'tp'), as said below
- extra_decay: float32 [16, 32768], P('tp', 'sp'), may hold values from -2 to 0
- out_gain: float32 [2048], P('tp'), may hold values from 0.1 to 1.9
- new_inputs: bfloat16 [128, 2048], replicated, may hold values from -6 to 6
Outputs:
- mixed_rows: bfloat16 [32768, 2048], P('sp', 'tp')
- prompt_state_cache: bfloat16 [16, 128, 128], P('tp')
- new_read: bfloat16 [128, 2048], P(None, 'tp')
The draws below stay inside these ranges and needn't reach their ends.
Inputs may be any that keep to these rules, and one draw needn't show every extreme that they name: `gate_room`: each entry lies between 0.5 / 32768 and 0.1.
All inputs are finite; a program needn't handle non-finite values.
Results may differ from the reference program's by a relative error of at most 0.012.
The reference program's roundings to bfloat16 on the way count: a program that leaves them out, or rounds other values in their place, can miss the bound.
Values may be sent and summed in bfloat16 or wider, within the bound.
A program may use at most 128 MiB of HBM per device.

```python
import jax
import jax.numpy as jnp
from jax import lax

D = 2048
HEADS = 16
HD = 128
BLOCK = 128
TOK_DEV = 1024
NEW = 128
LEN = 32768


def draw_inputs(key, part):
    noise_key, offset_key = jax.random.split(key)
    noise_part = jax.random.normal(noise_key, (LEN, D), jnp.float32)
    offset = 0.7 * jax.random.normal(offset_key, (D,), jnp.float32)
    return jnp.clip(noise_part + offset[None, :], -6.0, 6.0).astype(jnp.bfloat16)


def draw_gate_room(key, part):
    pick_key, slow_key, fast_key = jax.random.split(key, 3)
    slow_share = 0.5
    slow_head = jax.random.uniform(pick_key, (2, HEADS, 1), jnp.float32) < slow_share
    slow_value = jnp.exp(jax.random.uniform(slow_key, (2, HEADS, HD), jnp.float32, jnp.log(0.5), jnp.log(2.0))) / LEN
    fast_value = jnp.exp(jax.random.uniform(fast_key, (2, HEADS, HD), jnp.float32, jnp.log(0.03), jnp.log(0.1)))
    return jnp.where(slow_head, slow_value, fast_value).reshape(2, HEADS * HD)


def draw_extra_decay(key, part):
    scale_key, place_key, loss_key = jax.random.split(key, 3)
    low_end = 0.5
    high_end = 2.0
    factor = jnp.exp(jax.random.uniform(scale_key, (HEADS, LEN // TOK_DEV, 1), jnp.float32, jnp.log(low_end), jnp.log(high_end)))
    stable_result = -0.5 / LEN * jnp.broadcast_to(factor, (HEADS, LEN // TOK_DEV, TOK_DEV)).reshape(HEADS, LEN)
    places = jax.random.randint(place_key, (HEADS, 3, 1), 0, LEN)
    loss_values = jnp.log(jax.random.uniform(loss_key, (HEADS, 3, 1), jnp.float32, 0.6, 0.8))
    at_position = jnp.arange(LEN)[None, None, :] == places
    token_groups = jnp.sum(jnp.where(at_position, loss_values, 0.0), axis=1)
    return stable_result + token_groups


def block_scale(rng, shape, pieces, low, high):
    def one(dim, blocks):
        draws = jax.random.uniform(jax.random.fold_in(jax.random.fold_in(rng, 6), dim), (blocks,), jnp.float32, low / len(pieces), high / len(pieces))
        return jnp.repeat(jnp.exp(draws), shape[dim] // blocks).reshape((-1,) + (1,) * (len(shape) - dim - 1))

    loudness = one(*pieces[0])
    for cut in pieces[1:]:
        loudness = loudness * one(*cut)
    return loudness


def noise(stream_key, shape, spread, reach, cuts=(), held_as=jnp.bfloat16):
    entries = jax.random.normal(stream_key, shape, jnp.float32) * spread
    if len(cuts) > 0:
        entries = block_scale(stream_key, shape, cuts, -0.22, 0.18) * entries
    return jnp.clip(entries, min=-reach, max=reach).astype(held_as)


def setup_inputs(seed: int = 0) -> dict:
    key_list = jax.random.split(jax.random.key(seed), 10)
    inputs = draw_inputs(jax.random.fold_in(key_list[9], 71), 0)
    w_query = noise(key_list[1], (D, HEADS * HD), D ** -0.5, 0.125, ((1, 8),))
    w_value = noise(key_list[2], (D, HEADS * HD), D ** -0.5, 0.125, ((1, 8),))
    w_forget = noise(key_list[3], (2, D, HEADS * HD), D ** -0.5, 0.125, ((2, 8),))
    w_gate = noise(key_list[4], (D, HEADS * HD), D ** -0.5, 0.125, ((1, 8),))
    gate_room = draw_gate_room(jax.random.fold_in(key_list[9], 71), 0)
    extra_decay = draw_extra_decay(jax.random.fold_in(key_list[9], 71), 0)
    out_gain = jnp.clip(1.0 + 0.18 * jax.random.normal(key_list[7], (HEADS * HD,), jnp.float32), 0.1, 1.9)
    new_inputs = noise(key_list[8], (NEW, D), 1.0, 6.0)
    return {"inputs": inputs, "w_query": w_query, "w_value": w_value, "w_forget": w_forget, "w_gate": w_gate, "gate_room": gate_room, "extra_decay": extra_decay, "out_gain": out_gain, "new_inputs": new_inputs}


NORM_EPS = 1e-06
TOP_PRECISION = lax.Precision.HIGHEST

def rounded(matrix):
    return lax.optimization_barrier(matrix.astype(jnp.bfloat16)).astype(jnp.float32)

def gate_keys(gate_pre, room_row):
    return room_row * jax.nn.sigmoid(-gate_pre)

def finish(mixture, gain_rows, gate_pre):
    inverse_rms = lax.rsqrt(lax.optimization_barrier(jnp.mean(mixture * mixture, axis=-1, keepdims=True)) + NORM_EPS)
    return (mixture * inverse_rms * gain_rows * jax.nn.silu(gate_pre)).astype(jnp.bfloat16)

def block_states(query_rows, keys_in, values, log_decay, span_len):
    length, head_count, key_width = query_rows.shape
    value_width = values.shape[-1]
    blocks = length // span_len
    q_blocks = query_rows.reshape(blocks, span_len, head_count, key_width)
    k_blocks = keys_in.reshape(blocks, span_len, head_count, key_width)
    v_blocks = values.reshape(blocks, span_len, head_count, value_width)
    within = jnp.cumsum(log_decay.reshape(blocks, span_len, head_count, key_width), axis=1)
    middle = within[:, span_len // 2:span_len // 2 + 1]
    ending = within[:, span_len - 1:span_len]
    q_carried = q_blocks * jnp.exp(within)
    q_inside = q_blocks * jnp.exp(within - middle)
    k_inside = k_blocks * jnp.exp(middle - within)
    k_ending = k_blocks * jnp.exp(ending - within)
    scores = jnp.einsum('nthk,nshk->nhts', q_inside, k_inside, precision=TOP_PRECISION)
    earlier_mask = jnp.arange(span_len)[:, None] >= jnp.arange(span_len)[None, :]
    scores = jnp.where(earlier_mask, scores, 0.0)
    inside = jnp.einsum('nhts,nshv->nthv', scores, v_blocks, precision=TOP_PRECISION)
    additions = jnp.einsum('nshk,nshv->nhkv', k_ending, v_blocks, precision=TOP_PRECISION)
    block_decay = ending[:, 0]

    def advance(current, block_item):
        added_term, decay_sum = block_item
        return (jnp.exp(decay_sum)[:, :, None] * current + added_term, current)
    initial = jnp.zeros((head_count, key_width, value_width), jnp.float32)
    last_state, before = lax.scan(advance, initial, (additions, block_decay))
    carried = jnp.einsum('nthk,nhkv->nthv', q_carried, before, precision=TOP_PRECISION)
    offsets = jnp.cumsum(block_decay, axis=0) - block_decay
    cumulative = (within + offsets[:, None]).reshape(length, head_count, key_width)
    return ((inside + carried).reshape(length, head_count, value_width), last_state, cumulative)

def reference(inputs, w_query, w_value, w_forget, w_gate, gate_room, extra_decay, out_gain, new_inputs):
    head_count = extra_decay.shape[0]
    tokens = inputs.shape[0]
    channels = w_query.shape[1]
    key_width = channels // head_count
    split_heads = (tokens, head_count, key_width)

    def project(matrix_in, weight):
        return jnp.dot(matrix_in, weight, preferred_element_type=jnp.float32)
    query_rows = rounded(project(inputs, w_query)).reshape(split_heads)
    values = rounded(project(inputs, w_value)).reshape(split_heads)
    room_forward = gate_room[0].reshape(head_count, key_width)
    room_backward = gate_room[1].reshape(head_count, key_width)
    gain_rows = out_gain.reshape(head_count, key_width)
    extra_log = extra_decay.T[:, :, None]
    forward_key = gate_keys(project(inputs, w_forget[0]).reshape(split_heads), room_forward)
    backward_key = gate_keys(project(inputs, w_forget[1]).reshape(split_heads), room_backward)
    forward_log = jnp.log1p(-forward_key) + extra_log
    backward_log = jnp.log1p(-backward_key) + extra_log
    forward_out, last_state, unused_sum = block_states(query_rows, forward_key, values, forward_log, BLOCK)
    backward_rev, unused_state, unused_cum = block_states(query_rows[::-1], backward_key[::-1], values[::-1], backward_log[::-1], BLOCK)
    gate_pre = project(inputs, w_gate).reshape(split_heads)
    mixed_rows = finish(forward_out + backward_rev[::-1], gain_rows, gate_pre).reshape(tokens, channels)
    prompt_state_cache = last_state.astype(jnp.bfloat16)
    new_count = new_inputs.shape[0]
    new_heads = (new_count, head_count, key_width)
    fresh_query = rounded(project(new_inputs, w_query)).reshape(new_heads)
    new_value = rounded(project(new_inputs, w_value)).reshape(new_heads)
    fresh_forward = gate_keys(project(new_inputs, w_forget[0]).reshape(new_heads), room_forward)
    new_backward = gate_keys(project(new_inputs, w_forget[1]).reshape(new_heads), room_backward)
    new_gate = project(new_inputs, w_gate).reshape(new_heads)
    cache_entries = jnp.einsum('awe,wel->awl', fresh_query * (1.0 - fresh_forward), prompt_state_cache.astype(jnp.float32), precision=TOP_PRECISION)
    own_term = lax.optimization_barrier(jnp.sum(fresh_query * (fresh_forward + new_backward), axis=-1, keepdims=True)) * new_value
    new_read = finish(cache_entries + own_term, gain_rows, new_gate).reshape(new_count, channels)
    return (mixed_rows, prompt_state_cache, new_read)
```

```python
import jax
import jax.numpy as jnp
from jax import lax
from jax.experimental import pallas as pl
from jax.experimental.pallas import tpu as pltpu
from jax.sharding import PartitionSpec as P

MESH = pl.DeviceIdType.MESH
EPS = 1e-06
B = 128
HD = 128
F32 = jnp.float32
BF16 = jnp.bfloat16


def nn(a, b):
    return lax.dot_general(a, b, (((1,), (0,)), ((), ())), preferred_element_type=F32)


def nt(a, b):
    return lax.dot_general(a, b, (((1,), (1,)), ((), ())), preferred_element_type=F32)


def tn(a, b):
    return lax.dot_general(a, b, (((0,), (0,)), ((), ())), preferred_element_type=F32)


def split2(a):
    hi = a.astype(BF16)
    return hi, (a - hi.astype(F32)).astype(BF16)


def log_one_minus(k):
    s = jnp.full_like(k, 1.0 / 8.0)
    for n in (7, 6, 5, 4, 3, 2):
        s = s * k + (1.0 / n)
    return -(s * k + 1.0) * k


def body(n_sp, n_tp, n_chunk, heads, x_hbm, wq, wv, wf, wg, nx_hbm, room, extra, gain,
         mixed_out, cache_out, read_out,
         x, w, nx, qs, vs, cf, cb, kf_s, kb_s, gs, a_f, a_b, e_f, e_b, s_f, s_b, acc,
         inside, qc_hi, qc_lo, st_hi, st_lo, stage, got, stage2, got2, fin, nq_hi, nq_lo, nv, nown, ngate,
         load_sem, own_sem, ag_send, ag_recv, d2_send, d2_recv, p1_send, p1_recv, p2_send, p2_recv,
         p3_send, p3_recv):
    cols = heads * HD
    sp = lax.axis_index("sp")
    tp = lax.axis_index("tp")
    right = lax.rem(tp + 2, n_tp)
    left = lax.rem(tp + n_tp - 2, n_tp)
    far = lax.rem(tp + 4, n_tp)
    flip = 1 - 2 * lax.rem(tp, 2)
    mate = tp + flip

    barrier = pltpu.get_barrier_semaphore()
    for peer in (mate, left, right):
        pl.semaphore_signal(barrier, inc=1, device_id={"tp": peer}, device_id_type=MESH)

    def greet(i, c):
        pl.semaphore_signal(barrier, inc=1, device_id={"sp": lax.rem(sp + i, n_sp)}, device_id_type=MESH)
        return c

    lax.fori_loop(1, n_sp, greet, 0)

    def block(owner):
        return pl.ds(pl.multiple_of(owner * cols, cols), cols)

    def rows(j):
        return pl.ds(pl.multiple_of(j * B, B), B)

    loads = [pltpu.make_async_copy(x_hbm, x.at[:, block(tp)], load_sem.at[0]),
             pltpu.make_async_copy(nx_hbm, nx, load_sem.at[1]),
             pltpu.make_async_copy(wq, w.at[0], load_sem.at[2]),
             pltpu.make_async_copy(wv, w.at[1], load_sem.at[3]),
             pltpu.make_async_copy(wf.at[0], w.at[2], load_sem.at[4]),
             pltpu.make_async_copy(wf.at[1], w.at[3], load_sem.at[5]),
             pltpu.make_async_copy(wg, w.at[4], load_sem.at[6])]
    for load in loads:
        load.start()

    room_f = room[0:1, :]
    room_b = room[1:2, :]
    gain_row = gain[...]
    t_id = lax.broadcasted_iota(jnp.int32, (B, B), 0)
    s_id = lax.broadcasted_iota(jnp.int32, (B, B), 1)
    lower = t_id >= s_id
    upper = s_id >= t_id

    def silu_gain(g):
        return gain_row * (g / (1.0 + jnp.exp(-g)))

    def ring(kind, j):
        if kind == 0:
            src, to, r = block(tp), right, rows(j)
        elif kind == 1:
            src, to, r = block(tp), left, rows(j)
        elif kind == 2:
            src, to, r = block(left), right, pl.ds(pl.multiple_of(j * B, B), B // 2)
        else:
            src, to, r = block(right), left, pl.ds(pl.multiple_of(j * B + B // 2, B // 2), B // 2)
        return pltpu.make_async_remote_copy(
            src_ref=x.at[r, src], dst_ref=x.at[r, src], send_sem=ag_send.at[kind, j],
            recv_sem=ag_recv.at[kind, j], device_id={"tp": to}, device_id_type=MESH)

    def ring_in(kind, j):
        if kind == 0:
            src, r = block(left), rows(j)
        elif kind == 1:
            src, r = block(right), rows(j)
        elif kind == 2:
            src, r = block(far), pl.ds(pl.multiple_of(j * B, B), B // 2)
        else:
            src, r = block(far), pl.ds(pl.multiple_of(j * B + B // 2, B // 2), B // 2)
        return pltpu.make_async_remote_copy(
            src_ref=x.at[r, src], dst_ref=x.at[r, src], send_sem=ag_send.at[kind, j],
            recv_sem=ag_recv.at[kind, j], device_id={"tp": left}, device_id_type=MESH)

    def pair(kind, j, owner):
        return pltpu.make_async_remote_copy(
            src_ref=x.at[rows(j), block(owner)], dst_ref=x.at[rows(j), block(owner)],
            send_sem=d2_send.at[kind, j], recv_sem=d2_recv.at[kind, j],
            device_id={"tp": mate}, device_id_type=MESH)

    def pair_own(owner):
        return pltpu.make_async_remote_copy(
            src_ref=x.at[:, block(owner)], dst_ref=x.at[:, block(owner)],
            send_sem=own_sem.at[0], recv_sem=own_sem.at[1],
            device_id={"tp": mate}, device_id_type=MESH)

    for load in loads[1:]:
        load.wait()
    new = nx[...]
    nq_v = nn(new, w[0]).astype(BF16)
    nv[...] = nn(new, w[1]).astype(BF16)
    nf = room_f / (1.0 + jnp.exp(nn(new, w[2])))
    nb = room_b / (1.0 + jnp.exp(nn(new, w[3])))
    ngate[...] = silu_gain(nn(new, w[4]))
    nqf = nq_v.astype(F32)
    nq_hi[...], nq_lo[...] = split2(nqf * (1.0 - nf))
    nown[...] = nqf * (nf + nb)

    loads[0].wait()
    pl.semaphore_wait(barrier, n_sp + 2)

    pair_own(tp).start()
    for j in range(2):
        ring(0, j).start()
        ring(1, j).start()

    s_f[...] = jnp.zeros_like(s_f)
    s_b[...] = jnp.zeros_like(s_b)
    acc[...] = jnp.zeros_like(acc)

    def compute(c):
        r = rows(c)
        xc = x[r, :]
        fp = nn(xc, w[2])
        bp = nn(xc, w[3])
        kf = room_f / (1.0 + jnp.exp(fp))
        kb = room_b / (1.0 + jnp.exp(bp))
        kf_s[r, :] = kf
        kb_s[r, :] = kb
        vc = nn(xc, w[1]).astype(BF16)
        vs[r, :] = vc
        qs[r, :] = nn(xc, w[0]).astype(BF16)
        gs[r, :] = silu_gain(nn(xc, w[4]))
        tri_l = jnp.where(lower, 1.0, 0.0).astype(BF16)
        tri_u = jnp.where(upper, 1.0, 0.0).astype(BF16)
        lf_hi, lf_lo = split2(log_one_minus(kf))
        lb_hi, lb_lo = split2(log_one_minus(kb))
        wfc = nn(tri_l, lf_hi) + nn(tri_l, lf_lo)
        wbc = nn(tri_u, lb_hi) + nn(tri_u, lb_lo)
        ones = jnp.ones((B, HD), BF16)
        for h in range(heads):
            hs = slice(h * HD, (h + 1) * HD)
            ex = extra[h:h + 1, r]
            el_hi, el_lo = split2(jnp.where(lower, ex, 0.0))
            eu_hi, eu_lo = split2(jnp.where(upper, ex, 0.0))
            wfh = wfc[:, hs] + nn(el_hi, ones) + nn(el_lo, ones)
            wbh = wbc[:, hs] + nn(eu_hi, ones) + nn(eu_lo, ones)
            cf[r, hs] = wfh
            cb[r, hs] = wbh
            end_f = wfh[B - 1:B, :]
            end_b = wbh[0:1, :]
            ke_f = (kf[:, hs] * jnp.exp(end_f - wfh)).astype(BF16)
            ke_b = (kb[:, hs] * jnp.exp(end_b - wbh)).astype(BF16)
            af = tn(vc[:, hs], ke_f)
            ab = tn(vc[:, hs], ke_b)
            a_f[c, h] = af
            a_b[c, h] = ab
            e_f[c, h] = jnp.broadcast_to(jnp.exp(end_f), (8, HD))
            e_b[c, h] = jnp.broadcast_to(jnp.exp(end_b), (8, HD))
            s_f[h] = s_f[h] * jnp.exp(end_f) + af
            s_b[h] = s_b[h] + jnp.exp(acc[1, h, 0:1, :]) * ab
            acc[0, h] = acc[0, h] + end_f
            acc[1, h] = acc[1, h] + end_b

    def step(j, carry):
        @pl.when(j < n_chunk)
        def _():
            ring_in(0, j).wait_recv()
            ring_in(1, j).wait_recv()
            ring(2, j).start()
            ring(3, j).start()
            pair(0, j, left).start()
            pair(1, j, right).start()

        @pl.when(j + 2 < n_chunk)
        def _():
            ring(0, j + 2).start()
            ring(1, j + 2).start()

        @pl.when((j >= 1) & (j <= n_chunk))
        def _():
            ring_in(2, j - 1).wait_recv()
            ring_in(3, j - 1).wait_recv()
            pair(2, j - 1, far).start()

        @pl.when(j == 2)
        def _():
            pair_own(mate).wait_recv()

        @pl.when(j >= 2)
        def _():
            c = j - 2
            pair(0, c, left + flip).wait_recv()
            pair(1, c, right + flip).wait_recv()
            pair(2, c, far + flip).wait_recv()
            compute(c)

        return carry

    lax.fori_loop(0, n_chunk + 2, step, 0)

    per = n_sp // heads
    r_id = lax.broadcasted_iota(jnp.int32, (8, HD), 0)
    for h in range(heads):
        at = slice(h * per, (h + 1) * per)
        stage[at, 0] = s_f[h].reshape(per, 8, HD)
        stage[at, 1] = s_b[h].reshape(per, 8, HD)
        both = jnp.where(r_id == 0, acc[0, h], acc[1, h])
        stage[at, 2] = jnp.broadcast_to(both[None], (per, 8, HD))
    got[sp] = stage[sp]

    def send1(i, to, frm):
        return pltpu.make_async_remote_copy(
            src_ref=stage.at[to], dst_ref=got.at[frm], send_sem=p1_send.at[i], recv_sem=p1_recv.at[frm],
            device_id={"sp": to}, device_id_type=MESH)

    def send2(i, to, frm):
        return pltpu.make_async_remote_copy(
            src_ref=stage2.at[to], dst_ref=got2.at[frm], send_sem=p2_send.at[i], recv_sem=p2_recv.at[frm],
            device_id={"sp": to}, device_id_type=MESH)

    def send3(i, to, frm):
        return pltpu.make_async_remote_copy(
            src_ref=fin.at[sp], dst_ref=fin.at[frm], send_sem=p3_send.at[i], recv_sem=p3_recv.at[frm],
            device_id={"sp": to}, device_id_type=MESH)

    def spread(send):
        def one(i, c):
            send(i, lax.rem(sp + i, n_sp), sp).start()
            return c
        lax.fori_loop(1, n_sp, one, 0)

    def collect(send):
        def one(i, c):
            frm = lax.rem(sp + n_sp - i, n_sp)
            send(i, frm, frm).wait_recv()
            return c
        lax.fori_loop(1, n_sp, one, 0)

    def drain(send):
        def one(i, c):
            send(i, lax.rem(sp + i, n_sp), sp).wait_send()
            return c
        lax.fori_loop(1, n_sp, one, 0)

    spread(send1)

    def scores(c, carry):
        r = rows(c)
        for h in range(heads):
            hs = slice(h * HD, (h + 1) * HD)
            wfh = cf[r, hs]
            wbh = cb[r, hs]
            mid_f = wfh[B // 2:B // 2 + 1, :]
            mid_b = wbh[B // 2 - 1:B // 2, :]
            q = qs[r, hs].astype(F32)
            qi_f = (q * jnp.exp(wfh - mid_f)).astype(BF16)
            qi_b = (q * jnp.exp(wbh - mid_b)).astype(BF16)
            ki_f = (kf_s[r, hs] * jnp.exp(mid_f - wfh)).astype(BF16)
            ki_b = (kb_s[r, hs] * jnp.exp(mid_b - wbh)).astype(BF16)
            sc = jnp.where(lower, nt(qi_f, ki_f), 0.0) + jnp.where(upper, nt(qi_b, ki_b), 0.0)
            inside[r, hs] = nn(sc.astype(BF16), vs[r, hs])
            qc_hi[h, r, 0:HD], qc_lo[h, r, 0:HD] = split2(q * jnp.exp(wfh))
            qc_hi[h, r, HD:2 * HD], qc_lo[h, r, HD:2 * HD] = split2(q * jnp.exp(wbh))
        return carry

    half = n_chunk // 2
    lax.fori_loop(0, half, scores, 0)
    collect(send1)

    def decay(q, at):
        return jnp.exp(got[q, 2, at:at + 1, :])

    run = jnp.zeros((8, HD), F32)
    before = []
    for q in range(n_sp):
        before.append(run)
        run = run * decay(q, 0) + got[q, 0]
    fin[sp] = run
    run = jnp.zeros((8, HD), F32)
    for q in reversed(range(n_sp)):
        stage2[q, 0] = before[q]
        stage2[q, 1] = run
        run = run * decay(q, 1) + got[q, 1]
    got2[sp] = stage2[sp]
    spread(send2)
    spread(send3)

    lax.fori_loop(half, n_chunk, scores, 0)
    collect(send2)

    for h in range(heads):
        run = got2[h * per:(h + 1) * per, 0].reshape(HD, HD)
        for c in range(n_chunk):
            st_hi[h, c, :, 0:HD], st_lo[h, c, :, 0:HD] = split2(run)
            run = run * e_f[c, h, 0:1, :] + a_f[c, h]
        run = got2[h * per:(h + 1) * per, 1].reshape(HD, HD)
        for c in reversed(range(n_chunk)):
            st_hi[h, c, :, HD:2 * HD], st_lo[h, c, :, HD:2 * HD] = split2(run)
            run = run * e_b[c, h, 0:1, :] + a_b[c, h]

    def norm(mix, scale):
        return (mix * lax.rsqrt(jnp.mean(mix * mix, axis=-1, keepdims=True) + EPS) * scale).astype(BF16)

    def finish(c, carry):
        r = rows(c)
        for h in range(heads):
            hs = slice(h * HD, (h + 1) * HD)
            mix = (inside[r, hs] + nt(qc_lo[h, r, :], st_hi[h, c]) + nt(qc_hi[h, r, :], st_lo[h, c])
                   + nt(qc_hi[h, r, :], st_hi[h, c]))
            mixed_out[r, hs] = norm(mix, gs[r, hs])
        return carry

    lax.fori_loop(0, n_chunk, finish, 0)

    collect(send3)
    for h in range(heads):
        hs = slice(h * HD, (h + 1) * HD)
        last = fin[h * per:(h + 1) * per].reshape(HD, HD)
        cached = last.astype(BF16)
        cache_out[h] = last.T.astype(BF16)
        own = jnp.sum(nown[:, hs], axis=-1, keepdims=True) * nv[:, hs].astype(F32)
        read_out[:, hs] = norm(nt(nq_lo[:, hs], cached) + nt(nq_hi[:, hs], cached) + own, ngate[:, hs])

    def settle(j, c):
        for kind in range(4):
            ring(kind, j).wait_send()
        pair(0, j, left).wait_send()
        pair(1, j, right).wait_send()
        pair(2, j, far).wait_send()
        return c

    lax.fori_loop(0, n_chunk, settle, 0)
    pair_own(tp).wait_send()
    drain(send1)
    drain(send2)
    drain(send3)


def solution(mesh):
    n_sp, n_tp = mesh.shape["sp"], mesh.shape["tp"]

    def per_device(inputs, w_query, w_value, w_forget, w_gate, gate_room, extra_decay, out_gain, new_inputs):
        tokens, cols = inputs.shape
        depth = w_query.shape[0]
        heads = extra_decay.shape[0]
        fresh = new_inputs.shape[0]
        chunks = tokens // B
        anyspace = pl.BlockSpec(memory_space=pl.ANY)
        vmem = pl.BlockSpec(memory_space=pltpu.VMEM)

        def kernel(*refs):
            body(n_sp, n_tp, chunks, heads, *refs)

        dma = pltpu.SemaphoreType.DMA
        return pl.pallas_call(
            kernel,
            out_shape=(jax.ShapeDtypeStruct((tokens, cols), BF16),
                       jax.ShapeDtypeStruct((heads, HD, HD), BF16),
                       jax.ShapeDtypeStruct((fresh, cols), BF16)),
            in_specs=[anyspace] * 6 + [vmem] * 3,
            out_specs=(vmem, vmem, vmem),
            scratch_shapes=[
                pltpu.VMEM((tokens, depth), BF16),
                pltpu.VMEM((5, depth, cols), BF16),
                pltpu.VMEM((fresh, depth), BF16),
                pltpu.VMEM((tokens, cols), BF16),
                pltpu.VMEM((tokens, cols), BF16),
                pltpu.VMEM((tokens, cols), F32),
                pltpu.VMEM((tokens, cols), F32),
                pltpu.VMEM((tokens, cols), F32),
                pltpu.VMEM((tokens, cols), F32),
                pltpu.VMEM((tokens, cols), F32),
                pltpu.VMEM((chunks, heads, HD, HD), F32),
                pltpu.VMEM((chunks, heads, HD, HD), F32),
                pltpu.VMEM((chunks, heads, 8, HD), F32),
                pltpu.VMEM((chunks, heads, 8, HD), F32),
                pltpu.VMEM((heads, HD, HD), F32),
                pltpu.VMEM((heads, HD, HD), F32),
                pltpu.VMEM((2, heads, 8, HD), F32),
                pltpu.VMEM((tokens, cols), F32),
                pltpu.VMEM((heads, tokens, 2 * HD), BF16),
                pltpu.VMEM((heads, tokens, 2 * HD), BF16),
                pltpu.VMEM((heads, chunks, HD, 2 * HD), BF16),
                pltpu.VMEM((heads, chunks, HD, 2 * HD), BF16),
                pltpu.VMEM((n_sp, 3, 8, HD), F32),
                pltpu.VMEM((n_sp, 3, 8, HD), F32),
                pltpu.VMEM((n_sp, 2, 8, HD), F32),
                pltpu.VMEM((n_sp, 2, 8, HD), F32),
                pltpu.VMEM((n_sp, 8, HD), F32),
                pltpu.VMEM((fresh, cols), BF16),
                pltpu.VMEM((fresh, cols), BF16),
                pltpu.VMEM((fresh, cols), BF16),
                pltpu.VMEM((fresh, cols), F32),
                pltpu.VMEM((fresh, cols), F32),
                dma((7,)), dma((2,)),
                dma((4, chunks)), dma((4, chunks)),
                dma((3, chunks)), dma((3, chunks)),
                dma((n_sp,)), dma((n_sp,)),
                dma((n_sp,)), dma((n_sp,)),
                dma((n_sp,)), dma((n_sp,)),
            ],
            compiler_params=pltpu.CompilerParams(collective_id=0, has_side_effects=True,
                                                 vmem_limit_bytes=60 * 1024 * 1024),
        )(inputs, w_query, w_value, w_forget, w_gate, new_inputs, gate_room, extra_decay, out_gain.reshape(1, cols))

    return jax.shard_map(
        per_device,
        mesh=mesh,
        in_specs=(P("sp", "tp"), P(None, "tp"), P(None, "tp"), P(None, None, "tp"), P(None, "tp"),
                  P(None, "tp"), P("tp", "sp"), P("tp"), P()),
        out_specs=(P("sp", "tp"), P("tp", None, None), P(None, "tp")),
        check_vma=False,
    )
```

```python
import jax
import jax.numpy as jnp
from jax import lax
from jax.experimental import pallas as pl
from jax.experimental.pallas import tpu as pltpu
from jax.sharding import PartitionSpec as P

MESH = pl.DeviceIdType.MESH
EPS = 1e-06
B = 128
HD = 128
VM1 = 48
NX = 4
F32 = jnp.float32
BF16 = jnp.bfloat16


def nn(a, b):
    return lax.dot_general(a, b, (((1,), (0,)), ((), ())), preferred_element_type=F32)


def nt(a, b):
    return lax.dot_general(a, b, (((1,), (1,)), ((), ())), preferred_element_type=F32)


def tn(a, b):
    return lax.dot_general(a, b, (((0,), (0,)), ((), ())), preferred_element_type=F32)


def split2(a):
    hi = a.astype(BF16)
    return hi, (a - hi.astype(F32)).astype(BF16)


def log_one_minus(k):
    s = jnp.full_like(k, 1.0 / 8.0)
    for n in (7, 6, 5, 4, 3, 2):
        s = s * k + (1.0 / n)
    return -(s * k + 1.0) * k


def body(n_sp, n_tp, n_chunk, heads, x_hbm, wq, wv, wf, wg, nx_hbm, room_hbm, extra_hbm, gain_hbm,
         mixed_out, cache_out, read_out,
         x, w, nx, room, extra, gain, qs, vs, cf, cb, kf_s, kb_s, gs, a_f, a_b, e_f, e_b, s_f, s_b, acc,
         inside, qc_hi, qc_lo, st_hi, st_lo, stage_f, stage_b, stage_d, got_f, got_b, got_d, stage2, got2, fin, nq_hi, nq_lo, nv, nown, ngate,
         load_sem, own_sem, ag_send, ag_recv, d2_send, d2_recv, p1_send, p1_recv, p2_send, p2_recv,
         p3_send, p3_recv):
    cols = heads * HD
    sp = lax.axis_index("sp")
    tp = lax.axis_index("tp")
    right = lax.rem(tp + 2, n_tp)
    left = lax.rem(tp + n_tp - 2, n_tp)
    far = lax.rem(tp + 4, n_tp)
    flip = 1 - 2 * lax.rem(tp, 2)
    mate = tp + flip

    barrier = pltpu.get_barrier_semaphore()
    for peer in (mate, left, right):
        pl.semaphore_signal(barrier, inc=1, device_id={"tp": peer}, device_id_type=MESH)

    def greet(i, c):
        pl.semaphore_signal(barrier, inc=1, device_id={"sp": lax.rem(sp + i, n_sp)}, device_id_type=MESH)
        return c

    lax.fori_loop(1, n_sp, greet, 0)

    def block(owner):
        return pl.ds(pl.multiple_of(owner * cols, cols), cols)

    def rows(j):
        return pl.ds(pl.multiple_of(j * B, B), B)

    loads = [pltpu.make_async_copy(src, dst, load_sem.at[i]) for i, (src, dst) in enumerate((
        (x_hbm, x.at[:, block(tp)]), (room_hbm, room), (extra_hbm, extra), (wf.at[0], w.at[2]), (wf.at[1], w.at[3]),
        (wv, w.at[1]), (gain_hbm, gain), (wq, w.at[0]), (wg, w.at[4]), (nx_hbm, nx)))]
    for load in loads:
        load.start()

    t_id = lax.broadcasted_iota(jnp.int32, (B, B), 0)
    s_id = lax.broadcasted_iota(jnp.int32, (B, B), 1)
    lower = t_id >= s_id
    upper = s_id >= t_id

    def silu_gain(g):
        return gain[...] * (g / (1.0 + jnp.exp(-g)))

    def ring(kind, j):
        if kind == 0:
            src, to, r = block(tp), right, rows(j)
        elif kind == 1:
            src, to, r = block(tp), left, rows(j)
        elif kind == 2:
            src, to, r = block(left), right, pl.ds(pl.multiple_of(j * B, B), B // 2)
        else:
            src, to, r = block(right), left, pl.ds(pl.multiple_of(j * B + B // 2, B // 2), B // 2)
        return pltpu.make_async_remote_copy(
            src_ref=x.at[r, src], dst_ref=x.at[r, src], send_sem=ag_send.at[kind, j],
            recv_sem=ag_recv.at[kind, j], device_id={"tp": to}, device_id_type=MESH)

    def ring_in(kind, j):
        if kind == 0:
            src, r = block(left), rows(j)
        elif kind == 1:
            src, r = block(right), rows(j)
        elif kind == 2:
            src, r = block(far), pl.ds(pl.multiple_of(j * B, B), B // 2)
        else:
            src, r = block(far), pl.ds(pl.multiple_of(j * B + B // 2, B // 2), B // 2)
        return pltpu.make_async_remote_copy(
            src_ref=x.at[r, src], dst_ref=x.at[r, src], send_sem=ag_send.at[kind, j],
            recv_sem=ag_recv.at[kind, j], device_id={"tp": left}, device_id_type=MESH)

    def pair(kind, j, owner):
        return pltpu.make_async_remote_copy(
            src_ref=x.at[rows(j), block(owner)], dst_ref=x.at[rows(j), block(owner)],
            send_sem=d2_send.at[kind, j], recv_sem=d2_recv.at[kind, j],
            device_id={"tp": mate}, device_id_type=MESH)

    def pair_own(owner):
        return pltpu.make_async_remote_copy(
            src_ref=x.at[:, block(owner)], dst_ref=x.at[:, block(owner)],
            send_sem=own_sem.at[0], recv_sem=own_sem.at[1],
            device_id={"tp": mate}, device_id_type=MESH)

    loads[0].wait()
    pl.semaphore_wait(barrier, n_sp + 2)

    pair_own(tp).start()
    for j in range(2):
        ring(0, j).start()
        ring(1, j).start()

    s_f[...] = jnp.zeros_like(s_f)
    s_b[...] = jnp.zeros_like(s_b)
    acc[...] = jnp.zeros_like(acc)

    def compute(c):
        r = rows(c)
        xc = x[r, :]
        kf = room[0:1, :] / (1.0 + jnp.exp(nn(xc, w[2])))
        kb = room[1:2, :] / (1.0 + jnp.exp(nn(xc, w[3])))
        kf_s[r, :] = kf
        kb_s[r, :] = kb
        vc = nn(xc, w[1]).astype(BF16)
        vs[r, :] = vc
        tri_l = jnp.where(lower, 1.0, 0.0).astype(BF16)
        tri_u = jnp.where(upper, 1.0, 0.0).astype(BF16)
        lf_hi, lf_lo = split2(log_one_minus(kf))
        lb_hi, lb_lo = split2(log_one_minus(kb))
        wfc = nn(tri_l, lf_hi) + nn(tri_l, lf_lo)
        wbc = nn(tri_u, lb_hi) + nn(tri_u, lb_lo)
        ones = jnp.ones((B, HD), BF16)
        for h in range(heads):
            hs = slice(h * HD, (h + 1) * HD)
            ex = extra[h:h + 1, r]
            el_hi, el_lo = split2(jnp.where(lower, ex, 0.0))
            eu_hi, eu_lo = split2(jnp.where(upper, ex, 0.0))
            wfh = wfc[:, hs] + nn(el_hi, ones) + nn(el_lo, ones)
            wbh = wbc[:, hs] + nn(eu_hi, ones) + nn(eu_lo, ones)
            cf[r, hs] = wfh
            cb[r, hs] = wbh
            end_f = wfh[B - 1:B, :]
            end_b = wbh[0:1, :]
            ke_hi, ke_lo = split2(kf[:, hs] * jnp.exp(end_f - wfh))
            ke_b = (kb[:, hs] * jnp.exp(end_b - wbh)).astype(BF16)
            af = tn(vc[:, hs], ke_hi) + tn(vc[:, hs], ke_lo)
            ab = tn(vc[:, hs], ke_b)
            a_f[c, h] = af
            a_b[c, h] = ab
            e_f[c, h] = jnp.broadcast_to(jnp.exp(end_f), (8, HD))
            e_b[c, h] = jnp.broadcast_to(jnp.exp(end_b), (8, HD))
            s_f[h] = s_f[h] * jnp.exp(end_f) + af
            s_b[h] = s_b[h] + jnp.exp(acc[1, h, 0:1, :]) * ab
            acc[0, h] = acc[0, h] + end_f
            acc[1, h] = acc[1, h] + end_b

    def step(j, carry):
        @pl.when(j < n_chunk)
        def _():
            ring_in(0, j).wait_recv()
            ring_in(1, j).wait_recv()
            ring(2, j).start()
            ring(3, j).start()
            pair(0, j, left).start()
            pair(1, j, right).start()

        @pl.when(j + 2 < n_chunk)
        def _():
            ring(0, j + 2).start()
            ring(1, j + 2).start()

        @pl.when(j == 2)
        def _():
            pair_own(mate).wait_recv()
            for load in loads[1:6]:
                load.wait()

        @pl.when(j >= 2)
        def _():
            c = j - 2
            pair(0, c, left + flip).wait_recv()
            pair(1, c, right + flip).wait_recv()
            pair(2, c, far + flip).wait_recv()
            compute(c)

        @pl.when((j >= 1) & (j <= n_chunk))
        def _():
            ring_in(2, j - 1).wait_recv()
            ring_in(3, j - 1).wait_recv()
            pair(2, j - 1, far).start()

        return carry

    lax.fori_loop(0, n_chunk + 2, step, 0)

    per = n_sp // heads
    nz = n_sp // NX
    r_id = lax.broadcasted_iota(jnp.int32, (2, HD), 0)
    for h in range(heads):
        at = slice(h * per, (h + 1) * per)
        stage_f[at] = s_f[h].reshape(per, 8, HD)
        stage_b[at] = s_b[h].reshape(per, 8, HD).astype(BF16)
        both = jnp.where(r_id == 0, acc[0, h, 0:2], acc[1, h, 0:2])
        stage_d[at] = jnp.broadcast_to(both[None], (per, 2, HD))
    got_f[sp] = stage_f[sp]
    got_b[sp] = stage_b[sp]
    got_d[sp] = stage_d[sp]

    def other(i, sign):
        m, n = i // NX, lax.rem(i, NX)
        dz = nz // 2 + ((m + 1) // 2) * (1 - 2 * lax.rem(m, 2))
        dx = NX // 2 + ((n + 1) // 2) * (1 - 2 * lax.rem(n, 2))
        z, xx = sp // NX, lax.rem(sp, NX)
        return lax.rem(z + sign * dz + 2 * nz, nz) * NX + lax.rem(xx + sign * dx + 2 * NX, NX)

    def exchange(stages, gots, sends, recvs, whole=False):
        def copies(i, to, frm):
            return [pltpu.make_async_remote_copy(
                src_ref=st.at[sp] if whole else st.at[to], dst_ref=gt.at[frm], send_sem=sends.at[n, i],
                recv_sem=recvs.at[n, frm], device_id={"sp": to}, device_id_type=MESH)
                for n, (st, gt) in enumerate(zip(stages, gots))]

        def spread():
            def one(i, c):
                for copy in copies(i, other(i, 1), sp):
                    copy.start()
                return c
            lax.fori_loop(0, n_sp - 1, one, 0)

        def collect():
            def one(i, c):
                frm = other(i, -1)
                for copy in copies(i, frm, frm):
                    copy.wait_recv()
                return c
            lax.fori_loop(0, n_sp - 1, one, 0)

        def drain():
            def one(i, c):
                for copy in copies(i, other(i, 1), sp):
                    copy.wait_send()
                return c
            lax.fori_loop(0, n_sp - 1, one, 0)

        return spread, collect, drain

    spread1, collect1, drain1 = exchange((stage_d, stage_f, stage_b), (got_d, got_f, got_b), p1_send, p1_recv)
    spread2, collect2, drain2 = exchange((stage2,), (got2,), p2_send, p2_recv)
    spread3, collect3, drain3 = exchange((fin,), (fin,), p3_send, p3_recv, whole=True)

    spread1()

    def queries(c, carry):
        r = rows(c)
        xc = x[r, :]
        qs[r, :] = nn(xc, w[0]).astype(BF16)
        gs[r, :] = silu_gain(nn(xc, w[4]))
        return carry

    def scores(c, carry):
        r = rows(c)
        for h in range(heads):
            hs = slice(h * HD, (h + 1) * HD)
            wfh = cf[r, hs]
            wbh = cb[r, hs]
            mid_f = wfh[B // 2:B // 2 + 1, :]
            mid_b = wbh[B // 2 - 1:B // 2, :]
            q = qs[r, hs].astype(F32)
            qi_f = (q * jnp.exp(wfh - mid_f)).astype(BF16)
            qi_b = (q * jnp.exp(wbh - mid_b)).astype(BF16)
            ki_f = (kf_s[r, hs] * jnp.exp(mid_f - wfh)).astype(BF16)
            ki_b = (kb_s[r, hs] * jnp.exp(mid_b - wbh)).astype(BF16)
            sc = jnp.where(lower, nt(qi_f, ki_f), 0.0) + jnp.where(upper, nt(qi_b, ki_b), 0.0)
            inside[r, hs] = nn(sc.astype(BF16), vs[r, hs])
            qc_hi[h, r, 0:HD], qc_lo[h, r, 0:HD] = split2(q * jnp.exp(wfh))
            qc_hi[h, r, HD:2 * HD], qc_lo[h, r, HD:2 * HD] = split2(q * jnp.exp(wbh))
        return carry

    def inner(c, carry):
        queries(c, 0)
        return scores(c, 0)

    for load in loads[6:]:
        load.wait()
    early = n_chunk // 2
    lax.fori_loop(0, early, inner, 0)
    new = nx[...]
    nqf = nn(new, w[0]).astype(BF16).astype(F32)
    nv[...] = nn(new, w[1]).astype(BF16)
    nf = room[0:1, :] / (1.0 + jnp.exp(nn(new, w[2])))
    nb = room[1:2, :] / (1.0 + jnp.exp(nn(new, w[3])))
    ngate[...] = silu_gain(nn(new, w[4]))
    nq_hi[...], nq_lo[...] = split2(nqf * (1.0 - nf))
    nown[...] = nqf * (nf + nb)

    collect1()

    def decay(q, at):
        return jnp.exp(got_d[q, at:at + 1, :])

    run = jnp.zeros((8, HD), F32)
    before = []
    for q in range(n_sp):
        before.append(run)
        run = run * decay(q, 0) + got_f[q]
    fin[sp] = run.astype(BF16)
    run = jnp.zeros((8, HD), F32)
    for q in reversed(range(n_sp)):
        stage2[q, 0] = before[q]
        stage2[q, 1] = run
        run = run * decay(q, 1) + got_b[q].astype(F32)
    got2[sp] = stage2[sp]
    spread2()
    spread3()

    lax.fori_loop(early, n_chunk, inner, 0)

    def settle(j, c):
        for kind in range(4):
            ring(kind, j).wait_send()
        pair(0, j, left).wait_send()
        pair(1, j, right).wait_send()
        pair(2, j, far).wait_send()
        return c

    lax.fori_loop(0, n_chunk, settle, 0)
    pair_own(tp).wait_send()
    drain1()
    collect2()

    for h in range(heads):
        run = got2[h * per:(h + 1) * per, 0].reshape(HD, HD)
        for c in range(n_chunk):
            st_hi[h, c, :, 0:HD], st_lo[h, c, :, 0:HD] = split2(run)
            run = run * e_f[c, h, 0:1, :] + a_f[c, h]
        run = got2[h * per:(h + 1) * per, 1].reshape(HD, HD)
        for c in reversed(range(n_chunk)):
            st_hi[h, c, :, HD:2 * HD], st_lo[h, c, :, HD:2 * HD] = split2(run)
            run = run * e_b[c, h, 0:1, :] + a_b[c, h]

    def norm(mix, scale):
        return (mix * lax.rsqrt(jnp.mean(mix * mix, axis=-1, keepdims=True) + EPS) * scale).astype(BF16)

    def finish(c, carry):
        r = rows(c)
        for h in range(heads):
            hs = slice(h * HD, (h + 1) * HD)
            mix = (inside[r, hs] + nt(qc_lo[h, r, :], st_hi[h, c]) + nt(qc_hi[h, r, :], st_lo[h, c])
                   + nt(qc_hi[h, r, :], st_hi[h, c]))
            mixed_out[r, hs] = norm(mix, gs[r, hs])
        return carry

    lax.fori_loop(0, n_chunk, finish, 0, unroll=2)

    collect3()
    for h in range(heads):
        hs = slice(h * HD, (h + 1) * HD)
        last = fin[h * per:(h + 1) * per].astype(F32).reshape(HD, HD)
        cached = last.astype(BF16)
        cache_out[h] = last.T.astype(BF16)
        own = jnp.sum(nown[:, hs], axis=-1, keepdims=True) * nv[:, hs].astype(F32)
        read_out[:, hs] = norm(nt(nq_lo[:, hs], cached) + nt(nq_hi[:, hs], cached) + own, ngate[:, hs])

    drain2()
    drain3()


def solution(mesh):
    n_sp, n_tp = mesh.shape["sp"], mesh.shape["tp"]

    def per_device(inputs, w_query, w_value, w_forget, w_gate, gate_room, extra_decay, out_gain, new_inputs):
        tokens, cols = inputs.shape
        depth = w_query.shape[0]
        heads = extra_decay.shape[0]
        fresh = new_inputs.shape[0]
        chunks = tokens // B
        hbm = pl.BlockSpec(memory_space=pltpu.HBM)
        vmem = pl.BlockSpec(memory_space=pltpu.VMEM)

        def kernel(*refs):
            body(n_sp, n_tp, chunks, heads, *refs)

        dma = pltpu.SemaphoreType.DMA
        done = pl.pallas_call(
            kernel,
            out_shape=(jax.ShapeDtypeStruct((tokens, cols), BF16),
                       jax.ShapeDtypeStruct((heads, HD, HD), BF16),
                       jax.ShapeDtypeStruct((fresh, cols), BF16)),
            in_specs=[hbm] * 9,
            out_specs=(vmem, vmem, vmem),
            scratch_shapes=[
                pltpu.VMEM((tokens, depth), BF16),
                pltpu.VMEM((5, depth, cols), BF16),
                pltpu.VMEM((fresh, depth), BF16),
                pltpu.VMEM((2, cols), F32),
                pltpu.VMEM((heads, tokens), F32),
                pltpu.VMEM((1, cols), F32),
                pltpu.VMEM((tokens, cols), BF16),
                pltpu.VMEM((tokens, cols), BF16),
                pltpu.VMEM((tokens, cols), F32),
                pltpu.VMEM((tokens, cols), F32),
                pltpu.VMEM((tokens, cols), F32),
                pltpu.VMEM((tokens, cols), F32),
                pltpu.VMEM((tokens, cols), F32),
                pltpu.VMEM((chunks, heads, HD, HD), F32),
                pltpu.VMEM((chunks, heads, HD, HD), F32),
                pltpu.VMEM((chunks, heads, 8, HD), F32),
                pltpu.VMEM((chunks, heads, 8, HD), F32),
                pltpu.VMEM((heads, HD, HD), F32),
                pltpu.VMEM((heads, HD, HD), F32),
                pltpu.VMEM((2, heads, 8, HD), F32),
                pltpu.VMEM((tokens, cols), F32),
                pltpu.VMEM((heads, tokens, 2 * HD), BF16),
                pltpu.VMEM((heads, tokens, 2 * HD), BF16),
                pltpu.VMEM((heads, chunks, HD, 2 * HD), BF16),
                pltpu.VMEM((heads, chunks, HD, 2 * HD), BF16),
                pltpu.VMEM((n_sp, 8, HD), F32),
                pltpu.VMEM((n_sp, 8, HD), BF16),
                pltpu.VMEM((n_sp, 2, HD), F32),
                pltpu.VMEM((n_sp, 8, HD), F32),
                pltpu.VMEM((n_sp, 8, HD), BF16),
                pltpu.VMEM((n_sp, 2, HD), F32),
                pltpu.VMEM((n_sp, 2, 8, HD), F32),
                pltpu.VMEM((n_sp, 2, 8, HD), F32),
                pltpu.VMEM((n_sp, 8, HD), BF16),
                pltpu.VMEM((fresh, cols), BF16),
                pltpu.VMEM((fresh, cols), BF16),
                pltpu.VMEM((fresh, cols), BF16),
                pltpu.VMEM((fresh, cols), F32),
                pltpu.VMEM((fresh, cols), F32),
                dma((10,)), dma((2,)),
                dma((4, chunks)), dma((4, chunks)),
                dma((3, chunks)), dma((3, chunks)),
                dma((3, n_sp)), dma((3, n_sp)),
                dma((1, n_sp)), dma((1, n_sp)),
                dma((1, n_sp)), dma((1, n_sp)),
            ],
            compiler_params=pltpu.CompilerParams(collective_id=0, has_side_effects=True,
                                                 vmem_limit_bytes=VM1 * 1024 * 1024),
        )(*(pltpu.with_memory_space_constraint(a, pltpu.HBM) for a in (
            inputs, w_query, w_value, w_forget, w_gate, new_inputs, gate_room, extra_decay, out_gain.reshape(1, cols))))

        def put(a, b, c, a_out, b_out, c_out, sems):
            copies = [pltpu.make_async_copy(s, d, sems.at[i])
                      for i, (s, d) in enumerate(((a, a_out), (b, b_out), (c, c_out)))]
            for copy in copies:
                copy.start()
            for copy in copies:
                copy.wait()

        return pl.pallas_call(
            put,
            out_shape=tuple(jax.ShapeDtypeStruct(d.shape, d.dtype) for d in done),
            in_specs=[vmem] * 3,
            out_specs=(hbm,) * 3,
            scratch_shapes=[dma((3,))],
            compiler_params=pltpu.CompilerParams(vmem_limit_bytes=4 * 1024 * 1024),
        )(*done)

    return jax.shard_map(
        per_device,
        mesh=mesh,
        in_specs=(P("sp", "tp"), P(None, "tp"), P(None, "tp"), P(None, None, "tp"), P(None, "tp"),
                  P(None, "tp"), P("tp", "sp"), P("tp"), P()),
        out_specs=(P("sp", "tp"), P("tp", None, None), P(None, "tp")),
        check_vma=False,
    )
```

```python
import jax
import jax.numpy as jnp
from jax import lax
from jax.experimental import pallas as pl
from jax.experimental.pallas import tpu as pltpu
from jax.sharding import PartitionSpec as P

MESH = pl.DeviceIdType.MESH
EPS = 1e-06
B = 128
HD = 128
VM1 = 48
LEAD = 3
NX = 4
F32 = jnp.float32
BF16 = jnp.bfloat16


def nn(a, b):
    return lax.dot_general(a, b, (((1,), (0,)), ((), ())), preferred_element_type=F32)


def nt(a, b):
    return lax.dot_general(a, b, (((1,), (1,)), ((), ())), preferred_element_type=F32)


def tn(a, b):
    return lax.dot_general(a, b, (((0,), (0,)), ((), ())), preferred_element_type=F32)


def split2(a):
    hi = a.astype(BF16)
    return hi, (a - hi.astype(F32)).astype(BF16)


def log_one_minus(k):
    s = jnp.full_like(k, 1.0 / 8.0)
    for n in (7, 6, 5, 4, 3, 2):
        s = s * k + (1.0 / n)
    return -(s * k + 1.0) * k


def body(n_sp, n_tp, n_chunk, heads, x_hbm, wq, wv, wf, wg, nx_hbm, room_hbm, extra_hbm, gain_hbm,
         mixed_out, cache_out, read_out,
         x, w, nx, part, room, extra, gain, qs, vs, cf, cb, kf_s, kb_s, gs, a_f, a_b, e_f, e_b, s_f, s_b, acc,
         inside, qc_hi, qc_lo, st_hi, st_lo, stage_f, stage_b, stage_d, got_f, got_b, got_d, stage2, got2, fin, nq_hi, nq_lo, nv, nown, ngate,
         load_sem, own_sem, out_sem, near_in, far_in, mate_near, mate_far, p1_send, p1_recv, p2_send, p2_recv,
         p3_send, p3_recv):
    cols = heads * HD
    sp = lax.axis_index("sp")
    tp = lax.axis_index("tp")
    right = lax.rem(tp + 2, n_tp)
    left = lax.rem(tp + n_tp - 2, n_tp)
    far = lax.rem(tp + 4, n_tp)
    flip = 1 - 2 * lax.rem(tp, 2)
    mate = tp + flip

    barrier = pltpu.get_barrier_semaphore()
    for peer in (mate, left, right):
        pl.semaphore_signal(barrier, inc=1, device_id={"tp": peer}, device_id_type=MESH)

    def greet(i, c):
        pl.semaphore_signal(barrier, inc=1, device_id={"sp": lax.rem(sp + i, n_sp)}, device_id_type=MESH)
        return c

    lax.fori_loop(1, n_sp, greet, 0)

    def block(owner):
        return pl.ds(pl.multiple_of(owner * cols, cols), cols)

    def rows(j):
        return pl.ds(pl.multiple_of(j * B, B), B)

    loads = [pltpu.make_async_copy(src, dst, load_sem.at[i]) for i, (src, dst) in enumerate((
        (x_hbm, x.at[:, block(tp)]), (room_hbm, room), (extra_hbm, extra), (wf.at[0], w.at[2]), (wf.at[1], w.at[3]),
        (wv, w.at[1]), (gain_hbm, gain), (wq, w.at[0]), (wg, w.at[4]), (nx_hbm, nx)))]
    for load in loads:
        load.start()

    t_id = lax.broadcasted_iota(jnp.int32, (B, B), 0)
    s_id = lax.broadcasted_iota(jnp.int32, (B, B), 1)
    lower = t_id >= s_id
    upper = s_id >= t_id

    def silu_gain(g):
        return gain[...] * (g / (1.0 + jnp.exp(-g)))

    def half(j, k):
        return pl.ds(pl.multiple_of(j * B + k * (B // 2), B // 2), B // 2)

    def chip(owner):
        return pl.ds(pl.multiple_of((owner // 2) * (2 * cols), 2 * cols), 2 * cols)

    def push(r, c, to, out, inn):
        return pltpu.make_async_remote_copy(
            src_ref=x.at[r, c], dst_ref=x.at[r, c], send_sem=out, recv_sem=inn,
            device_id={"tp": to}, device_id_type=MESH)

    def send_own(j):
        push(rows(j), block(tp), right, out_sem.at[0], near_in.at[j]).start()
        push(rows(j), block(tp), left, out_sem.at[0], near_in.at[j]).start()

    def pass_near(j):
        push(half(j, 0), block(left), right, out_sem.at[1], far_in.at[j]).start()
        push(half(j, 1), block(right), left, out_sem.at[1], far_in.at[j]).start()
        push(rows(j), block(left), mate, out_sem.at[2], mate_near.at[j]).start()
        push(rows(j), block(right), mate, out_sem.at[2], mate_near.at[j]).start()

    def pass_far(j):
        push(rows(j), block(far), mate, out_sem.at[3], mate_far.at[j]).start()

    whole = pl.ds(0, n_chunk * B)

    def pair_own(owner):
        return push(whole, block(owner), mate, own_sem.at[0], own_sem.at[1])

    loads[0].wait()
    pl.semaphore_wait(barrier, n_sp + 2)

    pair_own(tp).start()
    for j in range(LEAD):
        send_own(j)

    kinds = (2, 3, 1)

    def own_part(c, carry):
        r = rows(c)
        xc = x[r, chip(tp)]
        for n, i in enumerate(kinds):
            part[n, r, :] = nn(xc, w[i, chip(tp), :])
        return carry

    def near_part(c):
        r = rows(c)
        xl, xr = x[r, chip(left)], x[r, chip(right)]
        for n, i in enumerate(kinds):
            part[n, r, :] += nn(xl, w[i, chip(left), :]) + nn(xr, w[i, chip(right), :])

    for load in loads[1:6]:
        load.wait()
    pair_own(mate).wait_recv()
    lax.fori_loop(0, n_chunk, own_part, 0)

    s_f[...] = jnp.zeros_like(s_f)
    s_b[...] = jnp.zeros_like(s_b)
    acc[...] = jnp.zeros_like(acc)

    def compute(c):
        r = rows(c)
        xc = x[r, chip(far)]
        kf = room[0:1, :] / (1.0 + jnp.exp(part[0, r, :] + nn(xc, w[2, chip(far), :])))
        kb = room[1:2, :] / (1.0 + jnp.exp(part[1, r, :] + nn(xc, w[3, chip(far), :])))
        kf_s[r, :] = kf
        kb_s[r, :] = kb
        vc = (part[2, r, :] + nn(xc, w[1, chip(far), :])).astype(BF16)
        vs[r, :] = vc
        tri_l = jnp.where(lower, 1.0, 0.0).astype(BF16)
        tri_u = jnp.where(upper, 1.0, 0.0).astype(BF16)
        lf_hi, lf_lo = split2(log_one_minus(kf))
        lb_hi, lb_lo = split2(log_one_minus(kb))
        wfc = nn(tri_l, lf_hi) + nn(tri_l, lf_lo)
        wbc = nn(tri_u, lb_hi) + nn(tri_u, lb_lo)
        ones = jnp.ones((B, HD), BF16)
        for h in range(heads):
            hs = slice(h * HD, (h + 1) * HD)
            ex = extra[h:h + 1, r]
            el_hi, el_lo = split2(jnp.where(lower, ex, 0.0))
            eu_hi, eu_lo = split2(jnp.where(upper, ex, 0.0))
            wfh = wfc[:, hs] + nn(el_hi, ones) + nn(el_lo, ones)
            wbh = wbc[:, hs] + nn(eu_hi, ones) + nn(eu_lo, ones)
            cf[r, hs] = wfh
            cb[r, hs] = wbh
            end_f = wfh[B - 1:B, :]
            end_b = wbh[0:1, :]
            ke_hi, ke_lo = split2(kf[:, hs] * jnp.exp(end_f - wfh))
            ke_b = (kb[:, hs] * jnp.exp(end_b - wbh)).astype(BF16)
            af = tn(vc[:, hs], ke_hi) + tn(vc[:, hs], ke_lo)
            ab = tn(vc[:, hs], ke_b)
            a_f[c, h] = af
            a_b[c, h] = ab
            e_f[c, h] = jnp.broadcast_to(jnp.exp(end_f), (8, HD))
            e_b[c, h] = jnp.broadcast_to(jnp.exp(end_b), (8, HD))
            s_f[h] = s_f[h] * jnp.exp(end_f) + af
            s_b[h] = s_b[h] + jnp.exp(acc[1, h, 0:1, :]) * ab
            acc[0, h] = acc[0, h] + end_f
            acc[1, h] = acc[1, h] + end_b

    def step(j, carry):
        @pl.when(j < n_chunk)
        def _():
            push(rows(j), chip(left), left, out_sem.at[0], near_in.at[j]).wait_recv()
            pass_near(j)

        @pl.when(j + LEAD < n_chunk)
        def _():
            send_own(j + LEAD)

        @pl.when((j >= 1) & (j <= n_chunk))
        def _():
            c = j - 1
            push(rows(c), chip(left), mate, out_sem.at[2], mate_near.at[c]).wait_recv()
            near_part(c)
            push(rows(c), block(far), left, out_sem.at[1], far_in.at[c]).wait_recv()
            pass_far(c)

        @pl.when(j >= 2)
        def _():
            c = j - 2
            push(rows(c), block(far), mate, out_sem.at[3], mate_far.at[c]).wait_recv()
            compute(c)

        return carry

    lax.fori_loop(0, n_chunk + 2, step, 0)

    per = n_sp // heads
    nz = n_sp // NX
    r_id = lax.broadcasted_iota(jnp.int32, (2, HD), 0)
    for h in range(heads):
        at = slice(h * per, (h + 1) * per)
        stage_f[at] = s_f[h].reshape(per, 8, HD)
        stage_b[at] = s_b[h].reshape(per, 8, HD).astype(BF16)
        both = jnp.where(r_id == 0, acc[0, h, 0:2], acc[1, h, 0:2])
        stage_d[at] = jnp.broadcast_to(both[None], (per, 2, HD))
    got_f[sp] = stage_f[sp]
    got_b[sp] = stage_b[sp]
    got_d[sp] = stage_d[sp]

    def other(i):
        m, n = i // NX, lax.rem(i, NX)
        dz = nz // 2 + ((m + 1) // 2) * (1 - 2 * lax.rem(m, 2))
        dx = NX // 2 + ((n + 1) // 2) * (1 - 2 * lax.rem(n, 2))
        z, xx = sp // NX, lax.rem(sp, NX)
        return lax.rem(z + dz, nz) * NX + lax.rem(xx + dx, NX)

    def exchange(stages, gots, sends, recvs, whole=False):
        def copies(to, frm):
            return [pltpu.make_async_remote_copy(
                src_ref=st.at[sp] if whole else st.at[to], dst_ref=gt.at[frm], send_sem=sends.at[n],
                recv_sem=recvs.at[n], device_id={"sp": to}, device_id_type=MESH)
                for n, (st, gt) in enumerate(zip(stages, gots))]

        def spread():
            def one(i, c):
                for copy in copies(other(i), sp):
                    copy.start()
                return c
            lax.fori_loop(0, n_sp - 1, one, 0)

        every = [pltpu.make_async_remote_copy(
            src_ref=st.at[pl.ds(0, n_sp - 1)], dst_ref=gt.at[pl.ds(0, n_sp - 1)], send_sem=sends.at[n],
            recv_sem=recvs.at[n], device_id={"sp": other(0)}, device_id_type=MESH)
            for n, (st, gt) in enumerate(zip(stages, gots))]

        def collect():
            for copy in every:
                copy.wait_recv()

        def drain():
            for copy in every:
                copy.wait_send()

        return spread, collect, drain

    spread1, collect1, drain1 = exchange((stage_d, stage_f, stage_b), (got_d, got_f, got_b), p1_send, p1_recv)
    spread2, collect2, drain2 = exchange((stage2,), (got2,), p2_send, p2_recv)
    spread3, collect3, drain3 = exchange((fin,), (fin,), p3_send, p3_recv, whole=True)

    spread1()

    def queries(c, carry):
        r = rows(c)
        xc = x[r, :]
        qs[r, :] = nn(xc, w[0]).astype(BF16)
        gs[r, :] = silu_gain(nn(xc, w[4]))
        return carry

    def scores(c, carry):
        r = rows(c)
        for h in range(heads):
            hs = slice(h * HD, (h + 1) * HD)
            wfh = cf[r, hs]
            wbh = cb[r, hs]
            mid_f = wfh[B // 2:B // 2 + 1, :]
            mid_b = wbh[B // 2 - 1:B // 2, :]
            q = qs[r, hs].astype(F32)
            qi_f = (q * jnp.exp(wfh - mid_f)).astype(BF16)
            qi_b = (q * jnp.exp(wbh - mid_b)).astype(BF16)
            ki_f = (kf_s[r, hs] * jnp.exp(mid_f - wfh)).astype(BF16)
            ki_b = (kb_s[r, hs] * jnp.exp(mid_b - wbh)).astype(BF16)
            sc = jnp.where(lower, nt(qi_f, ki_f), 0.0) + jnp.where(upper, nt(qi_b, ki_b), 0.0)
            inside[r, hs] = nn(sc.astype(BF16), vs[r, hs])
            qc_hi[h, r, 0:HD], qc_lo[h, r, 0:HD] = split2(q * jnp.exp(wfh))
            qc_hi[h, r, HD:2 * HD], qc_lo[h, r, HD:2 * HD] = split2(q * jnp.exp(wbh))
        return carry

    def inner(c, carry):
        queries(c, 0)
        return scores(c, 0)

    for load in loads[6:]:
        load.wait()
    early = n_chunk // 2
    lax.fori_loop(0, early, inner, 0)
    new = nx[...]
    nqf = nn(new, w[0]).astype(BF16).astype(F32)
    nv[...] = nn(new, w[1]).astype(BF16)
    nf = room[0:1, :] / (1.0 + jnp.exp(nn(new, w[2])))
    nb = room[1:2, :] / (1.0 + jnp.exp(nn(new, w[3])))
    ngate[...] = silu_gain(nn(new, w[4]))
    nq_hi[...], nq_lo[...] = split2(nqf * (1.0 - nf))
    nown[...] = nqf * (nf + nb)

    collect1()

    def decay(q, at):
        return jnp.exp(got_d[q, at:at + 1, :])

    run = jnp.zeros((8, HD), F32)
    before = []
    for q in range(n_sp):
        before.append(run)
        run = run * decay(q, 0) + got_f[q]
    fin[sp] = run.astype(BF16)
    run = jnp.zeros((8, HD), F32)
    for q in reversed(range(n_sp)):
        stage2[q, 0] = before[q]
        stage2[q, 1] = run
        run = run * decay(q, 1) + got_b[q].astype(F32)
    got2[sp] = stage2[sp]
    spread2()
    inner(early, 0)
    spread3()
    lax.fori_loop(early + 1, n_chunk, inner, 0)

    push(whole, chip(tp), left, out_sem.at[0], near_in.at[0]).wait_send()
    push(whole, block(tp), left, out_sem.at[1], near_in.at[0]).wait_send()
    push(whole, chip(tp), left, out_sem.at[2], near_in.at[0]).wait_send()
    push(whole, block(tp), left, out_sem.at[3], near_in.at[0]).wait_send()
    pair_own(tp).wait_send()
    drain1()
    collect2()

    for h in range(heads):
        run = got2[h * per:(h + 1) * per, 0].reshape(HD, HD)
        for c in range(n_chunk):
            st_hi[h, c, :, 0:HD], st_lo[h, c, :, 0:HD] = split2(run)
            run = run * e_f[c, h, 0:1, :] + a_f[c, h]
        run = got2[h * per:(h + 1) * per, 1].reshape(HD, HD)
        for c in reversed(range(n_chunk)):
            st_hi[h, c, :, HD:2 * HD], st_lo[h, c, :, HD:2 * HD] = split2(run)
            run = run * e_b[c, h, 0:1, :] + a_b[c, h]

    def norm(mix, scale):
        return (mix * lax.rsqrt(jnp.mean(mix * mix, axis=-1, keepdims=True) + EPS) * scale).astype(BF16)

    def finish(c, carry):
        r = rows(c)
        for h in range(heads):
            hs = slice(h * HD, (h + 1) * HD)
            mix = (inside[r, hs] + nt(qc_lo[h, r, :], st_hi[h, c]) + nt(qc_hi[h, r, :], st_lo[h, c])
                   + nt(qc_hi[h, r, :], st_hi[h, c]))
            mixed_out[r, hs] = norm(mix, gs[r, hs])
        return carry

    lax.fori_loop(0, n_chunk, finish, 0, unroll=2)

    collect3()
    for h in range(heads):
        hs = slice(h * HD, (h + 1) * HD)
        last = fin[h * per:(h + 1) * per].astype(F32).reshape(HD, HD)
        cached = last.astype(BF16)
        cache_out[h] = last.T.astype(BF16)
        own = jnp.sum(nown[:, hs], axis=-1, keepdims=True) * nv[:, hs].astype(F32)
        read_out[:, hs] = norm(nt(nq_lo[:, hs], cached) + nt(nq_hi[:, hs], cached) + own, ngate[:, hs])

    drain2()
    drain3()


def solution(mesh):
    n_sp, n_tp = mesh.shape["sp"], mesh.shape["tp"]

    def per_device(inputs, w_query, w_value, w_forget, w_gate, gate_room, extra_decay, out_gain, new_inputs):
        tokens, cols = inputs.shape
        depth = w_query.shape[0]
        heads = extra_decay.shape[0]
        fresh = new_inputs.shape[0]
        chunks = tokens // B
        hbm = pl.BlockSpec(memory_space=pltpu.HBM)
        vmem = pl.BlockSpec(memory_space=pltpu.VMEM)

        def kernel(*refs):
            body(n_sp, n_tp, chunks, heads, *refs)

        dma = pltpu.SemaphoreType.DMA
        done = pl.pallas_call(
            kernel,
            out_shape=(jax.ShapeDtypeStruct((tokens, cols), BF16),
                       jax.ShapeDtypeStruct((heads, HD, HD), BF16),
                       jax.ShapeDtypeStruct((fresh, cols), BF16)),
            in_specs=[hbm] * 9,
            out_specs=(vmem, vmem, vmem),
            scratch_shapes=[
                pltpu.VMEM((tokens, depth), BF16),
                pltpu.VMEM((5, depth, cols), BF16),
                pltpu.VMEM((fresh, depth), BF16),
                pltpu.VMEM((3, tokens, cols), F32),
                pltpu.VMEM((2, cols), F32),
                pltpu.VMEM((heads, tokens), F32),
                pltpu.VMEM((1, cols), F32),
                pltpu.VMEM((tokens, cols), BF16),
                pltpu.VMEM((tokens, cols), BF16),
                pltpu.VMEM((tokens, cols), F32),
                pltpu.VMEM((tokens, cols), F32),
                pltpu.VMEM((tokens, cols), F32),
                pltpu.VMEM((tokens, cols), F32),
                pltpu.VMEM((tokens, cols), F32),
                pltpu.VMEM((chunks, heads, HD, HD), F32),
                pltpu.VMEM((chunks, heads, HD, HD), F32),
                pltpu.VMEM((chunks, heads, 8, HD), F32),
                pltpu.VMEM((chunks, heads, 8, HD), F32),
                pltpu.VMEM((heads, HD, HD), F32),
                pltpu.VMEM((heads, HD, HD), F32),
                pltpu.VMEM((2, heads, 8, HD), F32),
                pltpu.VMEM((tokens, cols), F32),
                pltpu.VMEM((heads, tokens, 2 * HD), BF16),
                pltpu.VMEM((heads, tokens, 2 * HD), BF16),
                pltpu.VMEM((heads, chunks, HD, 2 * HD), BF16),
                pltpu.VMEM((heads, chunks, HD, 2 * HD), BF16),
                pltpu.VMEM((n_sp, 8, HD), F32),
                pltpu.VMEM((n_sp, 8, HD), BF16),
                pltpu.VMEM((n_sp, 2, HD), F32),
                pltpu.VMEM((n_sp, 8, HD), F32),
                pltpu.VMEM((n_sp, 8, HD), BF16),
                pltpu.VMEM((n_sp, 2, HD), F32),
                pltpu.VMEM((n_sp, 2, 8, HD), F32),
                pltpu.VMEM((n_sp, 2, 8, HD), F32),
                pltpu.VMEM((n_sp, 8, HD), BF16),
                pltpu.VMEM((fresh, cols), BF16),
                pltpu.VMEM((fresh, cols), BF16),
                pltpu.VMEM((fresh, cols), BF16),
                pltpu.VMEM((fresh, cols), F32),
                pltpu.VMEM((fresh, cols), F32),
                dma((10,)), dma((2,)),
                dma((4,)), dma((chunks,)), dma((chunks,)), dma((chunks,)), dma((chunks,)),
                dma((3,)), dma((3,)), dma((1,)), dma((1,)), dma((1,)), dma((1,)),
            ],
            compiler_params=pltpu.CompilerParams(collective_id=0, has_side_effects=True,
                                                 vmem_limit_bytes=VM1 * 1024 * 1024),
        )(*(pltpu.with_memory_space_constraint(a, pltpu.HBM) for a in (
            inputs, w_query, w_value, w_forget, w_gate, new_inputs, gate_room, extra_decay, out_gain.reshape(1, cols))))

        def put(a, b, c, a_out, b_out, c_out, sems):
            copies = [pltpu.make_async_copy(s, d, sems.at[i])
                      for i, (s, d) in enumerate(((a, a_out), (b, b_out), (c, c_out)))]
            for copy in copies:
                copy.start()
            for copy in copies:
                copy.wait()

        return pl.pallas_call(
            put,
            out_shape=tuple(jax.ShapeDtypeStruct(d.shape, d.dtype) for d in done),
            in_specs=[vmem] * 3,
            out_specs=(hbm,) * 3,
            scratch_shapes=[dma((3,))],
            compiler_params=pltpu.CompilerParams(vmem_limit_bytes=4 * 1024 * 1024),
        )(*done)

    return jax.shard_map(
        per_device,
        mesh=mesh,
        in_specs=(P("sp", "tp"), P(None, "tp"), P(None, "tp"), P(None, None, "tp"), P(None, "tp"),
                  P(None, "tp"), P("tp", "sp"), P("tp"), P()),
        out_specs=(P("sp", "tp"), P("tp", None, None), P(None, "tp")),
        check_vma=False,
    )
```

```python
import jax
import jax.numpy as jnp
from jax import lax
from jax.experimental import pallas as pl
from jax.experimental.pallas import tpu as pltpu
from jax.sharding import PartitionSpec as P

MESH = pl.DeviceIdType.MESH
EPS = 1e-06
B = 128
HD = 128
VM1 = 48
LEAD = 3
LAG = 2
NX = 4
F32 = jnp.float32
BF16 = jnp.bfloat16


def nn(a, b):
    return lax.dot_general(a, b, (((1,), (0,)), ((), ())), preferred_element_type=F32)


def nt(a, b):
    return lax.dot_general(a, b, (((1,), (1,)), ((), ())), preferred_element_type=F32)


def tn(a, b):
    return lax.dot_general(a, b, (((0,), (0,)), ((), ())), preferred_element_type=F32)


def split2(a):
    hi = a.astype(BF16)
    return hi, (a - hi.astype(F32)).astype(BF16)


def log_one_minus(k):
    s = jnp.full_like(k, 1.0 / 8.0)
    for n in (7, 6, 5, 4, 3, 2):
        s = s * k + (1.0 / n)
    return -(s * k + 1.0) * k


def body(n_sp, n_tp, n_chunk, heads, x_hbm, wq, wv, wf, wg, nx_hbm, room_hbm, extra_hbm, gain_hbm,
         mixed_out, cache_out, read_out,
         x, w, nx, part, room, extra, gain, qs, vs, cf, cb, kf_s, kb_s, gs, a_f, a_b, e_f, e_b, s_f, s_b, acc,
         inside, qc, st, stage_f, stage_b, stage_d, got_f, got_b, got_d, stage2, got2, fin, nq_hi, nq_lo, nv, nown, ngate,
         load_sem, own_sem, out_sem, near_in, far_in, mate_near, mate_far, p1_send, p1_recv, p2_send, p2_recv,
         p3_send, p3_recv):
    cols = heads * HD
    sp = lax.axis_index("sp")
    tp = lax.axis_index("tp")
    right = lax.rem(tp + 2, n_tp)
    left = lax.rem(tp + n_tp - 2, n_tp)
    far = lax.rem(tp + 4, n_tp)
    flip = 1 - 2 * lax.rem(tp, 2)
    mate = tp + flip

    barrier = pltpu.get_barrier_semaphore()
    for peer in (mate, left, right):
        pl.semaphore_signal(barrier, inc=1, device_id={"tp": peer}, device_id_type=MESH)

    def greet(i, c):
        pl.semaphore_signal(barrier, inc=1, device_id={"sp": lax.rem(sp + i, n_sp)}, device_id_type=MESH)
        return c

    lax.fori_loop(1, n_sp, greet, 0)

    def block(owner):
        return pl.ds(pl.multiple_of(owner * cols, cols), cols)

    def rows(j):
        return pl.ds(pl.multiple_of(j * B, B), B)

    loads = [pltpu.make_async_copy(src, dst, load_sem.at[i]) for i, (src, dst) in enumerate((
        (x_hbm, x.at[:, block(tp)]), (room_hbm, room), (extra_hbm, extra), (wf.at[0], w.at[2]), (wf.at[1], w.at[3]),
        (wv, w.at[1]), (gain_hbm, gain), (wq, w.at[0]), (wg, w.at[4]), (nx_hbm, nx)))]
    for load in loads:
        load.start()

    t_id = lax.broadcasted_iota(jnp.int32, (B, B), 0)
    s_id = lax.broadcasted_iota(jnp.int32, (B, B), 1)
    lower = t_id >= s_id
    upper = s_id >= t_id

    def silu_gain(g):
        return gain[...] * (g / (1.0 + jnp.exp(-g)))

    def half(j, k):
        return pl.ds(pl.multiple_of(j * B + k * (B // 2), B // 2), B // 2)

    def chip(owner):
        return pl.ds(pl.multiple_of((owner // 2) * (2 * cols), 2 * cols), 2 * cols)

    def push(r, c, to, out, inn):
        return pltpu.make_async_remote_copy(
            src_ref=x.at[r, c], dst_ref=x.at[r, c], send_sem=out, recv_sem=inn,
            device_id={"tp": to}, device_id_type=MESH)

    def send_own(j):
        push(rows(j), block(tp), right, out_sem.at[0], near_in.at[j]).start()
        push(rows(j), block(tp), left, out_sem.at[0], near_in.at[j]).start()

    def pass_near(j):
        push(half(j, 0), block(left), right, out_sem.at[1], far_in.at[j]).start()
        push(half(j, 1), block(right), left, out_sem.at[1], far_in.at[j]).start()
        push(rows(j), block(left), mate, out_sem.at[2], mate_near.at[j]).start()
        push(rows(j), block(right), mate, out_sem.at[2], mate_near.at[j]).start()

    def pass_far(j):
        push(rows(j), block(far), mate, out_sem.at[3], mate_far.at[j]).start()

    whole = pl.ds(0, n_chunk * B)

    def pair_own(owner):
        return push(whole, block(owner), mate, own_sem.at[0], own_sem.at[1])

    loads[0].wait()
    pl.semaphore_wait(barrier, n_sp + 2)

    pair_own(tp).start()
    for j in range(LEAD):
        send_own(j)

    kinds = (2, 3, 1)

    def own_part(c, carry):
        r = rows(c)
        xc = x[r, chip(tp)]
        for n, i in enumerate(kinds):
            part[n, r, :] = nn(xc, w[i, chip(tp), :])
        return carry

    def near_part(c):
        r = rows(c)
        xl, xr = x[r, chip(left)], x[r, chip(right)]
        for n, i in enumerate(kinds):
            part[n, r, :] += nn(xl, w[i, chip(left), :]) + nn(xr, w[i, chip(right), :])

    for load in loads[1:6]:
        load.wait()
    pair_own(mate).wait_recv()
    lax.fori_loop(0, n_chunk, own_part, 0)

    s_f[...] = jnp.zeros_like(s_f)
    s_b[...] = jnp.zeros_like(s_b)
    acc[...] = jnp.zeros_like(acc)

    def compute(c):
        r = rows(c)
        xc = x[r, chip(far)]
        kf = room[0:1, :] / (1.0 + jnp.exp(part[0, r, :] + nn(xc, w[2, chip(far), :])))
        kb = room[1:2, :] / (1.0 + jnp.exp(part[1, r, :] + nn(xc, w[3, chip(far), :])))
        kf_s[r, :] = kf
        kb_s[r, :] = kb
        vc = (part[2, r, :] + nn(xc, w[1, chip(far), :])).astype(BF16)
        vs[r, :] = vc
        tri_l = jnp.where(lower, 1.0, 0.0).astype(BF16)
        tri_u = jnp.where(upper, 1.0, 0.0).astype(BF16)
        lf_hi, lf_lo = split2(log_one_minus(kf))
        lb_hi, lb_lo = split2(log_one_minus(kb))
        wfc = nn(tri_l, lf_hi) + nn(tri_l, lf_lo)
        wbc = nn(tri_u, lb_hi) + nn(tri_u, lb_lo)
        ones = jnp.ones((B, HD), BF16)
        for h in range(heads):
            hs = slice(h * HD, (h + 1) * HD)
            ex = extra[h:h + 1, r]
            el_hi, el_lo = split2(jnp.where(lower, ex, 0.0))
            eu_hi, eu_lo = split2(jnp.where(upper, ex, 0.0))
            wfh = wfc[:, hs] + nn(el_hi, ones) + nn(el_lo, ones)
            wbh = wbc[:, hs] + nn(eu_hi, ones) + nn(eu_lo, ones)
            cf[r, hs] = wfh
            cb[r, hs] = wbh
            end_f = wfh[B - 1:B, :]
            end_b = wbh[0:1, :]
            ke_hi, ke_lo = split2(kf[:, hs] * jnp.exp(end_f - wfh))
            ke_b = (kb[:, hs] * jnp.exp(end_b - wbh)).astype(BF16)
            af = tn(vc[:, hs], ke_hi) + tn(vc[:, hs], ke_lo)
            ab = tn(vc[:, hs], ke_b)
            a_f[c, h] = af
            a_b[c, h] = ab
            e_f[c, h] = jnp.broadcast_to(jnp.exp(end_f), (8, HD))
            e_b[c, h] = jnp.broadcast_to(jnp.exp(end_b), (8, HD))
            s_f[h] = s_f[h] * jnp.exp(end_f) + af
            s_b[h] = s_b[h] + jnp.exp(acc[1, h, 0:1, :]) * ab
            acc[0, h] = acc[0, h] + end_f
            acc[1, h] = acc[1, h] + end_b

    def step(j, carry):
        @pl.when(j < n_chunk)
        def _():
            push(rows(j), chip(left), left, out_sem.at[0], near_in.at[j]).wait_recv()
            pass_near(j)

        @pl.when(j + LEAD < n_chunk)
        def _():
            send_own(j + LEAD)

        @pl.when((j >= 1) & (j <= n_chunk))
        def _():
            c = j - 1
            push(rows(c), chip(left), mate, out_sem.at[2], mate_near.at[c]).wait_recv()
            near_part(c)

        @pl.when((j >= LAG) & (j < n_chunk + LAG))
        def _():
            c = j - LAG
            push(rows(c), block(far), left, out_sem.at[1], far_in.at[c]).wait_recv()
            pass_far(c)

        @pl.when(j >= LAG + 1)
        def _():
            c = j - LAG - 1
            push(rows(c), block(far), mate, out_sem.at[3], mate_far.at[c]).wait_recv()
            compute(c)

        return carry

    lax.fori_loop(0, n_chunk + LAG + 1, step, 0)

    per = n_sp // heads
    nz = n_sp // NX
    r_id = lax.broadcasted_iota(jnp.int32, (2, HD), 0)
    for h in range(heads):
        at = slice(h * per, (h + 1) * per)
        stage_f[at] = s_f[h].reshape(per, 8, HD)
        stage_b[at] = s_b[h].reshape(per, 8, HD).astype(BF16)
        both = jnp.where(r_id == 0, acc[0, h, 0:2], acc[1, h, 0:2])
        stage_d[at] = jnp.broadcast_to(both[None], (per, 2, HD))
    got_f[sp] = stage_f[sp]
    got_b[sp] = stage_b[sp]
    got_d[sp] = stage_d[sp]

    my_z, my_x = sp // NX, lax.rem(sp, NX)

    def outward(n):
        return [n // 2 + ((i + 1) // 2) * (1 - 2 * (i % 2)) for i in range(n)]

    z_at = {d: lax.rem(my_z + d, nz) * NX for d in range(nz)}
    x_at = {d: lax.rem(my_x + d, NX) for d in range(NX)}
    others = [z_at[dz] + x_at[dx] for dz in outward(nz) for dx in outward(NX) if dz or dx]

    def exchange(stages, gots, sends, recvs, whole=False):
        def copies(to, frm):
            return [pltpu.make_async_remote_copy(
                src_ref=st.at[sp] if whole else st.at[to], dst_ref=gt.at[frm], send_sem=sends.at[n],
                recv_sem=recvs.at[n], device_id={"sp": to}, device_id_type=MESH)
                for n, (st, gt) in enumerate(zip(stages, gots))]

        def spread():
            for to in others:
                for copy in copies(to, sp):
                    copy.start()

        every = [pltpu.make_async_remote_copy(
            src_ref=st.at[pl.ds(0, n_sp - 1)], dst_ref=gt.at[pl.ds(0, n_sp - 1)], send_sem=sends.at[n],
            recv_sem=recvs.at[n], device_id={"sp": others[0]}, device_id_type=MESH)
            for n, (st, gt) in enumerate(zip(stages, gots))]

        def collect():
            for copy in every:
                copy.wait_recv()

        def drain():
            for copy in every:
                copy.wait_send()

        return spread, collect, drain

    spread1, collect1, drain1 = exchange((stage_d, stage_f, stage_b), (got_d, got_f, got_b), p1_send, p1_recv)
    spread2, collect2, drain2 = exchange((stage2,), (got2,), p2_send, p2_recv)
    spread3, collect3, drain3 = exchange((fin,), (fin,), p3_send, p3_recv, whole=True)

    spread1()

    def queries(c, carry):
        r = rows(c)
        xc = x[r, :]
        qs[r, :] = nn(xc, w[0]).astype(BF16)
        gs[r, :] = silu_gain(nn(xc, w[4]))
        return carry

    def scores(c, carry):
        r = rows(c)
        for h in range(heads):
            hs = slice(h * HD, (h + 1) * HD)
            wfh = cf[r, hs]
            wbh = cb[r, hs]
            mid_f = wfh[B // 2:B // 2 + 1, :]
            mid_b = wbh[B // 2 - 1:B // 2, :]
            q = qs[r, hs].astype(F32)
            qi_f = (q * jnp.exp(wfh - mid_f)).astype(BF16)
            qi_b = (q * jnp.exp(wbh - mid_b)).astype(BF16)
            ki_f = (kf_s[r, hs] * jnp.exp(mid_f - wfh)).astype(BF16)
            ki_b = (kb_s[r, hs] * jnp.exp(mid_b - wbh)).astype(BF16)
            sc = jnp.where(lower, nt(qi_f, ki_f), 0.0) + jnp.where(upper, nt(qi_b, ki_b), 0.0)
            inside[r, hs] = nn(sc.astype(BF16), vs[r, hs])
            qc[h, c, 0:B, 0:HD], qc[h, c, B:2 * B, 0:HD] = split2(q * jnp.exp(wfh))
            qc[h, c, 0:B, HD:2 * HD], qc[h, c, B:2 * B, HD:2 * HD] = split2(q * jnp.exp(wbh))
        return carry

    def inner(c, carry):
        queries(c, 0)
        return scores(c, 0)

    for load in loads[6:]:
        load.wait()
    early = n_chunk // 2
    lax.fori_loop(0, early, inner, 0)
    new = nx[...]
    nqf = nn(new, w[0]).astype(BF16).astype(F32)
    nv[...] = nn(new, w[1]).astype(BF16)
    nf = room[0:1, :] / (1.0 + jnp.exp(nn(new, w[2])))
    nb = room[1:2, :] / (1.0 + jnp.exp(nn(new, w[3])))
    ngate[...] = silu_gain(nn(new, w[4]))
    nq_hi[...], nq_lo[...] = split2(nqf * (1.0 - nf))
    nown[...] = nqf * (nf + nb)

    collect1()

    def decay(q, at):
        return jnp.exp(got_d[q, at:at + 1, :])

    run = jnp.zeros((8, HD), F32)
    before = []
    for q in range(n_sp):
        before.append(run)
        run = run * decay(q, 0) + got_f[q]
    fin[sp] = run.astype(BF16)
    run = jnp.zeros((8, HD), F32)
    for q in reversed(range(n_sp)):
        stage2[q, 0] = before[q]
        stage2[q, 1] = run
        run = run * decay(q, 1) + got_b[q].astype(F32)
    got2[sp] = stage2[sp]
    spread2()
    lax.fori_loop(early, n_chunk, inner, 0)
    spread3()

    push(whole, chip(tp), left, out_sem.at[0], near_in.at[0]).wait_send()
    push(whole, block(tp), left, out_sem.at[1], near_in.at[0]).wait_send()
    push(whole, chip(tp), left, out_sem.at[2], near_in.at[0]).wait_send()
    push(whole, block(tp), left, out_sem.at[3], near_in.at[0]).wait_send()
    pair_own(tp).wait_send()
    drain1()
    collect2()

    for h in range(heads):
        run = got2[h * per:(h + 1) * per, 0].reshape(HD, HD)
        for c in range(n_chunk):
            st[h, c, 0:HD, 0:HD], st[h, c, HD:2 * HD, 0:HD] = split2(run)
            run = run * e_f[c, h, 0:1, :] + a_f[c, h]
        run = got2[h * per:(h + 1) * per, 1].reshape(HD, HD)
        for c in reversed(range(n_chunk)):
            st[h, c, 0:HD, HD:2 * HD], st[h, c, HD:2 * HD, HD:2 * HD] = split2(run)
            run = run * e_b[c, h, 0:1, :] + a_b[c, h]

    def norm(mix, scale):
        return (mix * lax.rsqrt(jnp.mean(mix * mix, axis=-1, keepdims=True) + EPS) * scale).astype(BF16)

    def finish(c, carry):
        r = rows(c)
        for h in range(heads):
            hs = slice(h * HD, (h + 1) * HD)
            carried = nt(qc[h, c], st[h, c])
            carried = carried[0:B] + carried[B:2 * B]
            mix = inside[r, hs] + (carried[:, HD:2 * HD] + carried[:, 0:HD])
            mixed_out[r, hs] = norm(mix, gs[r, hs])
        return carry

    lax.fori_loop(0, n_chunk, finish, 0, unroll=8)

    collect3()
    for h in range(heads):
        hs = slice(h * HD, (h + 1) * HD)
        last = fin[h * per:(h + 1) * per].astype(F32).reshape(HD, HD)
        cached = last.astype(BF16)
        cache_out[h] = last.T.astype(BF16)
        own = jnp.sum(nown[:, hs], axis=-1, keepdims=True) * nv[:, hs].astype(F32)
        read_out[:, hs] = norm(nt(nq_lo[:, hs], cached) + nt(nq_hi[:, hs], cached) + own, ngate[:, hs])

    drain2()
    drain3()


def solution(mesh):
    n_sp, n_tp = mesh.shape["sp"], mesh.shape["tp"]

    def per_device(inputs, w_query, w_value, w_forget, w_gate, gate_room, extra_decay, out_gain, new_inputs):
        tokens, cols = inputs.shape
        depth = w_query.shape[0]
        heads = extra_decay.shape[0]
        fresh = new_inputs.shape[0]
        chunks = tokens // B
        hbm = pl.BlockSpec(memory_space=pltpu.HBM)
        vmem = pl.BlockSpec(memory_space=pltpu.VMEM)

        def kernel(*refs):
            body(n_sp, n_tp, chunks, heads, *refs)

        dma = pltpu.SemaphoreType.DMA
        done = pl.pallas_call(
            kernel,
            out_shape=(jax.ShapeDtypeStruct((tokens, cols), BF16),
                       jax.ShapeDtypeStruct((heads, HD, HD), BF16),
                       jax.ShapeDtypeStruct((fresh, cols), BF16)),
            in_specs=[hbm] * 9,
            out_specs=(vmem, vmem, vmem),
            scratch_shapes=[
                pltpu.VMEM((tokens, depth), BF16),
                pltpu.VMEM((5, depth, cols), BF16),
                pltpu.VMEM((fresh, depth), BF16),
                pltpu.VMEM((3, tokens, cols), F32),
                pltpu.VMEM((2, cols), F32),
                pltpu.VMEM((heads, tokens), F32),
                pltpu.VMEM((1, cols), F32),
                pltpu.VMEM((tokens, cols), BF16),
                pltpu.VMEM((tokens, cols), BF16),
                pltpu.VMEM((tokens, cols), F32),
                pltpu.VMEM((tokens, cols), F32),
                pltpu.VMEM((tokens, cols), F32),
                pltpu.VMEM((tokens, cols), F32),
                pltpu.VMEM((tokens, cols), F32),
                pltpu.VMEM((chunks, heads, HD, HD), F32),
                pltpu.VMEM((chunks, heads, HD, HD), F32),
                pltpu.VMEM((chunks, heads, 8, HD), F32),
                pltpu.VMEM((chunks, heads, 8, HD), F32),
                pltpu.VMEM((heads, HD, HD), F32),
                pltpu.VMEM((heads, HD, HD), F32),
                pltpu.VMEM((2, heads, 8, HD), F32),
                pltpu.VMEM((tokens, cols), F32),
                pltpu.VMEM((heads, chunks, 2 * B, 2 * HD), BF16),
                pltpu.VMEM((heads, chunks, 2 * HD, 2 * HD), BF16),
                pltpu.VMEM((n_sp, 8, HD), F32),
                pltpu.VMEM((n_sp, 8, HD), BF16),
                pltpu.VMEM((n_sp, 2, HD), F32),
                pltpu.VMEM((n_sp, 8, HD), F32),
                pltpu.VMEM((n_sp, 8, HD), BF16),
                pltpu.VMEM((n_sp, 2, HD), F32),
                pltpu.VMEM((n_sp, 2, 8, HD), F32),
                pltpu.VMEM((n_sp, 2, 8, HD), F32),
                pltpu.VMEM((n_sp, 8, HD), BF16),
                pltpu.VMEM((fresh, cols), BF16),
                pltpu.VMEM((fresh, cols), BF16),
                pltpu.VMEM((fresh, cols), BF16),
                pltpu.VMEM((fresh, cols), F32),
                pltpu.VMEM((fresh, cols), F32),
                dma((10,)), dma((2,)),
                dma((4,)), dma((chunks,)), dma((chunks,)), dma((chunks,)), dma((chunks,)),
                dma((3,)), dma((3,)), dma((1,)), dma((1,)), dma((1,)), dma((1,)),
            ],
            compiler_params=pltpu.CompilerParams(collective_id=0, has_side_effects=True,
                                                 vmem_limit_bytes=VM1 * 1024 * 1024),
        )(*(pltpu.with_memory_space_constraint(a, pltpu.HBM) for a in (
            inputs, w_query, w_value, w_forget, w_gate, new_inputs, gate_room, extra_decay, out_gain.reshape(1, cols))))

        def put(a, b, c, a_out, b_out, c_out, sems):
            copies = [pltpu.make_async_copy(s, d, sems.at[i])
                      for i, (s, d) in enumerate(((a, a_out), (b, b_out), (c, c_out)))]
            for copy in copies:
                copy.start()
            for copy in copies:
                copy.wait()

        return pl.pallas_call(
            put,
            out_shape=tuple(jax.ShapeDtypeStruct(d.shape, d.dtype) for d in done),
            in_specs=[vmem] * 3,
            out_specs=(hbm,) * 3,
            scratch_shapes=[dma((3,))],
            compiler_params=pltpu.CompilerParams(vmem_limit_bytes=4 * 1024 * 1024),
        )(*done)

    return jax.shard_map(
        per_device,
        mesh=mesh,
        in_specs=(P("sp", "tp"), P(None, "tp"), P(None, "tp"), P(None, None, "tp"), P(None, "tp"),
                  P(None, "tp"), P("tp", "sp"), P("tp"), P()),
        out_specs=(P("sp", "tp"), P("tp", None, None), P(None, "tp")),
        check_vma=False,
    )
```

```python
import jax
import jax.numpy as jnp
from jax import lax
from jax.experimental import pallas as pl
from jax.experimental.pallas import tpu as pltpu
from jax.sharding import PartitionSpec as P

MESH = pl.DeviceIdType.MESH
EPS = 1e-06
B = 128
HD = 128
VM1 = 48
LEAD = 3
LAG = 2
NX = 4
F32 = jnp.float32
BF16 = jnp.bfloat16


def nn(a, b):
    return lax.dot_general(a, b, (((1,), (0,)), ((), ())), preferred_element_type=F32)


def nt(a, b):
    return lax.dot_general(a, b, (((1,), (1,)), ((), ())), preferred_element_type=F32)


def tn(a, b):
    return lax.dot_general(a, b, (((0,), (0,)), ((), ())), preferred_element_type=F32)


def split2(a):
    hi = a.astype(BF16)
    return hi, (a - hi.astype(F32)).astype(BF16)


def log_one_minus(k):
    s = jnp.full_like(k, 1.0 / 8.0)
    for n in (7, 6, 5, 4, 3, 2):
        s = s * k + (1.0 / n)
    return -(s * k + 1.0) * k


def body(n_sp, n_tp, n_chunk, heads, x_hbm, wq, wv, wf, wg, nx_hbm, room_hbm, extra_hbm, gain_hbm,
         mixed_out, cache_out, read_out,
         x, w, nx, part, room, extra, gain, qs, vs, cf, cb, kf_s, kb_s, gs, a_f, a_b, e_f, e_b, s_f, s_b, acc,
         inside, qc, st, stage_f, stage_b, stage_d, got_f, got_b, got_d, stage2, got2, fin, nq_hi, nq_lo, nv, nown, ngate,
         load_sem, own_sem, out_sem, near_in, far_in, mate_near, mate_far, word, p1_send, p1_recv, p2_send, p2_recv,
         p3_send, p3_recv):
    cols = heads * HD
    sp = lax.axis_index("sp")
    tp = lax.axis_index("tp")
    right = lax.rem(tp + 2, n_tp)
    left = lax.rem(tp + n_tp - 2, n_tp)
    far = lax.rem(tp + 4, n_tp)
    flip = 1 - 2 * lax.rem(tp, 2)
    mate = tp + flip

    nz = n_sp // NX
    my_z, my_x = sp // NX, lax.rem(sp, NX)

    barrier = pltpu.get_barrier_semaphore()
    z_sides = [lax.rem(my_z + d, nz) * NX + my_x for d in (1, nz - 1)]
    x_sides = [my_z * NX + lax.rem(my_x + d, NX) for d in (1, NX - 1)]
    for peer in (mate, left, right):
        pl.semaphore_signal(barrier, inc=1, device_id={"tp": peer}, device_id_type=MESH)
    for peer in z_sides + x_sides:
        pl.semaphore_signal(barrier, inc=1, device_id={"sp": peer}, device_id_type=MESH)
    rounds = 1 + nz // 2

    def tell(n, sides):
        for peer in sides:
            pl.semaphore_signal(word.at[n], inc=1, device_id={"sp": peer}, device_id_type=MESH)

    def block(owner):
        return pl.ds(pl.multiple_of(owner * cols, cols), cols)

    def rows(j):
        return pl.ds(pl.multiple_of(j * B, B), B)

    loads = [pltpu.make_async_copy(src, dst, load_sem.at[i]) for i, (src, dst) in enumerate((
        (x_hbm, x.at[:, block(tp)]), (room_hbm, room), (extra_hbm, extra), (wf.at[0], w.at[2]), (wf.at[1], w.at[3]),
        (wv, w.at[1]), (gain_hbm, gain), (wq, w.at[0]), (wg, w.at[4]), (nx_hbm, nx)))]
    for load in loads:
        load.start()

    t_id = lax.broadcasted_iota(jnp.int32, (B, B), 0)
    s_id = lax.broadcasted_iota(jnp.int32, (B, B), 1)
    lower = t_id >= s_id
    upper = s_id >= t_id

    def silu_gain(g):
        return gain[...] * (g / (1.0 + jnp.exp(-g)))

    def half(j, k):
        return pl.ds(pl.multiple_of(j * B + k * (B // 2), B // 2), B // 2)

    def chip(owner):
        return pl.ds(pl.multiple_of((owner // 2) * (2 * cols), 2 * cols), 2 * cols)

    def push(r, c, to, out, inn):
        return pltpu.make_async_remote_copy(
            src_ref=x.at[r, c], dst_ref=x.at[r, c], send_sem=out, recv_sem=inn,
            device_id={"tp": to}, device_id_type=MESH)

    def send_own(j):
        push(rows(j), block(tp), right, out_sem.at[0], near_in.at[j]).start()
        push(rows(j), block(tp), left, out_sem.at[0], near_in.at[j]).start()

    def pass_near(j):
        push(half(j, 0), block(left), right, out_sem.at[1], far_in.at[j]).start()
        push(half(j, 1), block(right), left, out_sem.at[1], far_in.at[j]).start()
        push(rows(j), block(left), mate, out_sem.at[2], mate_near.at[j]).start()
        push(rows(j), block(right), mate, out_sem.at[2], mate_near.at[j]).start()

    def pass_far(j):
        push(rows(j), block(far), mate, out_sem.at[3], mate_far.at[j]).start()

    whole = pl.ds(0, n_chunk * B)

    def pair_own(owner):
        return push(whole, block(owner), mate, own_sem.at[0], own_sem.at[1])

    loads[0].wait()
    pl.semaphore_wait(barrier, 7)

    pair_own(tp).start()
    tell(0, x_sides)
    for j in range(LEAD):
        send_own(j)

    kinds = (2, 3, 1)

    def own_part(c, carry):
        r = rows(c)
        xc = x[r, chip(tp)]
        for n, i in enumerate(kinds):
            part[n, r, :] = nn(xc, w[i, chip(tp), :])
        return carry

    def near_part(c):
        r = rows(c)
        xl, xr = x[r, chip(left)], x[r, chip(right)]
        for n, i in enumerate(kinds):
            part[n, r, :] += nn(xl, w[i, chip(left), :]) + nn(xr, w[i, chip(right), :])

    for load in loads[1:6]:
        load.wait()
    pair_own(mate).wait_recv()
    lax.fori_loop(0, n_chunk, own_part, 0)

    s_f[...] = jnp.zeros_like(s_f)
    s_b[...] = jnp.zeros_like(s_b)
    acc[...] = jnp.zeros_like(acc)

    def compute(c):
        r = rows(c)
        xc = x[r, chip(far)]
        kf = room[0:1, :] / (1.0 + jnp.exp(part[0, r, :] + nn(xc, w[2, chip(far), :])))
        kb = room[1:2, :] / (1.0 + jnp.exp(part[1, r, :] + nn(xc, w[3, chip(far), :])))
        kf_s[r, :] = kf
        kb_s[r, :] = kb
        vc = (part[2, r, :] + nn(xc, w[1, chip(far), :])).astype(BF16)
        vs[r, :] = vc
        tri_l = jnp.where(lower, 1.0, 0.0).astype(BF16)
        tri_u = jnp.where(upper, 1.0, 0.0).astype(BF16)
        lf_hi, lf_lo = split2(log_one_minus(kf))
        lb_hi, lb_lo = split2(log_one_minus(kb))
        wfc = nn(tri_l, lf_hi) + nn(tri_l, lf_lo)
        wbc = nn(tri_u, lb_hi) + nn(tri_u, lb_lo)
        ones = jnp.ones((B, HD), BF16)
        for h in range(heads):
            hs = slice(h * HD, (h + 1) * HD)
            ex = extra[h:h + 1, r]
            el_hi, el_lo = split2(jnp.where(lower, ex, 0.0))
            eu_hi, eu_lo = split2(jnp.where(upper, ex, 0.0))
            wfh = wfc[:, hs] + nn(el_hi, ones) + nn(el_lo, ones)
            wbh = wbc[:, hs] + nn(eu_hi, ones) + nn(eu_lo, ones)
            cf[r, hs] = wfh
            cb[r, hs] = wbh
            end_f = wfh[B - 1:B, :]
            end_b = wbh[0:1, :]
            ke_hi, ke_lo = split2(kf[:, hs] * jnp.exp(end_f - wfh))
            ke_b = (kb[:, hs] * jnp.exp(end_b - wbh)).astype(BF16)
            af = tn(vc[:, hs], ke_hi) + tn(vc[:, hs], ke_lo)
            ab = tn(vc[:, hs], ke_b)
            a_f[c, h] = af
            a_b[c, h] = ab
            e_f[c, h] = jnp.broadcast_to(jnp.exp(end_f), (8, HD))
            e_b[c, h] = jnp.broadcast_to(jnp.exp(end_b), (8, HD))
            s_f[h] = s_f[h] * jnp.exp(end_f) + af
            s_b[h] = s_b[h] + jnp.exp(acc[1, h, 0:1, :]) * ab
            acc[0, h] = acc[0, h] + end_f
            acc[1, h] = acc[1, h] + end_b

    def step(j, carry):
        @pl.when(j < n_chunk)
        def _():
            push(rows(j), chip(left), left, out_sem.at[0], near_in.at[j]).wait_recv()
            pass_near(j)

        @pl.when(j + LEAD < n_chunk)
        def _():
            send_own(j + LEAD)

        @pl.when((j >= 1) & (j <= rounds))
        def _():
            pl.semaphore_wait(word.at[j - 1], 2)

        @pl.when((j >= 1) & (j < rounds))
        def _():
            tell(j, z_sides)

        @pl.when((j >= 1) & (j <= n_chunk))
        def _():
            c = j - 1
            push(rows(c), chip(left), mate, out_sem.at[2], mate_near.at[c]).wait_recv()
            near_part(c)

        @pl.when((j >= LAG) & (j < n_chunk + LAG))
        def _():
            c = j - LAG
            push(rows(c), block(far), left, out_sem.at[1], far_in.at[c]).wait_recv()
            pass_far(c)

        @pl.when(j >= LAG + 1)
        def _():
            c = j - LAG - 1
            push(rows(c), block(far), mate, out_sem.at[3], mate_far.at[c]).wait_recv()
            compute(c)

        return carry

    lax.fori_loop(0, n_chunk + LAG + 1, step, 0)

    per = n_sp // heads
    r_id = lax.broadcasted_iota(jnp.int32, (2, HD), 0)
    for h in range(heads):
        at = slice(h * per, (h + 1) * per)
        stage_f[at] = s_f[h].reshape(per, 8, HD)
        stage_b[at] = s_b[h].reshape(per, 8, HD).astype(BF16)
        both = jnp.where(r_id == 0, acc[0, h, 0:2], acc[1, h, 0:2])
        stage_d[at] = jnp.broadcast_to(both[None], (per, 2, HD))
    got_f[sp] = stage_f[sp]
    got_b[sp] = stage_b[sp]
    got_d[sp] = stage_d[sp]

    def outward(n):
        return [n // 2 + ((i + 1) // 2) * (1 - 2 * (i % 2)) for i in range(n)]

    z_at = {d: lax.rem(my_z + d, nz) * NX for d in range(nz)}
    x_at = {d: lax.rem(my_x + d, NX) for d in range(NX)}
    others = [z_at[dz] + x_at[dx] for dz in outward(nz) for dx in outward(NX) if dz or dx]

    def exchange(stages, gots, sends, recvs, whole=False):
        def copies(to, frm):
            return [pltpu.make_async_remote_copy(
                src_ref=st.at[sp] if whole else st.at[to], dst_ref=gt.at[frm], send_sem=sends.at[n],
                recv_sem=recvs.at[n], device_id={"sp": to}, device_id_type=MESH)
                for n, (st, gt) in enumerate(zip(stages, gots))]

        def spread():
            for to in others:
                for copy in copies(to, sp):
                    copy.start()

        every = [pltpu.make_async_remote_copy(
            src_ref=st.at[pl.ds(0, n_sp - 1)], dst_ref=gt.at[pl.ds(0, n_sp - 1)], send_sem=sends.at[n],
            recv_sem=recvs.at[n], device_id={"sp": others[0]}, device_id_type=MESH)
            for n, (st, gt) in enumerate(zip(stages, gots))]

        def collect():
            for copy in every:
                copy.wait_recv()

        def drain():
            for copy in every:
                copy.wait_send()

        return spread, collect, drain

    spread1, collect1, drain1 = exchange((stage_d, stage_f, stage_b), (got_d, got_f, got_b), p1_send, p1_recv)
    spread2, collect2, drain2 = exchange((stage2,), (got2,), p2_send, p2_recv)
    spread3, collect3, drain3 = exchange((fin,), (fin,), p3_send, p3_recv, whole=True)

    spread1()

    def queries(c, carry):
        r = rows(c)
        xc = x[r, :]
        qs[r, :] = nn(xc, w[0]).astype(BF16)
        gs[r, :] = silu_gain(nn(xc, w[4]))
        return carry

    def scores(c, carry):
        r = rows(c)
        for h in range(heads):
            hs = slice(h * HD, (h + 1) * HD)
            wfh = cf[r, hs]
            wbh = cb[r, hs]
            mid_f = wfh[B // 2:B // 2 + 1, :]
            mid_b = wbh[B // 2 - 1:B // 2, :]
            q = qs[r, hs].astype(F32)
            qi_f = (q * jnp.exp(wfh - mid_f)).astype(BF16)
            qi_b = (q * jnp.exp(wbh - mid_b)).astype(BF16)
            ki_f = (kf_s[r, hs] * jnp.exp(mid_f - wfh)).astype(BF16)
            ki_b = (kb_s[r, hs] * jnp.exp(mid_b - wbh)).astype(BF16)
            sc = jnp.where(lower, nt(qi_f, ki_f), 0.0) + jnp.where(upper, nt(qi_b, ki_b), 0.0)
            inside[r, hs] = nn(sc.astype(BF16), vs[r, hs])
            qc[h, c, 0:B, 0:HD], qc[h, c, B:2 * B, 0:HD] = split2(q * jnp.exp(wfh))
            qc[h, c, 0:B, HD:2 * HD], qc[h, c, B:2 * B, HD:2 * HD] = split2(q * jnp.exp(wbh))
        return carry

    def inner(c, carry):
        queries(c, 0)
        return scores(c, 0)

    for load in loads[6:]:
        load.wait()
    early = n_chunk // 2
    lax.fori_loop(0, early, inner, 0)
    new = nx[...]
    nqf = nn(new, w[0]).astype(BF16).astype(F32)
    nv[...] = nn(new, w[1]).astype(BF16)
    nf = room[0:1, :] / (1.0 + jnp.exp(nn(new, w[2])))
    nb = room[1:2, :] / (1.0 + jnp.exp(nn(new, w[3])))
    ngate[...] = silu_gain(nn(new, w[4]))
    nq_hi[...], nq_lo[...] = split2(nqf * (1.0 - nf))
    nown[...] = nqf * (nf + nb)

    collect1()

    def decay(q, at):
        return jnp.exp(got_d[q, at:at + 1, :])

    run = jnp.zeros((8, HD), F32)
    before = []
    for q in range(n_sp):
        before.append(run)
        run = run * decay(q, 0) + got_f[q]
    fin[sp] = run.astype(BF16)
    run = jnp.zeros((8, HD), F32)
    for q in reversed(range(n_sp)):
        stage2[q, 0] = before[q]
        stage2[q, 1] = run
        run = run * decay(q, 1) + got_b[q].astype(F32)
    got2[sp] = stage2[sp]
    spread2()
    lax.fori_loop(early, n_chunk, inner, 0)
    spread3()

    push(whole, chip(tp), left, out_sem.at[0], near_in.at[0]).wait_send()
    push(whole, block(tp), left, out_sem.at[1], near_in.at[0]).wait_send()
    push(whole, chip(tp), left, out_sem.at[2], near_in.at[0]).wait_send()
    push(whole, block(tp), left, out_sem.at[3], near_in.at[0]).wait_send()
    pair_own(tp).wait_send()
    drain1()
    collect2()

    for h in range(heads):
        run = got2[h * per:(h + 1) * per, 0].reshape(HD, HD)
        for c in range(n_chunk):
            st[h, c, 0:HD, 0:HD], st[h, c, HD:2 * HD, 0:HD] = split2(run)
            run = run * e_f[c, h, 0:1, :] + a_f[c, h]
        run = got2[h * per:(h + 1) * per, 1].reshape(HD, HD)
        for c in reversed(range(n_chunk)):
            st[h, c, 0:HD, HD:2 * HD], st[h, c, HD:2 * HD, HD:2 * HD] = split2(run)
            run = run * e_b[c, h, 0:1, :] + a_b[c, h]

    def norm(mix, scale):
        return (mix * lax.rsqrt(jnp.mean(mix * mix, axis=-1, keepdims=True) + EPS) * scale).astype(BF16)

    def finish(c, carry):
        r = rows(c)
        for h in range(heads):
            hs = slice(h * HD, (h + 1) * HD)
            carried = nt(qc[h, c], st[h, c])
            carried = carried[0:B] + carried[B:2 * B]
            mix = inside[r, hs] + (carried[:, HD:2 * HD] + carried[:, 0:HD])
            mixed_out[r, hs] = norm(mix, gs[r, hs])
        return carry

    lax.fori_loop(0, n_chunk, finish, 0, unroll=8)

    collect3()
    for h in range(heads):
        hs = slice(h * HD, (h + 1) * HD)
        last = fin[h * per:(h + 1) * per].astype(F32).reshape(HD, HD)
        cached = last.astype(BF16)
        cache_out[h] = last.T.astype(BF16)
        own = jnp.sum(nown[:, hs], axis=-1, keepdims=True) * nv[:, hs].astype(F32)
        read_out[:, hs] = norm(nt(nq_lo[:, hs], cached) + nt(nq_hi[:, hs], cached) + own, ngate[:, hs])

    drain2()
    drain3()


def solution(mesh):
    n_sp, n_tp = mesh.shape["sp"], mesh.shape["tp"]

    def per_device(inputs, w_query, w_value, w_forget, w_gate, gate_room, extra_decay, out_gain, new_inputs):
        tokens, cols = inputs.shape
        depth = w_query.shape[0]
        heads = extra_decay.shape[0]
        fresh = new_inputs.shape[0]
        chunks = tokens // B
        hbm = pl.BlockSpec(memory_space=pltpu.HBM)
        vmem = pl.BlockSpec(memory_space=pltpu.VMEM)

        def kernel(*refs):
            body(n_sp, n_tp, chunks, heads, *refs)

        dma = pltpu.SemaphoreType.DMA
        done = pl.pallas_call(
            kernel,
            out_shape=(jax.ShapeDtypeStruct((tokens, cols), BF16),
                       jax.ShapeDtypeStruct((heads, HD, HD), BF16),
                       jax.ShapeDtypeStruct((fresh, cols), BF16)),
            in_specs=[hbm] * 9,
            out_specs=(vmem, vmem, vmem),
            scratch_shapes=[
                pltpu.VMEM((tokens, depth), BF16),
                pltpu.VMEM((5, depth, cols), BF16),
                pltpu.VMEM((fresh, depth), BF16),
                pltpu.VMEM((3, tokens, cols), F32),
                pltpu.VMEM((2, cols), F32),
                pltpu.VMEM((heads, tokens), F32),
                pltpu.VMEM((1, cols), F32),
                pltpu.VMEM((tokens, cols), BF16),
                pltpu.VMEM((tokens, cols), BF16),
                pltpu.VMEM((tokens, cols), F32),
                pltpu.VMEM((tokens, cols), F32),
                pltpu.VMEM((tokens, cols), F32),
                pltpu.VMEM((tokens, cols), F32),
                pltpu.VMEM((tokens, cols), F32),
                pltpu.VMEM((chunks, heads, HD, HD), F32),
                pltpu.VMEM((chunks, heads, HD, HD), F32),
                pltpu.VMEM((chunks, heads, 8, HD), F32),
                pltpu.VMEM((chunks, heads, 8, HD), F32),
                pltpu.VMEM((heads, HD, HD), F32),
                pltpu.VMEM((heads, HD, HD), F32),
                pltpu.VMEM((2, heads, 8, HD), F32),
                pltpu.VMEM((tokens, cols), F32),
                pltpu.VMEM((heads, chunks, 2 * B, 2 * HD), BF16),
                pltpu.VMEM((heads, chunks, 2 * HD, 2 * HD), BF16),
                pltpu.VMEM((n_sp, 8, HD), F32),
                pltpu.VMEM((n_sp, 8, HD), BF16),
                pltpu.VMEM((n_sp, 2, HD), F32),
                pltpu.VMEM((n_sp, 8, HD), F32),
                pltpu.VMEM((n_sp, 8, HD), BF16),
                pltpu.VMEM((n_sp, 2, HD), F32),
                pltpu.VMEM((n_sp, 2, 8, HD), F32),
                pltpu.VMEM((n_sp, 2, 8, HD), F32),
                pltpu.VMEM((n_sp, 8, HD), BF16),
                pltpu.VMEM((fresh, cols), BF16),
                pltpu.VMEM((fresh, cols), BF16),
                pltpu.VMEM((fresh, cols), BF16),
                pltpu.VMEM((fresh, cols), F32),
                pltpu.VMEM((fresh, cols), F32),
                dma((10,)), dma((2,)),
                dma((4,)), dma((chunks,)), dma((chunks,)), dma((chunks,)), dma((chunks,)),
                pltpu.SemaphoreType.REGULAR((1 + n_sp // NX // 2,)),
                dma((3,)), dma((3,)), dma((1,)), dma((1,)), dma((1,)), dma((1,)),
            ],
            compiler_params=pltpu.CompilerParams(collective_id=0, has_side_effects=True,
                                                 vmem_limit_bytes=VM1 * 1024 * 1024),
        )(*(pltpu.with_memory_space_constraint(a, pltpu.HBM) for a in (
            inputs, w_query, w_value, w_forget, w_gate, new_inputs, gate_room, extra_decay, out_gain.reshape(1, cols))))

        def put(a, b, c, a_out, b_out, c_out, sems):
            copies = [pltpu.make_async_copy(s, d, sems.at[i])
                      for i, (s, d) in enumerate(((a, a_out), (b, b_out), (c, c_out)))]
            for copy in copies:
                copy.start()
            for copy in copies:
                copy.wait()

        return pl.pallas_call(
            put,
            out_shape=tuple(jax.ShapeDtypeStruct(d.shape, d.dtype) for d in done),
            in_specs=[vmem] * 3,
            out_specs=(hbm,) * 3,
            scratch_shapes=[dma((3,))],
            compiler_params=pltpu.CompilerParams(vmem_limit_bytes=4 * 1024 * 1024),
        )(*done)

    return jax.shard_map(
        per_device,
        mesh=mesh,
        in_specs=(P("sp", "tp"), P(None, "tp"), P(None, "tp"), P(None, None, "tp"), P(None, "tp"),
                  P(None, "tp"), P("tp", "sp"), P("tp"), P()),
        out_specs=(P("sp", "tp"), P("tp", None, None), P(None, "tp")),
        check_vma=False,
    )
```

```python
import jax
import jax.numpy as jnp
from jax import lax
from jax.experimental import pallas as pl
from jax.experimental.pallas import tpu as pltpu
from jax.sharding import PartitionSpec as P

MESH = pl.DeviceIdType.MESH
EPS = 1e-06
B = 128
HD = 128
VM1 = 48
LEAD = 3
TILE = 32
LAG = 2
NX = 4
F32 = jnp.float32
BF16 = jnp.bfloat16


def nn(a, b):
    return lax.dot_general(a, b, (((1,), (0,)), ((), ())), preferred_element_type=F32)


def nt(a, b):
    return lax.dot_general(a, b, (((1,), (1,)), ((), ())), preferred_element_type=F32)


def tn(a, b):
    return lax.dot_general(a, b, (((0,), (0,)), ((), ())), preferred_element_type=F32)


def split2(a):
    hi = a.astype(BF16)
    return hi, (a - hi.astype(F32)).astype(BF16)


def log_one_minus(k):
    s = jnp.full_like(k, 1.0 / 8.0)
    for n in (7, 6, 5, 4, 3, 2):
        s = s * k + (1.0 / n)
    return -(s * k + 1.0) * k


def body(n_sp, n_tp, n_chunk, heads, x_hbm, wq, wv, wf, wg, nx_hbm, room_hbm, extra_hbm, gain_hbm,
         mixed_out, cache_out, read_out,
         x, w, nx, part, lg, room, extra, gain, qs, vs, cf, cb, kf_s, kb_s, gs, a_f, a_b, e_f, e_b, s_f, s_b, acc,
         inside, qc, st, stage_f, stage_b, stage_d, got_f, got_b, got_d, stage2, got2, fin, nq_hi, nq_lo, nv, nown, ngate,
         load_sem, own_sem, out_sem, near_in, far_in, mate_near, mate_far, word, p1_send, p1_recv, p2_send, p2_recv,
         p3_send, p3_recv):
    cols = heads * HD
    sp = lax.axis_index("sp")
    tp = lax.axis_index("tp")
    right = lax.rem(tp + 2, n_tp)
    left = lax.rem(tp + n_tp - 2, n_tp)
    far = lax.rem(tp + 4, n_tp)
    flip = 1 - 2 * lax.rem(tp, 2)
    mate = tp + flip

    nz = n_sp // NX
    my_z, my_x = sp // NX, lax.rem(sp, NX)

    barrier = pltpu.get_barrier_semaphore()
    z_sides = [lax.rem(my_z + d, nz) * NX + my_x for d in (1, nz - 1)]
    x_sides = [my_z * NX + lax.rem(my_x + d, NX) for d in (1, NX - 1)]
    for peer in (mate, left, right):
        pl.semaphore_signal(barrier, inc=1, device_id={"tp": peer}, device_id_type=MESH)
    for peer in z_sides + x_sides:
        pl.semaphore_signal(barrier, inc=1, device_id={"sp": peer}, device_id_type=MESH)
    rounds = 1 + nz // 2

    def tell(n, sides):
        for peer in sides:
            pl.semaphore_signal(word.at[n], inc=1, device_id={"sp": peer}, device_id_type=MESH)

    def block(owner):
        return pl.ds(pl.multiple_of(owner * cols, cols), cols)

    def rows(j):
        return pl.ds(pl.multiple_of(j * B, B), B)

    loads = [pltpu.make_async_copy(src, dst, load_sem.at[i]) for i, (src, dst) in enumerate((
        (x_hbm, x.at[:, block(tp)]), (room_hbm, room), (extra_hbm, extra), (wf.at[0], w.at[2]), (wf.at[1], w.at[3]),
        (wv, w.at[1]), (gain_hbm, gain), (wq, w.at[0]), (wg, w.at[4]), (nx_hbm, nx)))]
    for load in loads:
        load.start()

    t_id = lax.broadcasted_iota(jnp.int32, (B, B), 0)
    s_id = lax.broadcasted_iota(jnp.int32, (B, B), 1)
    lower = t_id >= s_id
    upper = s_id >= t_id

    def silu_gain(g):
        return gain[...] * (g / (1.0 + jnp.exp(-g)))

    def half(j, k):
        return pl.ds(pl.multiple_of(j * B + k * (B // 2), B // 2), B // 2)

    def chip(owner):
        return pl.ds(pl.multiple_of((owner // 2) * (2 * cols), 2 * cols), 2 * cols)

    def push(r, c, to, out, inn):
        return pltpu.make_async_remote_copy(
            src_ref=x.at[r, c], dst_ref=x.at[r, c], send_sem=out, recv_sem=inn,
            device_id={"tp": to}, device_id_type=MESH)

    def send_own(j):
        push(rows(j), block(tp), right, out_sem.at[0], near_in.at[j]).start()
        push(rows(j), block(tp), left, out_sem.at[0], near_in.at[j]).start()

    def pass_near(j):
        push(half(j, 0), block(left), right, out_sem.at[1], far_in.at[j]).start()
        push(half(j, 1), block(right), left, out_sem.at[1], far_in.at[j]).start()
        push(rows(j), block(left), mate, out_sem.at[2], mate_near.at[j]).start()
        push(rows(j), block(right), mate, out_sem.at[2], mate_near.at[j]).start()

    def pass_far(j):
        push(rows(j), block(far), mate, out_sem.at[3], mate_far.at[j]).start()

    whole = pl.ds(0, n_chunk * B)

    def pair_own(owner):
        return push(whole, block(owner), mate, own_sem.at[0], own_sem.at[1])

    loads[0].wait()
    pl.semaphore_wait(barrier, 7)

    pair_own(tp).start()
    tell(0, x_sides)
    for j in range(LEAD):
        send_own(j)

    kinds = (2, 3, 1)

    def own_part(c, carry):
        r = pl.ds(pl.multiple_of(c * 2 * B, 2 * B), 2 * B)
        xc = x[r, chip(tp)]
        for n, i in enumerate(kinds):
            part[n, r, :] = nn(xc, w[i, chip(tp), :])
        return carry

    def near_part(c):
        r = pl.ds(pl.multiple_of(c * B, B), 2 * B)
        xl, xr = x[r, chip(left)], x[r, chip(right)]
        for n, i in enumerate(kinds):
            part[n, r, :] += nn(xl, w[i, chip(left), :]) + nn(xr, w[i, chip(right), :])

    loads[2].wait()
    for h in range(heads):
        ex = jnp.concatenate([extra[h:h + 1, c * B:(c + 1) * B] for c in range(n_chunk)], axis=0)
        e_hi, e_lo = split2(ex)
        for mask, sums in ((upper, cf), (lower, cb)):
            tri = jnp.where(mask, 1.0, 0.0).astype(BF16)
            down = (nn(e_hi, tri) + nn(e_lo, tri)).T
            for c in range(n_chunk):
                sums[c * B:(c + 1) * B, h * HD:(h + 1) * HD] = jnp.broadcast_to(down[:, c:c + 1], (B, HD))

    for load in (loads[1], *loads[3:6]):
        load.wait()
    pair_own(mate).wait_recv()
    lax.fori_loop(0, n_chunk // 2, own_part, 0)

    s_f[...] = jnp.zeros_like(s_f)
    s_b[...] = jnp.zeros_like(s_b)
    acc[...] = jnp.zeros_like(acc)

    def compute(c):
        r = rows(c)
        xc = x[r, chip(far)]
        far_w = chip(far)
        part[0, r, :] += nn(xc, w[2, far_w, :])
        part[1, r, :] += nn(xc, w[3, far_w, :])
        vc = (part[2, r, :] + nn(xc, w[1, far_w, :])).astype(BF16)
        vs[r, :] = vc
        for t in range(B // TILE):
            rt = pl.ds(pl.multiple_of(c * B + t * TILE, TILE), TILE)
            for d, keys in ((0, kf_s), (1, kb_s)):
                key = room[d:d + 1, :] / (1.0 + jnp.exp(part[d, rt, :]))
                keys[rt, :] = key
                lg[d, t * TILE:(t + 1) * TILE], lg[d, B + t * TILE:B + (t + 1) * TILE] = split2(log_one_minus(key))
        for d, (mask, sums) in enumerate(((lower, cf), (upper, cb))):
            tri = jnp.where(mask, 1.0, 0.0).astype(BF16)
            sums[r, :] += nn(jnp.concatenate([tri, tri], axis=1), lg[d])
        for h in range(heads):
            hs = slice(h * HD, (h + 1) * HD)
            wf_h, wb_h = cf[r, hs], cb[r, hs]
            end_f, end_b = wf_h[B - 1:B, :], wb_h[0:1, :]
            f_hi, f_lo = split2(kf_s[r, hs] * jnp.exp(end_f - wf_h))
            b_hi, b_lo = split2(kb_s[r, hs] * jnp.exp(end_b - wb_h))
            keys = jnp.concatenate([jnp.concatenate([f_hi, b_hi], axis=1), jnp.concatenate([f_lo, b_lo], axis=1)], axis=0)
            vh = vc[:, hs]
            add = tn(jnp.concatenate([vh, vh], axis=0), keys)
            add_f, add_b = add[:, 0:HD], add[:, HD:2 * HD]
            a_f[c, h] = add_f
            a_b[c, h] = add_b
            e_f[c, h] = jnp.broadcast_to(jnp.exp(end_f), (8, HD))
            e_b[c, h] = jnp.broadcast_to(jnp.exp(end_b), (8, HD))
            s_f[h] = s_f[h] * jnp.exp(end_f) + add_f
            s_b[h] = s_b[h] + jnp.exp(acc[1, h, 0:1, :]) * add_b
            acc[0, h] = acc[0, h] + end_f
            acc[1, h] = acc[1, h] + end_b

    def step(j, carry):
        @pl.when(j < n_chunk)
        def _():
            push(rows(j), chip(left), left, out_sem.at[0], near_in.at[j]).wait_recv()
            pass_near(j)

        @pl.when(j + LEAD < n_chunk)
        def _():
            send_own(j + LEAD)

        @pl.when((j >= 1) & (j <= rounds))
        def _():
            pl.semaphore_wait(word.at[j - 1], 2)

        @pl.when((j >= 1) & (j < rounds))
        def _():
            tell(j, z_sides)

        @pl.when((j >= 1) & (j <= n_chunk))
        def _():
            c = j - 1
            push(rows(c), chip(left), mate, out_sem.at[2], mate_near.at[c]).wait_recv()

        @pl.when((j >= 2) & (j <= n_chunk) & (lax.rem(j, 2) == 0))
        def _():
            near_part(j - 2)

        @pl.when((j >= LAG) & (j < n_chunk + LAG))
        def _():
            c = j - LAG
            push(rows(c), block(far), left, out_sem.at[1], far_in.at[c]).wait_recv()
            pass_far(c)

        @pl.when(j >= LAG + 1)
        def _():
            c = j - LAG - 1
            push(rows(c), block(far), mate, out_sem.at[3], mate_far.at[c]).wait_recv()
            compute(c)

        return carry

    lax.fori_loop(0, n_chunk + LAG + 1, step, 0)

    per = n_sp // heads
    r_id = lax.broadcasted_iota(jnp.int32, (2, HD), 0)
    for h in range(heads):
        at = slice(h * per, (h + 1) * per)
        stage_f[at] = s_f[h].reshape(per, 8, HD)
        stage_b[at] = s_b[h].reshape(per, 8, HD).astype(BF16)
        both = jnp.where(r_id == 0, acc[0, h, 0:2], acc[1, h, 0:2])
        stage_d[at] = jnp.broadcast_to(both[None], (per, 2, HD))
    got_f[sp] = stage_f[sp]
    got_b[sp] = stage_b[sp]
    got_d[sp] = stage_d[sp]

    def outward(n):
        return [n // 2 + ((i + 1) // 2) * (1 - 2 * (i % 2)) for i in range(n)]

    z_at = {d: lax.rem(my_z + d, nz) * NX for d in range(nz)}
    x_at = {d: lax.rem(my_x + d, NX) for d in range(NX)}
    others = [z_at[dz] + x_at[dx] for dz in outward(nz) for dx in outward(NX) if dz or dx]

    def exchange(stages, gots, sends, recvs, whole=False):
        def copies(to, frm):
            return [pltpu.make_async_remote_copy(
                src_ref=st.at[sp] if whole else st.at[to], dst_ref=gt.at[frm], send_sem=sends.at[n],
                recv_sem=recvs.at[n], device_id={"sp": to}, device_id_type=MESH)
                for n, (st, gt) in enumerate(zip(stages, gots))]

        def spread():
            for to in others:
                for copy in copies(to, sp):
                    copy.start()

        every = [pltpu.make_async_remote_copy(
            src_ref=st.at[pl.ds(0, n_sp - 1)], dst_ref=gt.at[pl.ds(0, n_sp - 1)], send_sem=sends.at[n],
            recv_sem=recvs.at[n], device_id={"sp": others[0]}, device_id_type=MESH)
            for n, (st, gt) in enumerate(zip(stages, gots))]

        def collect():
            for copy in every:
                copy.wait_recv()

        def drain():
            for copy in every:
                copy.wait_send()

        return spread, collect, drain

    spread1, collect1, drain1 = exchange((stage_d, stage_f, stage_b), (got_d, got_f, got_b), p1_send, p1_recv)
    spread2, collect2, drain2 = exchange((stage2,), (got2,), p2_send, p2_recv)
    spread3, collect3, drain3 = exchange((fin,), (fin,), p3_send, p3_recv, whole=True)

    spread1()

    def queries(c, carry):
        r = rows(c)
        xc = x[r, :]
        qs[r, :] = nn(xc, w[0]).astype(BF16)
        gs[r, :] = silu_gain(nn(xc, w[4]))
        return carry

    def scores(c, carry):
        r = rows(c)
        for h in range(heads):
            hs = slice(h * HD, (h + 1) * HD)
            wfh = cf[r, hs]
            wbh = cb[r, hs]
            mid_f = wfh[B // 2:B // 2 + 1, :]
            mid_b = wbh[B // 2 - 1:B // 2, :]
            q = qs[r, hs].astype(F32)
            qi_f = (q * jnp.exp(wfh - mid_f)).astype(BF16)
            qi_b = (q * jnp.exp(wbh - mid_b)).astype(BF16)
            ki_f = (kf_s[r, hs] * jnp.exp(mid_f - wfh)).astype(BF16)
            ki_b = (kb_s[r, hs] * jnp.exp(mid_b - wbh)).astype(BF16)
            sc = jnp.where(lower, nt(qi_f, ki_f), 0.0) + jnp.where(upper, nt(qi_b, ki_b), 0.0)
            inside[r, hs] = nn(sc.astype(BF16), vs[r, hs])
            qc[h, c, 0:B, 0:HD], qc[h, c, B:2 * B, 0:HD] = split2(q * jnp.exp(wfh))
            qc[h, c, 0:B, HD:2 * HD], qc[h, c, B:2 * B, HD:2 * HD] = split2(q * jnp.exp(wbh))
        return carry

    def inner(c, carry):
        queries(c, 0)
        return scores(c, 0)

    for load in loads[6:]:
        load.wait()
    early = n_chunk // 2
    lax.fori_loop(0, early, inner, 0)
    new = nx[...]
    nqf = nn(new, w[0]).astype(BF16).astype(F32)
    nv[...] = nn(new, w[1]).astype(BF16)
    nf = room[0:1, :] / (1.0 + jnp.exp(nn(new, w[2])))
    nb = room[1:2, :] / (1.0 + jnp.exp(nn(new, w[3])))
    ngate[...] = silu_gain(nn(new, w[4]))
    nq_hi[...], nq_lo[...] = split2(nqf * (1.0 - nf))
    nown[...] = nqf * (nf + nb)

    collect1()

    def decay(q, at):
        return jnp.exp(got_d[q, at:at + 1, :])

    run = jnp.zeros((8, HD), F32)
    before = []
    for q in range(n_sp):
        before.append(run)
        run = run * decay(q, 0) + got_f[q]
    fin[sp] = run.astype(BF16)
    run = jnp.zeros((8, HD), F32)
    for q in reversed(range(n_sp)):
        stage2[q, 0] = before[q]
        stage2[q, 1] = run
        run = run * decay(q, 1) + got_b[q].astype(F32)
    got2[sp] = stage2[sp]
    spread2()
    lax.fori_loop(early, n_chunk, inner, 0)
    spread3()

    push(whole, chip(tp), left, out_sem.at[0], near_in.at[0]).wait_send()
    push(whole, block(tp), left, out_sem.at[1], near_in.at[0]).wait_send()
    push(whole, chip(tp), left, out_sem.at[2], near_in.at[0]).wait_send()
    push(whole, block(tp), left, out_sem.at[3], near_in.at[0]).wait_send()
    pair_own(tp).wait_send()
    drain1()
    collect2()

    for h in range(heads):
        run = got2[h * per:(h + 1) * per, 0].reshape(HD, HD)
        for c in range(n_chunk):
            st[h, c, 0:HD, 0:HD], st[h, c, HD:2 * HD, 0:HD] = split2(run)
            run = run * e_f[c, h, 0:1, :] + a_f[c, h]
        run = got2[h * per:(h + 1) * per, 1].reshape(HD, HD)
        for c in reversed(range(n_chunk)):
            st[h, c, 0:HD, HD:2 * HD], st[h, c, HD:2 * HD, HD:2 * HD] = split2(run)
            run = run * e_b[c, h, 0:1, :] + a_b[c, h]

    def norm(mix, scale):
        return (mix * lax.rsqrt(jnp.mean(mix * mix, axis=-1, keepdims=True) + EPS) * scale).astype(BF16)

    def finish(c, carry):
        r = rows(c)
        for h in range(heads):
            hs = slice(h * HD, (h + 1) * HD)
            carried = nt(qc[h, c], st[h, c])
            carried = carried[0:B] + carried[B:2 * B]
            mix = inside[r, hs] + (carried[:, HD:2 * HD] + carried[:, 0:HD])
            mixed_out[r, hs] = norm(mix, gs[r, hs])
        return carry

    lax.fori_loop(0, n_chunk, finish, 0, unroll=8)

    collect3()
    for h in range(heads):
        hs = slice(h * HD, (h + 1) * HD)
        last = fin[h * per:(h + 1) * per].astype(F32).reshape(HD, HD)
        cached = last.astype(BF16)
        cache_out[h] = last.T.astype(BF16)
        own = jnp.sum(nown[:, hs], axis=-1, keepdims=True) * nv[:, hs].astype(F32)
        read_out[:, hs] = norm(nt(nq_lo[:, hs], cached) + nt(nq_hi[:, hs], cached) + own, ngate[:, hs])

    drain2()
    drain3()


def solution(mesh):
    n_sp, n_tp = mesh.shape["sp"], mesh.shape["tp"]

    def per_device(inputs, w_query, w_value, w_forget, w_gate, gate_room, extra_decay, out_gain, new_inputs):
        tokens, cols = inputs.shape
        depth = w_query.shape[0]
        heads = extra_decay.shape[0]
        fresh = new_inputs.shape[0]
        chunks = tokens // B
        hbm = pl.BlockSpec(memory_space=pltpu.HBM)
        vmem = pl.BlockSpec(memory_space=pltpu.VMEM)

        def kernel(*refs):
            body(n_sp, n_tp, chunks, heads, *refs)

        dma = pltpu.SemaphoreType.DMA
        done = pl.pallas_call(
            kernel,
            out_shape=(jax.ShapeDtypeStruct((tokens, cols), BF16),
                       jax.ShapeDtypeStruct((heads, HD, HD), BF16),
                       jax.ShapeDtypeStruct((fresh, cols), BF16)),
            in_specs=[hbm] * 9,
            out_specs=(vmem, vmem, vmem),
            scratch_shapes=[
                pltpu.VMEM((tokens, depth), BF16),
                pltpu.VMEM((5, depth, cols), BF16),
                pltpu.VMEM((fresh, depth), BF16),
                pltpu.VMEM((3, tokens, cols), F32),
                pltpu.VMEM((2, 2 * B, cols), BF16),
                pltpu.VMEM((2, cols), F32),
                pltpu.VMEM((heads, tokens), F32),
                pltpu.VMEM((1, cols), F32),
                pltpu.VMEM((tokens, cols), BF16),
                pltpu.VMEM((tokens, cols), BF16),
                pltpu.VMEM((tokens, cols), F32),
                pltpu.VMEM((tokens, cols), F32),
                pltpu.VMEM((tokens, cols), F32),
                pltpu.VMEM((tokens, cols), F32),
                pltpu.VMEM((tokens, cols), F32),
                pltpu.VMEM((chunks, heads, HD, HD), F32),
                pltpu.VMEM((chunks, heads, HD, HD), F32),
                pltpu.VMEM((chunks, heads, 8, HD), F32),
                pltpu.VMEM((chunks, heads, 8, HD), F32),
                pltpu.VMEM((heads, HD, HD), F32),
                pltpu.VMEM((heads, HD, HD), F32),
                pltpu.VMEM((2, heads, 8, HD), F32),
                pltpu.VMEM((tokens, cols), F32),
                pltpu.VMEM((heads, chunks, 2 * B, 2 * HD), BF16),
                pltpu.VMEM((heads, chunks, 2 * HD, 2 * HD), BF16),
                pltpu.VMEM((n_sp, 8, HD), F32),
                pltpu.VMEM((n_sp, 8, HD), BF16),
                pltpu.VMEM((n_sp, 2, HD), F32),
                pltpu.VMEM((n_sp, 8, HD), F32),
                pltpu.VMEM((n_sp, 8, HD), BF16),
                pltpu.VMEM((n_sp, 2, HD), F32),
                pltpu.VMEM((n_sp, 2, 8, HD), F32),
                pltpu.VMEM((n_sp, 2, 8, HD), F32),
                pltpu.VMEM((n_sp, 8, HD), BF16),
                pltpu.VMEM((fresh, cols), BF16),
                pltpu.VMEM((fresh, cols), BF16),
                pltpu.VMEM((fresh, cols), BF16),
                pltpu.VMEM((fresh, cols), F32),
                pltpu.VMEM((fresh, cols), F32),
                dma((10,)), dma((2,)),
                dma((4,)), dma((chunks,)), dma((chunks,)), dma((chunks,)), dma((chunks,)),
                pltpu.SemaphoreType.REGULAR((1 + n_sp // NX // 2,)),
                dma((3,)), dma((3,)), dma((1,)), dma((1,)), dma((1,)), dma((1,)),
            ],
            compiler_params=pltpu.CompilerParams(collective_id=0, has_side_effects=True,
                                                 vmem_limit_bytes=VM1 * 1024 * 1024),
        )(*(pltpu.with_memory_space_constraint(a, pltpu.HBM) for a in (
            inputs, w_query, w_value, w_forget, w_gate, new_inputs, gate_room, extra_decay, out_gain.reshape(1, cols))))

        def put(a, b, c, a_out, b_out, c_out, sems):
            copies = [pltpu.make_async_copy(s, d, sems.at[i])
                      for i, (s, d) in enumerate(((a, a_out), (b, b_out), (c, c_out)))]
            for copy in copies:
                copy.start()
            for copy in copies:
                copy.wait()

        return pl.pallas_call(
            put,
            out_shape=tuple(jax.ShapeDtypeStruct(d.shape, d.dtype) for d in done),
            in_specs=[vmem] * 3,
            out_specs=(hbm,) * 3,
            scratch_shapes=[dma((3,))],
            compiler_params=pltpu.CompilerParams(vmem_limit_bytes=4 * 1024 * 1024),
        )(*done)

    return jax.shard_map(
        per_device,
        mesh=mesh,
        in_specs=(P("sp", "tp"), P(None, "tp"), P(None, "tp"), P(None, None, "tp"), P(None, "tp"),
                  P(None, "tp"), P("tp", "sp"), P("tp"), P()),
        out_specs=(P("sp", "tp"), P("tp", None, None), P(None, "tp")),
        check_vma=False,
    )
```

```python
import jax
import jax.numpy as jnp
from jax import lax
from jax.experimental import pallas as pl
from jax.experimental.pallas import tpu as pltpu
from jax.sharding import PartitionSpec as P

MESH = pl.DeviceIdType.MESH
EPS = 1e-06
B = 128
HD = 128
VM1 = 48
LEAD = 3
TILE = 32
LAG = 2
NX = 4
F32 = jnp.float32
BF16 = jnp.bfloat16


def nn(a, b):
    return lax.dot_general(a, b, (((1,), (0,)), ((), ())), preferred_element_type=F32)


def nt(a, b):
    return lax.dot_general(a, b, (((1,), (1,)), ((), ())), preferred_element_type=F32)


def tn(a, b):
    return lax.dot_general(a, b, (((0,), (0,)), ((), ())), preferred_element_type=F32)


def split2(a):
    hi = a.astype(BF16)
    return hi, (a - hi.astype(F32)).astype(BF16)


def log_one_minus(k):
    s = jnp.full_like(k, 1.0 / 8.0)
    for n in (7, 6, 5, 4, 3, 2):
        s = s * k + (1.0 / n)
    return -(s * k + 1.0) * k


def body(n_sp, n_tp, n_chunk, heads, x_hbm, wq, wv, wf, wg, nx_hbm, room_hbm, extra_hbm, gain_hbm,
         mixed_out, cache_out, read_out,
         x, w, nx, part, lg, room, extra, gain, qs, vs, cf, cb, kf_s, kb_s, gs, a_f, a_b, e_f, e_b, s_f, s_b, acc,
         inside, qc, st, stage_f, stage_l, stage_b, stage_d, got_f, got_l, got_b, got_d, stage2, got2, fin, nq_hi, nq_lo, nv, nown, ngate,
         load_sem, own_sem, out_sem, near_in, far_in, mate_near, mate_far, word, p1_send, p1_recv, p2_send, p2_recv,
         p3_send, p3_recv, p4_send, p4_recv):
    cols = heads * HD
    sp = lax.axis_index("sp")
    tp = lax.axis_index("tp")
    right = lax.rem(tp + 2, n_tp)
    left = lax.rem(tp + n_tp - 2, n_tp)
    far = lax.rem(tp + 4, n_tp)
    flip = 1 - 2 * lax.rem(tp, 2)
    mate = tp + flip

    nz = n_sp // NX
    my_z, my_x = sp // NX, lax.rem(sp, NX)

    barrier = pltpu.get_barrier_semaphore()
    z_sides = [lax.rem(my_z + d, nz) * NX + my_x for d in (1, nz - 1)]
    x_sides = [my_z * NX + lax.rem(my_x + d, NX) for d in (1, NX - 1)]
    for peer in (mate, left, right):
        pl.semaphore_signal(barrier, inc=1, device_id={"tp": peer}, device_id_type=MESH)
    for peer in z_sides + x_sides:
        pl.semaphore_signal(barrier, inc=1, device_id={"sp": peer}, device_id_type=MESH)
    rounds = 1 + nz // 2

    def tell(n, sides):
        for peer in sides:
            pl.semaphore_signal(word.at[n], inc=1, device_id={"sp": peer}, device_id_type=MESH)

    def block(owner):
        return pl.ds(pl.multiple_of(owner * cols, cols), cols)

    def rows(j):
        return pl.ds(pl.multiple_of(j * B, B), B)

    loads = [pltpu.make_async_copy(src, dst, load_sem.at[i]) for i, (src, dst) in enumerate((
        (x_hbm, x.at[:, block(tp)]), (room_hbm, room), (extra_hbm, extra), (wf.at[0], w.at[2]), (wf.at[1], w.at[3]),
        (wv, w.at[1]), (gain_hbm, gain), (wq, w.at[0]), (wg, w.at[4]), (nx_hbm, nx)))]
    for load in loads:
        load.start()

    t_id = lax.broadcasted_iota(jnp.int32, (B, B), 0)
    s_id = lax.broadcasted_iota(jnp.int32, (B, B), 1)
    lower = t_id >= s_id
    upper = s_id >= t_id

    def silu_gain(g):
        return gain[...] * (g / (1.0 + jnp.exp(-g)))

    def half(j, k):
        return pl.ds(pl.multiple_of(j * B + k * (B // 2), B // 2), B // 2)

    def chip(owner):
        return pl.ds(pl.multiple_of((owner // 2) * (2 * cols), 2 * cols), 2 * cols)

    def push(r, c, to, out, inn):
        return pltpu.make_async_remote_copy(
            src_ref=x.at[r, c], dst_ref=x.at[r, c], send_sem=out, recv_sem=inn,
            device_id={"tp": to}, device_id_type=MESH)

    def send_own(j):
        push(rows(j), block(tp), right, out_sem.at[0], near_in.at[j]).start()
        push(rows(j), block(tp), left, out_sem.at[0], near_in.at[j]).start()

    def pass_near(j):
        push(half(j, 0), block(left), right, out_sem.at[1], far_in.at[j]).start()
        push(half(j, 1), block(right), left, out_sem.at[1], far_in.at[j]).start()
        push(rows(j), block(left), mate, out_sem.at[2], mate_near.at[j]).start()
        push(rows(j), block(right), mate, out_sem.at[2], mate_near.at[j]).start()

    def pass_far(j):
        push(rows(j), block(far), mate, out_sem.at[3], mate_far.at[j]).start()

    whole = pl.ds(0, n_chunk * B)

    def pair_own(owner):
        return push(whole, block(owner), mate, own_sem.at[0], own_sem.at[1])

    loads[0].wait()
    pl.semaphore_wait(barrier, 7)

    pair_own(tp).start()
    tell(0, x_sides)
    for j in range(LEAD):
        send_own(j)

    kinds = (2, 3, 1)

    def own_part(c, carry):
        r = pl.ds(pl.multiple_of(c * 2 * B, 2 * B), 2 * B)
        xc = x[r, chip(tp)]
        for n, i in enumerate(kinds):
            part[n, r, :] = nn(xc, w[i, chip(tp), :])
        return carry

    def near_part(c):
        r = pl.ds(pl.multiple_of(c * B, B), 2 * B)
        xl, xr = x[r, chip(left)], x[r, chip(right)]
        for n, i in enumerate(kinds):
            part[n, r, :] += nn(xl, w[i, chip(left), :]) + nn(xr, w[i, chip(right), :])

    loads[2].wait()
    for h in range(heads):
        ex = jnp.concatenate([extra[h:h + 1, c * B:(c + 1) * B] for c in range(n_chunk)], axis=0)
        e_hi, e_lo = split2(ex)
        for mask, sums in ((upper, cf), (lower, cb)):
            tri = jnp.where(mask, 1.0, 0.0).astype(BF16)
            down = (nn(e_hi, tri) + nn(e_lo, tri)).T
            for c in range(n_chunk):
                sums[c * B:(c + 1) * B, h * HD:(h + 1) * HD] = jnp.broadcast_to(down[:, c:c + 1], (B, HD))

    for load in (loads[1], *loads[3:6]):
        load.wait()
    pair_own(mate).wait_recv()
    lax.fori_loop(0, n_chunk // 2, own_part, 0)

    s_f[...] = jnp.zeros_like(s_f)
    s_b[...] = jnp.zeros_like(s_b)
    acc[...] = jnp.zeros_like(acc)

    def compute(c):
        r = rows(c)
        xc = x[r, chip(far)]
        far_w = chip(far)
        part[0, r, :] += nn(xc, w[2, far_w, :])
        part[1, r, :] += nn(xc, w[3, far_w, :])
        vc = (part[2, r, :] + nn(xc, w[1, far_w, :])).astype(BF16)
        vs[r, :] = vc
        for t in range(B // TILE):
            rt = pl.ds(pl.multiple_of(c * B + t * TILE, TILE), TILE)
            for d, keys in ((0, kf_s), (1, kb_s)):
                key = room[d:d + 1, :] / (1.0 + jnp.exp(part[d, rt, :]))
                keys[rt, :] = key
                lg[d, t * TILE:(t + 1) * TILE], lg[d, B + t * TILE:B + (t + 1) * TILE] = split2(log_one_minus(key))
        for d, (mask, sums) in enumerate(((lower, cf), (upper, cb))):
            tri = jnp.where(mask, 1.0, 0.0).astype(BF16)
            sums[r, :] += nn(jnp.concatenate([tri, tri], axis=1), lg[d])
        for h in range(heads):
            hs = slice(h * HD, (h + 1) * HD)
            wf_h, wb_h = cf[r, hs], cb[r, hs]
            end_f, end_b = wf_h[B - 1:B, :], wb_h[0:1, :]
            f_hi, f_lo = split2(kf_s[r, hs] * jnp.exp(end_f - wf_h))
            b_hi, b_lo = split2(kb_s[r, hs] * jnp.exp(end_b - wb_h))
            keys = jnp.concatenate([jnp.concatenate([f_hi, b_hi], axis=1), jnp.concatenate([f_lo, b_lo], axis=1)], axis=0)
            vh = vc[:, hs]
            add = tn(jnp.concatenate([vh, vh], axis=0), keys)
            add_f, add_b = add[:, 0:HD], add[:, HD:2 * HD]
            a_f[c, h] = add_f
            a_b[c, h] = add_b
            e_f[c, h] = jnp.broadcast_to(jnp.exp(end_f), (8, HD))
            e_b[c, h] = jnp.broadcast_to(jnp.exp(end_b), (8, HD))
            s_f[h] = s_f[h] * jnp.exp(end_f) + add_f
            s_b[h] = s_b[h] + jnp.exp(acc[1, h, 0:1, :]) * add_b
            acc[0, h] = acc[0, h] + end_f
            acc[1, h] = acc[1, h] + end_b

    def step(j, carry):
        @pl.when(j < n_chunk)
        def _():
            push(rows(j), chip(left), left, out_sem.at[0], near_in.at[j]).wait_recv()
            pass_near(j)

        @pl.when(j + LEAD < n_chunk)
        def _():
            send_own(j + LEAD)

        @pl.when((j >= 1) & (j <= rounds))
        def _():
            pl.semaphore_wait(word.at[j - 1], 2)

        @pl.when((j >= 1) & (j < rounds))
        def _():
            tell(j, z_sides)

        @pl.when((j >= 1) & (j <= n_chunk))
        def _():
            c = j - 1
            push(rows(c), chip(left), mate, out_sem.at[2], mate_near.at[c]).wait_recv()

        @pl.when((j >= 2) & (j <= n_chunk) & (lax.rem(j, 2) == 0))
        def _():
            near_part(j - 2)

        @pl.when((j >= LAG) & (j < n_chunk + LAG))
        def _():
            c = j - LAG
            push(rows(c), block(far), left, out_sem.at[1], far_in.at[c]).wait_recv()
            pass_far(c)

        @pl.when(j >= LAG + 1)
        def _():
            c = j - LAG - 1
            push(rows(c), block(far), mate, out_sem.at[3], mate_far.at[c]).wait_recv()
            compute(c)

        return carry

    lax.fori_loop(0, n_chunk + LAG + 1, step, 0)

    per = n_sp // heads
    r_id = lax.broadcasted_iota(jnp.int32, (2, HD), 0)
    for h in range(heads):
        at = slice(h * per, (h + 1) * per)
        stage_f[at], stage_l[at] = split2(s_f[h].reshape(per, 8, HD))
        stage_b[at] = s_b[h].reshape(per, 8, HD).astype(BF16)
        both = jnp.where(r_id == 0, acc[0, h, 0:2], acc[1, h, 0:2])
        stage_d[at] = jnp.broadcast_to(both[None], (per, 2, HD))
    got_f[sp] = stage_f[sp]
    got_b[sp] = stage_b[sp]
    got_l[sp] = stage_l[sp]
    got_d[sp] = stage_d[sp]

    def outward(n):
        return [n // 2 + ((i + 1) // 2) * (1 - 2 * (i % 2)) for i in range(n)]

    z_at = {d: lax.rem(my_z + d, nz) * NX for d in range(nz)}
    x_at = {d: lax.rem(my_x + d, NX) for d in range(NX)}
    others = [z_at[dz] + x_at[dx] for dz in outward(nz) for dx in outward(NX) if dz or dx]

    def exchange(stages, gots, sends, recvs, whole=False):
        def copies(to, frm):
            return [pltpu.make_async_remote_copy(
                src_ref=st.at[sp] if whole else st.at[to], dst_ref=gt.at[frm], send_sem=sends.at[n],
                recv_sem=recvs.at[n], device_id={"sp": to}, device_id_type=MESH)
                for n, (st, gt) in enumerate(zip(stages, gots))]

        def spread():
            for to in others:
                for copy in copies(to, sp):
                    copy.start()

        every = [pltpu.make_async_remote_copy(
            src_ref=st.at[pl.ds(0, n_sp - 1)], dst_ref=gt.at[pl.ds(0, n_sp - 1)], send_sem=sends.at[n],
            recv_sem=recvs.at[n], device_id={"sp": others[0]}, device_id_type=MESH)
            for n, (st, gt) in enumerate(zip(stages, gots))]

        def collect():
            for copy in every:
                copy.wait_recv()

        def drain():
            for copy in every:
                copy.wait_send()

        return spread, collect, drain

    spread1, collect1, drain1 = exchange((stage_d, stage_f, stage_b), (got_d, got_f, got_b), p1_send, p1_recv)
    spread2, collect2, drain2 = exchange((stage2,), (got2,), p2_send, p2_recv)
    spread4, collect4, drain4 = exchange((stage_l,), (got_l,), p4_send, p4_recv)
    spread3, collect3, drain3 = exchange((fin,), (fin,), p3_send, p3_recv, whole=True)

    spread1()
    spread4()

    def queries(c, carry):
        r = rows(c)
        xc = x[r, :]
        qs[r, :] = nn(xc, w[0]).astype(BF16)
        gs[r, :] = silu_gain(nn(xc, w[4]))
        return carry

    def scores(c, carry):
        r = rows(c)
        for h in range(heads):
            hs = slice(h * HD, (h + 1) * HD)
            wfh = cf[r, hs]
            wbh = cb[r, hs]
            mid_f = wfh[B // 2:B // 2 + 1, :]
            mid_b = wbh[B // 2 - 1:B // 2, :]
            q = qs[r, hs].astype(F32)
            qi_f = (q * jnp.exp(wfh - mid_f)).astype(BF16)
            qi_b = (q * jnp.exp(wbh - mid_b)).astype(BF16)
            ki_f = (kf_s[r, hs] * jnp.exp(mid_f - wfh)).astype(BF16)
            ki_b = (kb_s[r, hs] * jnp.exp(mid_b - wbh)).astype(BF16)
            sc = jnp.where(lower, nt(qi_f, ki_f), 0.0) + jnp.where(upper, nt(qi_b, ki_b), 0.0)
            inside[r, hs] = nn(sc.astype(BF16), vs[r, hs])
            qc[h, c, 0:B, 0:HD], qc[h, c, B:2 * B, 0:HD] = split2(q * jnp.exp(wfh))
            qc[h, c, 0:B, HD:2 * HD], qc[h, c, B:2 * B, HD:2 * HD] = split2(q * jnp.exp(wbh))
        return carry

    def inner(c, carry):
        queries(c, 0)
        return scores(c, 0)

    for load in loads[6:]:
        load.wait()
    early = n_chunk // 2
    lax.fori_loop(0, early, inner, 0)
    collect1()

    def decay(q, at):
        return jnp.exp(got_d[q, at:at + 1, :])

    run = jnp.zeros((8, HD), F32)
    before = []
    for q in range(n_sp):
        before.append(run)
        run = run * decay(q, 0) + got_f[q].astype(F32)
    run = jnp.zeros((8, HD), F32)
    for q in reversed(range(n_sp)):
        stage2[q, 0] = before[q]
        stage2[q, 1] = run
        run = run * decay(q, 1) + got_b[q].astype(F32)
    got2[sp] = stage2[sp]
    spread2()
    lax.fori_loop(early, early + n_chunk // 4, inner, 0)
    collect4()
    run = jnp.zeros((8, HD), F32)
    for q in range(n_sp):
        run = run * decay(q, 0) + (got_f[q].astype(F32) + got_l[q].astype(F32))
    fin[sp] = run.astype(BF16)
    spread3()
    lax.fori_loop(early + n_chunk // 4, n_chunk, inner, 0)
    new = nx[...]
    nqf = nn(new, w[0]).astype(BF16).astype(F32)
    nv[...] = nn(new, w[1]).astype(BF16)
    nf = room[0:1, :] / (1.0 + jnp.exp(nn(new, w[2])))
    nb = room[1:2, :] / (1.0 + jnp.exp(nn(new, w[3])))
    ngate[...] = silu_gain(nn(new, w[4]))
    nq_hi[...], nq_lo[...] = split2(nqf * (1.0 - nf))
    nown[...] = nqf * (nf + nb)


    push(whole, chip(tp), left, out_sem.at[0], near_in.at[0]).wait_send()
    push(whole, block(tp), left, out_sem.at[1], near_in.at[0]).wait_send()
    push(whole, chip(tp), left, out_sem.at[2], near_in.at[0]).wait_send()
    push(whole, block(tp), left, out_sem.at[3], near_in.at[0]).wait_send()
    pair_own(tp).wait_send()
    drain1()
    drain4()
    collect2()

    for h in range(heads):
        run = got2[h * per:(h + 1) * per, 0].reshape(HD, HD)
        for c in range(n_chunk):
            st[h, c, 0:HD, 0:HD], st[h, c, HD:2 * HD, 0:HD] = split2(run)
            run = run * e_f[c, h, 0:1, :] + a_f[c, h]
        run = got2[h * per:(h + 1) * per, 1].reshape(HD, HD)
        for c in reversed(range(n_chunk)):
            st[h, c, 0:HD, HD:2 * HD], st[h, c, HD:2 * HD, HD:2 * HD] = split2(run)
            run = run * e_b[c, h, 0:1, :] + a_b[c, h]

    def norm(mix, scale):
        return (mix * lax.rsqrt(jnp.mean(mix * mix, axis=-1, keepdims=True) + EPS) * scale).astype(BF16)

    def finish(c, carry):
        r = rows(c)
        for h in range(heads):
            hs = slice(h * HD, (h + 1) * HD)
            carried = nt(qc[h, c], st[h, c])
            carried = carried[0:B] + carried[B:2 * B]
            mix = inside[r, hs] + (carried[:, HD:2 * HD] + carried[:, 0:HD])
            mixed_out[r, hs] = norm(mix, gs[r, hs])
        return carry

    lax.fori_loop(0, n_chunk, finish, 0, unroll=8)

    collect3()
    for h in range(heads):
        hs = slice(h * HD, (h + 1) * HD)
        last = fin[h * per:(h + 1) * per].astype(F32).reshape(HD, HD)
        cached = last.astype(BF16)
        cache_out[h] = last.T.astype(BF16)
        own = jnp.sum(nown[:, hs], axis=-1, keepdims=True) * nv[:, hs].astype(F32)
        read_out[:, hs] = norm(nt(nq_lo[:, hs], cached) + nt(nq_hi[:, hs], cached) + own, ngate[:, hs])

    drain2()
    drain3()


def solution(mesh):
    n_sp, n_tp = mesh.shape["sp"], mesh.shape["tp"]

    def per_device(inputs, w_query, w_value, w_forget, w_gate, gate_room, extra_decay, out_gain, new_inputs):
        tokens, cols = inputs.shape
        depth = w_query.shape[0]
        heads = extra_decay.shape[0]
        fresh = new_inputs.shape[0]
        chunks = tokens // B
        hbm = pl.BlockSpec(memory_space=pltpu.HBM)
        vmem = pl.BlockSpec(memory_space=pltpu.VMEM)

        def kernel(*refs):
            body(n_sp, n_tp, chunks, heads, *refs)

        dma = pltpu.SemaphoreType.DMA
        done = pl.pallas_call(
            kernel,
            out_shape=(jax.ShapeDtypeStruct((tokens, cols), BF16),
                       jax.ShapeDtypeStruct((heads, HD, HD), BF16),
                       jax.ShapeDtypeStruct((fresh, cols), BF16)),
            in_specs=[hbm] * 9,
            out_specs=(vmem, vmem, vmem),
            scratch_shapes=[
                pltpu.VMEM((tokens, depth), BF16),
                pltpu.VMEM((5, depth, cols), BF16),
                pltpu.VMEM((fresh, depth), BF16),
                pltpu.VMEM((3, tokens, cols), F32),
                pltpu.VMEM((2, 2 * B, cols), BF16),
                pltpu.VMEM((2, cols), F32),
                pltpu.VMEM((heads, tokens), F32),
                pltpu.VMEM((1, cols), F32),
                pltpu.VMEM((tokens, cols), BF16),
                pltpu.VMEM((tokens, cols), BF16),
                pltpu.VMEM((tokens, cols), F32),
                pltpu.VMEM((tokens, cols), F32),
                pltpu.VMEM((tokens, cols), F32),
                pltpu.VMEM((tokens, cols), F32),
                pltpu.VMEM((tokens, cols), F32),
                pltpu.VMEM((chunks, heads, HD, HD), F32),
                pltpu.VMEM((chunks, heads, HD, HD), F32),
                pltpu.VMEM((chunks, heads, 8, HD), F32),
                pltpu.VMEM((chunks, heads, 8, HD), F32),
                pltpu.VMEM((heads, HD, HD), F32),
                pltpu.VMEM((heads, HD, HD), F32),
                pltpu.VMEM((2, heads, 8, HD), F32),
                pltpu.VMEM((tokens, cols), F32),
                pltpu.VMEM((heads, chunks, 2 * B, 2 * HD), BF16),
                pltpu.VMEM((heads, chunks, 2 * HD, 2 * HD), BF16),
                pltpu.VMEM((n_sp, 8, HD), BF16),
                pltpu.VMEM((n_sp, 8, HD), BF16),
                pltpu.VMEM((n_sp, 8, HD), BF16),
                pltpu.VMEM((n_sp, 2, HD), F32),
                pltpu.VMEM((n_sp, 8, HD), BF16),
                pltpu.VMEM((n_sp, 8, HD), BF16),
                pltpu.VMEM((n_sp, 8, HD), BF16),
                pltpu.VMEM((n_sp, 2, HD), F32),
                pltpu.VMEM((n_sp, 2, 8, HD), F32),
                pltpu.VMEM((n_sp, 2, 8, HD), F32),
                pltpu.VMEM((n_sp, 8, HD), BF16),
                pltpu.VMEM((fresh, cols), BF16),
                pltpu.VMEM((fresh, cols), BF16),
                pltpu.VMEM((fresh, cols), BF16),
                pltpu.VMEM((fresh, cols), F32),
                pltpu.VMEM((fresh, cols), F32),
                dma((10,)), dma((2,)),
                dma((4,)), dma((chunks,)), dma((chunks,)), dma((chunks,)), dma((chunks,)),
                pltpu.SemaphoreType.REGULAR((1 + n_sp // NX // 2,)),
                dma((3,)), dma((3,)), dma((1,)), dma((1,)), dma((1,)), dma((1,)), dma((1,)), dma((1,)),
            ],
            compiler_params=pltpu.CompilerParams(collective_id=0, has_side_effects=True,
                                                 vmem_limit_bytes=VM1 * 1024 * 1024),
        )(*(pltpu.with_memory_space_constraint(a, pltpu.HBM) for a in (
            inputs, w_query, w_value, w_forget, w_gate, new_inputs, gate_room, extra_decay, out_gain.reshape(1, cols))))

        def put(a, b, c, a_out, b_out, c_out, sems):
            copies = [pltpu.make_async_copy(s, d, sems.at[i])
                      for i, (s, d) in enumerate(((a, a_out), (b, b_out), (c, c_out)))]
            for copy in copies:
                copy.start()
            for copy in copies:
                copy.wait()

        return pl.pallas_call(
            put,
            out_shape=tuple(jax.ShapeDtypeStruct(d.shape, d.dtype) for d in done),
            in_specs=[vmem] * 3,
            out_specs=(hbm,) * 3,
            scratch_shapes=[dma((3,))],
            compiler_params=pltpu.CompilerParams(vmem_limit_bytes=4 * 1024 * 1024),
        )(*done)

    return jax.shard_map(
        per_device,
        mesh=mesh,
        in_specs=(P("sp", "tp"), P(None, "tp"), P(None, "tp"), P(None, None, "tp"), P(None, "tp"),
                  P(None, "tp"), P("tp", "sp"), P("tp"), P()),
        out_specs=(P("sp", "tp"), P("tp", None, None), P(None, "tp")),
        check_vma=False,
    )
```

```python
import jax
import jax.numpy as jnp
from jax import lax
from jax.experimental import pallas as pl
from jax.experimental.pallas import tpu as pltpu
from jax.sharding import PartitionSpec as P

MESH = pl.DeviceIdType.MESH
EPS = 1e-06
B = 128
HD = 128
VM1 = 48
LEAD = 3
TILE = 32
LAG = 2
NX = 4
F32 = jnp.float32
BF16 = jnp.bfloat16


def nn(a, b):
    return lax.dot_general(a, b, (((1,), (0,)), ((), ())), preferred_element_type=F32)


def nt(a, b):
    return lax.dot_general(a, b, (((1,), (1,)), ((), ())), preferred_element_type=F32)


def tn(a, b):
    return lax.dot_general(a, b, (((0,), (0,)), ((), ())), preferred_element_type=F32)


def split2(a):
    hi = a.astype(BF16)
    return hi, (a - hi.astype(F32)).astype(BF16)


def log_one_minus(k):
    s = jnp.full_like(k, 1.0 / 8.0)
    for n in (7, 6, 5, 4, 3, 2):
        s = s * k + (1.0 / n)
    return -(s * k + 1.0) * k


def body(n_sp, n_tp, n_chunk, heads, x_hbm, wq, wv, wf, wg, nx_hbm, room_hbm, extra_hbm, gain_hbm,
         mixed_out, cache_out, read_out,
         x, w, nx, part, lg, room, extra, gain, qs, vs, cf, cb, kf_s, kb_s, gs, a_f, a_b, e_f, e_b, s_f, s_b, acc,
         inside, qc, st, stage_f, stage_l, stage_b, stage_d, got_f, got_l, got_b, got_d, out_f, out_b, in_f, in_b, fin, nq_hi, nq_lo, nv, nown, ngate,
         load_sem, own_sem, out_sem, near_in, far_in, mate_near, mate_far, word, p1_send, p1_recv, p2_send, p2_recv,
         p3_send, p3_recv, p4_send, p4_recv,
         p5_send, p5_recv, p6_send, p6_recv):
    cols = heads * HD
    sp = lax.axis_index("sp")
    tp = lax.axis_index("tp")
    right = lax.rem(tp + 2, n_tp)
    left = lax.rem(tp + n_tp - 2, n_tp)
    far = lax.rem(tp + 4, n_tp)
    flip = 1 - 2 * lax.rem(tp, 2)
    mate = tp + flip

    nz = n_sp // NX
    my_z, my_x = sp // NX, lax.rem(sp, NX)

    def block(owner):
        return pl.ds(pl.multiple_of(owner * cols, cols), cols)

    own_load = pltpu.make_async_copy(x_hbm, x.at[:, block(tp)], load_sem.at[0])
    own_load.start()
    barrier = pltpu.get_barrier_semaphore()
    z_sides = [lax.rem(my_z + d, nz) * NX + my_x for d in (1, nz - 1)]
    x_sides = [my_z * NX + lax.rem(my_x + d, NX) for d in (1, NX - 1)]
    for peer in (mate, left, right):
        pl.semaphore_signal(barrier, inc=1, device_id={"tp": peer}, device_id_type=MESH)
    for peer in z_sides + x_sides:
        pl.semaphore_signal(barrier, inc=1, device_id={"sp": peer}, device_id_type=MESH)
    rounds = 1 + nz // 2

    def tell(n, sides):
        for peer in sides:
            pl.semaphore_signal(word.at[n], inc=1, device_id={"sp": peer}, device_id_type=MESH)

    def rows(j):
        return pl.ds(pl.multiple_of(j * B, B), B)

    loads = [pltpu.make_async_copy(src, dst, load_sem.at[i + 1]) for i, (src, dst) in enumerate((
        (room_hbm, room), (extra_hbm, extra), (wf.at[0], w.at[2]), (wf.at[1], w.at[3]),
        (wv, w.at[1]), (gain_hbm, gain), (wq, w.at[0]), (wg, w.at[4]), (nx_hbm, nx)))]
    for load in loads:
        load.start()

    t_id = lax.broadcasted_iota(jnp.int32, (B, B), 0)
    s_id = lax.broadcasted_iota(jnp.int32, (B, B), 1)
    lower = t_id >= s_id
    upper = s_id >= t_id

    def silu_gain(g):
        return gain[...] * (g / (1.0 + jnp.exp(-g)))

    def half(j, k):
        return pl.ds(pl.multiple_of(j * B + k * (B // 2), B // 2), B // 2)

    def chip(owner):
        return pl.ds(pl.multiple_of((owner // 2) * (2 * cols), 2 * cols), 2 * cols)

    def push(r, c, to, out, inn):
        return pltpu.make_async_remote_copy(
            src_ref=x.at[r, c], dst_ref=x.at[r, c], send_sem=out, recv_sem=inn,
            device_id={"tp": to}, device_id_type=MESH)

    def send_own(j):
        push(rows(j), block(tp), right, out_sem.at[0], near_in.at[j]).start()
        push(rows(j), block(tp), left, out_sem.at[0], near_in.at[j]).start()

    def pass_near(j):
        push(half(j, 0), block(left), right, out_sem.at[1], far_in.at[j]).start()
        push(half(j, 1), block(right), left, out_sem.at[1], far_in.at[j]).start()
        push(rows(j), block(left), mate, out_sem.at[2], mate_near.at[j]).start()
        push(rows(j), block(right), mate, out_sem.at[2], mate_near.at[j]).start()

    def pass_far(j):
        push(rows(j), block(far), mate, out_sem.at[3], mate_far.at[j]).start()

    whole = pl.ds(0, n_chunk * B)

    def pair_own(owner):
        return push(whole, block(owner), mate, own_sem.at[0], own_sem.at[1])

    own_load.wait()
    pl.semaphore_wait(barrier, 7)

    pair_own(tp).start()
    tell(0, x_sides)
    for j in range(LEAD):
        send_own(j)

    kinds = (2, 3, 1)

    def own_part(c, carry):
        r = pl.ds(pl.multiple_of(c * 2 * B, 2 * B), 2 * B)
        xc = x[r, chip(tp)]
        for n, i in enumerate(kinds):
            part[n, r, :] = nn(xc, w[i, chip(tp), :])
        return carry

    def near_part(c):
        r = pl.ds(pl.multiple_of(c * B, B), 2 * B)
        xl, xr = x[r, chip(left)], x[r, chip(right)]
        for n, i in enumerate(kinds):
            part[n, r, :] += nn(xl, w[i, chip(left), :]) + nn(xr, w[i, chip(right), :])

    loads[1].wait()
    for h in range(heads):
        ex = jnp.concatenate([extra[h:h + 1, c * B:(c + 1) * B] for c in range(n_chunk)], axis=0)
        e_hi, e_lo = split2(ex)
        for mask, sums in ((upper, cf), (lower, cb)):
            tri = jnp.where(mask, 1.0, 0.0).astype(BF16)
            down = (nn(e_hi, tri) + nn(e_lo, tri)).T
            for c in range(n_chunk):
                sums[c * B:(c + 1) * B, h * HD:(h + 1) * HD] = jnp.broadcast_to(down[:, c:c + 1], (B, HD))

    for load in (loads[0], *loads[2:5]):
        load.wait()
    pair_own(mate).wait_recv()
    lax.fori_loop(0, n_chunk // 2, own_part, 0)

    s_f[...] = jnp.zeros_like(s_f)
    s_b[...] = jnp.zeros_like(s_b)
    acc[...] = jnp.zeros_like(acc)

    def compute(c):
        r = rows(c)
        xc = x[r, chip(far)]
        far_w = chip(far)
        part[0, r, :] += nn(xc, w[2, far_w, :])
        part[1, r, :] += nn(xc, w[3, far_w, :])
        vc = (part[2, r, :] + nn(xc, w[1, far_w, :])).astype(BF16)
        vs[r, :] = vc
        for t in range(B // TILE):
            rt = pl.ds(pl.multiple_of(c * B + t * TILE, TILE), TILE)
            for d, keys in ((0, kf_s), (1, kb_s)):
                key = room[d:d + 1, :] / (1.0 + jnp.exp(part[d, rt, :]))
                keys[rt, :] = key
                lg[d, t * TILE:(t + 1) * TILE], lg[d, B + t * TILE:B + (t + 1) * TILE] = split2(log_one_minus(key))
        for d, (mask, sums) in enumerate(((lower, cf), (upper, cb))):
            tri = jnp.where(mask, 1.0, 0.0).astype(BF16)
            sums[r, :] += nn(jnp.concatenate([tri, tri], axis=1), lg[d])
        for h in range(heads):
            hs = slice(h * HD, (h + 1) * HD)
            wf_h, wb_h = cf[r, hs], cb[r, hs]
            end_f, end_b = wf_h[B - 1:B, :], wb_h[0:1, :]
            f_hi, f_lo = split2(kf_s[r, hs] * jnp.exp(end_f - wf_h))
            b_hi, b_lo = split2(kb_s[r, hs] * jnp.exp(end_b - wb_h))
            keys = jnp.concatenate([jnp.concatenate([f_hi, b_hi], axis=1), jnp.concatenate([f_lo, b_lo], axis=1)], axis=0)
            vh = vc[:, hs]
            add = tn(jnp.concatenate([vh, vh], axis=0), keys)
            add_f, add_b = add[:, 0:HD], add[:, HD:2 * HD]
            a_f[c, h] = add_f
            a_b[c, h] = add_b
            e_f[c, h] = jnp.broadcast_to(jnp.exp(end_f), (8, HD))
            e_b[c, h] = jnp.broadcast_to(jnp.exp(end_b), (8, HD))
            s_f[h] = s_f[h] * jnp.exp(end_f) + add_f
            s_b[h] = s_b[h] + jnp.exp(acc[1, h, 0:1, :]) * add_b
            acc[0, h] = acc[0, h] + end_f
            acc[1, h] = acc[1, h] + end_b

    def step(j, carry):
        @pl.when(j < n_chunk)
        def _():
            push(rows(j), chip(left), left, out_sem.at[0], near_in.at[j]).wait_recv()
            pass_near(j)

        @pl.when(j + LEAD < n_chunk)
        def _():
            send_own(j + LEAD)

        @pl.when((j >= 1) & (j <= rounds))
        def _():
            pl.semaphore_wait(word.at[j - 1], 2)

        @pl.when((j >= 1) & (j < rounds))
        def _():
            tell(j, z_sides)

        @pl.when((j >= 1) & (j <= n_chunk))
        def _():
            c = j - 1
            push(rows(c), chip(left), mate, out_sem.at[2], mate_near.at[c]).wait_recv()

        @pl.when((j >= 2) & (j <= n_chunk) & (lax.rem(j, 2) == 0))
        def _():
            near_part(j - 2)

        @pl.when((j >= LAG) & (j < n_chunk + LAG))
        def _():
            c = j - LAG
            push(rows(c), block(far), left, out_sem.at[1], far_in.at[c]).wait_recv()
            pass_far(c)

        @pl.when(j >= LAG + 1)
        def _():
            c = j - LAG - 1
            push(rows(c), block(far), mate, out_sem.at[3], mate_far.at[c]).wait_recv()
            compute(c)

        return carry

    lax.fori_loop(0, n_chunk + LAG + 1, step, 0)

    per = n_sp // heads
    r_id = lax.broadcasted_iota(jnp.int32, (2, HD), 0)
    for h in range(heads):
        at = slice(h * per, (h + 1) * per)
        stage_f[at], stage_l[at] = split2(s_f[h].reshape(per, 8, HD))
        stage_b[at] = s_b[h].reshape(per, 8, HD).astype(BF16)
        both = jnp.where(r_id == 0, acc[0, h, 0:2], acc[1, h, 0:2])
        stage_d[at] = jnp.broadcast_to(both[None], (per, 2, HD))
    got_f[sp] = stage_f[sp]
    got_b[sp] = stage_b[sp]
    got_l[sp] = stage_l[sp]
    got_d[sp] = stage_d[sp]

    def outward(n):
        return [n // 2 + ((i + 1) // 2) * (1 - 2 * (i % 2)) for i in range(n)]

    z_at = {d: lax.rem(my_z + d, nz) * NX for d in range(nz)}
    x_at = {d: lax.rem(my_x + d, NX) for d in range(NX)}
    others = [z_at[dz] + x_at[dx] for dz in outward(nz) for dx in outward(NX) if dz or dx]

    def exchange(stages, gots, sends, recvs, whole=False):
        def copies(to, frm):
            return [pltpu.make_async_remote_copy(
                src_ref=st.at[sp] if whole else st.at[to], dst_ref=gt.at[frm], send_sem=sends.at[n],
                recv_sem=recvs.at[n], device_id={"sp": to}, device_id_type=MESH)
                for n, (st, gt) in enumerate(zip(stages, gots))]

        def spread():
            for to in others:
                for copy in copies(to, sp):
                    copy.start()

        every = [pltpu.make_async_remote_copy(
            src_ref=st.at[pl.ds(0, n_sp - 1)], dst_ref=gt.at[pl.ds(0, n_sp - 1)], send_sem=sends.at[n],
            recv_sem=recvs.at[n], device_id={"sp": others[0]}, device_id_type=MESH)
            for n, (st, gt) in enumerate(zip(stages, gots))]

        def collect():
            for copy in every:
                copy.wait_recv()

        def drain():
            for copy in every:
                copy.wait_send()

        return spread, collect, drain

    spread1, collect1, drain1 = exchange((stage_d, stage_f), (got_d, got_f), p1_send, p1_recv)
    spread5, collect5, drain5 = exchange((stage_b,), (got_b,), p5_send, p5_recv)
    spread2, collect2, drain2 = exchange((out_f,), (in_f,), p2_send, p2_recv)
    spread6, collect6, drain6 = exchange((out_b,), (in_b,), p6_send, p6_recv)
    spread4, collect4, drain4 = exchange((stage_l,), (got_l,), p4_send, p4_recv)
    spread3, collect3, drain3 = exchange((fin,), (fin,), p3_send, p3_recv, whole=True)

    spread1()
    spread5()
    spread4()

    def queries(c, carry):
        r = rows(c)
        xc = x[r, :]
        qs[r, :] = nn(xc, w[0]).astype(BF16)
        gs[r, :] = silu_gain(nn(xc, w[4]))
        return carry

    def scores(c, carry):
        r = rows(c)
        for h in range(heads):
            hs = slice(h * HD, (h + 1) * HD)
            wfh = cf[r, hs]
            wbh = cb[r, hs]
            mid_f = wfh[B // 2:B // 2 + 1, :]
            mid_b = wbh[B // 2 - 1:B // 2, :]
            q = qs[r, hs].astype(F32)
            qi_f = (q * jnp.exp(wfh - mid_f)).astype(BF16)
            qi_b = (q * jnp.exp(wbh - mid_b)).astype(BF16)
            ki_f = (kf_s[r, hs] * jnp.exp(mid_f - wfh)).astype(BF16)
            ki_b = (kb_s[r, hs] * jnp.exp(mid_b - wbh)).astype(BF16)
            sc = jnp.where(lower, nt(qi_f, ki_f), 0.0) + jnp.where(upper, nt(qi_b, ki_b), 0.0)
            inside[r, hs] = nn(sc.astype(BF16), vs[r, hs])
            qc[h, c, 0:B, 0:HD], qc[h, c, B:2 * B, 0:HD] = split2(q * jnp.exp(wfh))
            qc[h, c, 0:B, HD:2 * HD], qc[h, c, B:2 * B, HD:2 * HD] = split2(q * jnp.exp(wbh))
        return carry

    def inner(c, carry):
        queries(c, 0)
        return scores(c, 0)

    for load in loads[5:]:
        load.wait()
    early = n_chunk // 2
    lax.fori_loop(0, early, inner, 0)
    collect1()

    def decay(q, at):
        return jnp.exp(got_d[q, at:at + 1, :])

    run = jnp.zeros((8, HD), F32)
    for q in range(n_sp):
        out_f[q] = run
        run = run * decay(q, 0) + got_f[q].astype(F32)
    in_f[sp] = out_f[sp]
    spread2()
    collect5()
    run = jnp.zeros((8, HD), F32)
    for q in reversed(range(n_sp)):
        out_b[q] = run
        run = run * decay(q, 1) + got_b[q].astype(F32)
    in_b[sp] = out_b[sp]
    spread6()
    lax.fori_loop(early, early + n_chunk // 4, inner, 0)
    collect4()
    run = jnp.zeros((8, HD), F32)
    for q in range(n_sp):
        run = run * decay(q, 0) + (got_f[q].astype(F32) + got_l[q].astype(F32))
    fin[sp] = run.astype(BF16)
    spread3()
    lax.fori_loop(early + n_chunk // 4, n_chunk, inner, 0)
    new = nx[...]
    nqf = nn(new, w[0]).astype(BF16).astype(F32)
    nv[...] = nn(new, w[1]).astype(BF16)
    nf = room[0:1, :] / (1.0 + jnp.exp(nn(new, w[2])))
    nb = room[1:2, :] / (1.0 + jnp.exp(nn(new, w[3])))
    ngate[...] = silu_gain(nn(new, w[4]))
    nq_hi[...], nq_lo[...] = split2(nqf * (1.0 - nf))
    nown[...] = nqf * (nf + nb)


    push(whole, chip(tp), left, out_sem.at[0], near_in.at[0]).wait_send()
    push(whole, block(tp), left, out_sem.at[1], near_in.at[0]).wait_send()
    push(whole, chip(tp), left, out_sem.at[2], near_in.at[0]).wait_send()
    push(whole, block(tp), left, out_sem.at[3], near_in.at[0]).wait_send()
    pair_own(tp).wait_send()
    drain1()
    drain5()
    drain4()
    collect2()
    collect6()

    for h in range(heads):
        run = in_f[h * per:(h + 1) * per].reshape(HD, HD)
        for c in range(n_chunk):
            st[h, c, 0:HD, 0:HD], st[h, c, HD:2 * HD, 0:HD] = split2(run)
            run = run * e_f[c, h, 0:1, :] + a_f[c, h]
        run = in_b[h * per:(h + 1) * per].reshape(HD, HD)
        for c in reversed(range(n_chunk)):
            st[h, c, 0:HD, HD:2 * HD], st[h, c, HD:2 * HD, HD:2 * HD] = split2(run)
            run = run * e_b[c, h, 0:1, :] + a_b[c, h]

    def norm(mix, scale):
        return (mix * lax.rsqrt(jnp.mean(mix * mix, axis=-1, keepdims=True) + EPS) * scale).astype(BF16)

    def finish(c, carry):
        r = rows(c)
        for h in range(heads):
            hs = slice(h * HD, (h + 1) * HD)
            carried = nt(qc[h, c], st[h, c])
            carried = carried[0:B] + carried[B:2 * B]
            mix = inside[r, hs] + (carried[:, HD:2 * HD] + carried[:, 0:HD])
            mixed_out[r, hs] = norm(mix, gs[r, hs])
        return carry

    lax.fori_loop(0, n_chunk, finish, 0, unroll=8)

    collect3()
    for h in range(heads):
        hs = slice(h * HD, (h + 1) * HD)
        last = fin[h * per:(h + 1) * per].astype(F32).reshape(HD, HD)
        cached = last.astype(BF16)
        cache_out[h] = last.T.astype(BF16)
        own = jnp.sum(nown[:, hs], axis=-1, keepdims=True) * nv[:, hs].astype(F32)
        read_out[:, hs] = norm(nt(nq_lo[:, hs], cached) + nt(nq_hi[:, hs], cached) + own, ngate[:, hs])

    drain2()
    drain6()
    drain3()


def solution(mesh):
    n_sp, n_tp = mesh.shape["sp"], mesh.shape["tp"]

    def per_device(inputs, w_query, w_value, w_forget, w_gate, gate_room, extra_decay, out_gain, new_inputs):
        tokens, cols = inputs.shape
        depth = w_query.shape[0]
        heads = extra_decay.shape[0]
        fresh = new_inputs.shape[0]
        chunks = tokens // B
        hbm = pl.BlockSpec(memory_space=pltpu.HBM)
        vmem = pl.BlockSpec(memory_space=pltpu.VMEM)

        def kernel(*refs):
            body(n_sp, n_tp, chunks, heads, *refs)

        dma = pltpu.SemaphoreType.DMA
        done = pl.pallas_call(
            kernel,
            out_shape=(jax.ShapeDtypeStruct((tokens, cols), BF16),
                       jax.ShapeDtypeStruct((heads, HD, HD), BF16),
                       jax.ShapeDtypeStruct((fresh, cols), BF16)),
            in_specs=[hbm] * 9,
            out_specs=(vmem, vmem, vmem),
            scratch_shapes=[
                pltpu.VMEM((tokens, depth), BF16),
                pltpu.VMEM((5, depth, cols), BF16),
                pltpu.VMEM((fresh, depth), BF16),
                pltpu.VMEM((3, tokens, cols), F32),
                pltpu.VMEM((2, 2 * B, cols), BF16),
                pltpu.VMEM((2, cols), F32),
                pltpu.VMEM((heads, tokens), F32),
                pltpu.VMEM((1, cols), F32),
                pltpu.VMEM((tokens, cols), BF16),
                pltpu.VMEM((tokens, cols), BF16),
                pltpu.VMEM((tokens, cols), F32),
                pltpu.VMEM((tokens, cols), F32),
                pltpu.VMEM((tokens, cols), F32),
                pltpu.VMEM((tokens, cols), F32),
                pltpu.VMEM((tokens, cols), F32),
                pltpu.VMEM((chunks, heads, HD, HD), F32),
                pltpu.VMEM((chunks, heads, HD, HD), F32),
                pltpu.VMEM((chunks, heads, 8, HD), F32),
                pltpu.VMEM((chunks, heads, 8, HD), F32),
                pltpu.VMEM((heads, HD, HD), F32),
                pltpu.VMEM((heads, HD, HD), F32),
                pltpu.VMEM((2, heads, 8, HD), F32),
                pltpu.VMEM((tokens, cols), F32),
                pltpu.VMEM((heads, chunks, 2 * B, 2 * HD), BF16),
                pltpu.VMEM((heads, chunks, 2 * HD, 2 * HD), BF16),
                pltpu.VMEM((n_sp, 8, HD), BF16),
                pltpu.VMEM((n_sp, 8, HD), BF16),
                pltpu.VMEM((n_sp, 8, HD), BF16),
                pltpu.VMEM((n_sp, 2, HD), F32),
                pltpu.VMEM((n_sp, 8, HD), BF16),
                pltpu.VMEM((n_sp, 8, HD), BF16),
                pltpu.VMEM((n_sp, 8, HD), BF16),
                pltpu.VMEM((n_sp, 2, HD), F32),
                pltpu.VMEM((n_sp, 8, HD), F32),
                pltpu.VMEM((n_sp, 8, HD), F32),
                pltpu.VMEM((n_sp, 8, HD), F32),
                pltpu.VMEM((n_sp, 8, HD), F32),
                pltpu.VMEM((n_sp, 8, HD), BF16),
                pltpu.VMEM((fresh, cols), BF16),
                pltpu.VMEM((fresh, cols), BF16),
                pltpu.VMEM((fresh, cols), BF16),
                pltpu.VMEM((fresh, cols), F32),
                pltpu.VMEM((fresh, cols), F32),
                dma((10,)), dma((2,)),
                dma((4,)), dma((chunks,)), dma((chunks,)), dma((chunks,)), dma((chunks,)),
                pltpu.SemaphoreType.REGULAR((1 + n_sp // NX // 2,)),
                dma((2,)), dma((2,)), dma((1,)), dma((1,)), dma((1,)), dma((1,)), dma((1,)), dma((1,)),
                dma((1,)), dma((1,)), dma((1,)), dma((1,)),
            ],
            compiler_params=pltpu.CompilerParams(collective_id=0, has_side_effects=True,
                                                 vmem_limit_bytes=VM1 * 1024 * 1024),
        )(*(pltpu.with_memory_space_constraint(a, pltpu.HBM) for a in (
            inputs, w_query, w_value, w_forget, w_gate, new_inputs, gate_room, extra_decay, out_gain.reshape(1, cols))))

        def put(a, b, c, a_out, b_out, c_out, sems):
            copies = [pltpu.make_async_copy(s, d, sems.at[i])
                      for i, (s, d) in enumerate(((a, a_out), (b, b_out), (c, c_out)))]
            for copy in copies:
                copy.start()
            for copy in copies:
                copy.wait()

        return pl.pallas_call(
            put,
            out_shape=tuple(jax.ShapeDtypeStruct(d.shape, d.dtype) for d in done),
            in_specs=[vmem] * 3,
            out_specs=(hbm,) * 3,
            scratch_shapes=[dma((3,))],
            compiler_params=pltpu.CompilerParams(vmem_limit_bytes=4 * 1024 * 1024),
        )(*done)

    return jax.shard_map(
        per_device,
        mesh=mesh,
        in_specs=(P("sp", "tp"), P(None, "tp"), P(None, "tp"), P(None, None, "tp"), P(None, "tp"),
                  P(None, "tp"), P("tp", "sp"), P("tp"), P()),
        out_specs=(P("sp", "tp"), P("tp", None, None), P(None, "tp")),
        check_vma=False,
    )
```

```python
import jax
import jax.numpy as jnp
from jax import lax
from jax.experimental import pallas as pl
from jax.experimental.pallas import tpu as pltpu
from jax.sharding import PartitionSpec as P

MESH = pl.DeviceIdType.MESH
EPS = 1e-06
B = 128
HD = 128
VM1 = 48
LEAD = 3
TILE = 32
LAG = 2
NX = 4
F32 = jnp.float32
BF16 = jnp.bfloat16


def nn(a, b):
    return lax.dot_general(a, b, (((1,), (0,)), ((), ())), preferred_element_type=F32)


def nt(a, b):
    return lax.dot_general(a, b, (((1,), (1,)), ((), ())), preferred_element_type=F32)


def tn(a, b):
    return lax.dot_general(a, b, (((0,), (0,)), ((), ())), preferred_element_type=F32)


def split2(a):
    hi = a.astype(BF16)
    return hi, (a - hi.astype(F32)).astype(BF16)


def log_one_minus(k):
    s = jnp.full_like(k, 1.0 / 8.0)
    for n in (7, 6, 5, 4, 3, 2):
        s = s * k + (1.0 / n)
    return -(s * k + 1.0) * k


def body(n_sp, n_tp, n_chunk, heads, x_hbm, wq, wv, wf, wg, nx_hbm, room_hbm, extra_hbm, gain_hbm,
         mixed_out, cache_out, read_out,
         x, w, nx, part, lg, room, extra, gain, qs, vs, cf, cb, kf_s, kb_s, gs, a_f, a_b, e_f, e_b, s_f, s_b, acc,
         inside, qc, st, stage_f, stage_l, stage_b, stage_d, got_f, got_l, got_b, got_d, out_f, out_b, in_f, in_b, fin, nq_hi, nq_lo, nv, nown, ngate,
         load_sem, own_sem, out_sem, near_in, far_in, mate_near, mate_far, word, p1_send, p1_recv, p2_send, p2_recv,
         p3_send, p3_recv, p4_send, p4_recv,
         p5_send, p5_recv, p6_send, p6_recv):
    cols = heads * HD
    sp = lax.axis_index("sp")
    tp = lax.axis_index("tp")
    right = lax.rem(tp + 2, n_tp)
    left = lax.rem(tp + n_tp - 2, n_tp)
    far = lax.rem(tp + 4, n_tp)
    flip = 1 - 2 * lax.rem(tp, 2)
    mate = tp + flip

    nz = n_sp // NX
    my_z, my_x = sp // NX, lax.rem(sp, NX)

    def block(owner):
        return pl.ds(pl.multiple_of(owner * cols, cols), cols)

    own_load = pltpu.make_async_copy(x_hbm, x.at[:, block(tp)], load_sem.at[0])
    own_load.start()
    barrier = pltpu.get_barrier_semaphore()
    z_sides = [lax.rem(my_z + d, nz) * NX + my_x for d in (1, nz - 1)]
    x_sides = [my_z * NX + lax.rem(my_x + d, NX) for d in (1, NX - 1)]
    for peer in (mate, left, right):
        pl.semaphore_signal(barrier, inc=1, device_id={"tp": peer}, device_id_type=MESH)
    for peer in z_sides + x_sides:
        pl.semaphore_signal(barrier, inc=1, device_id={"sp": peer}, device_id_type=MESH)
    rounds = 1 + nz // 2

    def tell(n, sides):
        for peer in sides:
            pl.semaphore_signal(word.at[n], inc=1, device_id={"sp": peer}, device_id_type=MESH)

    def rows(j):
        return pl.ds(pl.multiple_of(j * B, B), B)

    loads = [pltpu.make_async_copy(src, dst, load_sem.at[i + 1]) for i, (src, dst) in enumerate((
        (room_hbm, room), (extra_hbm, extra), (wf.at[0], w.at[2]), (wf.at[1], w.at[3]),
        (wv, w.at[1]), (gain_hbm, gain), (wq, w.at[0]), (wg, w.at[4]), (nx_hbm, nx)))]
    for load in loads:
        load.start()

    t_id = lax.broadcasted_iota(jnp.int32, (B, B), 0)
    s_id = lax.broadcasted_iota(jnp.int32, (B, B), 1)
    lower = t_id >= s_id
    upper = s_id >= t_id

    def silu_gain(g):
        return gain[...] * (g / (1.0 + jnp.exp(-g)))

    def half(j, k):
        return pl.ds(pl.multiple_of(j * B + k * (B // 2), B // 2), B // 2)

    def chip(owner):
        return pl.ds(pl.multiple_of((owner // 2) * (2 * cols), 2 * cols), 2 * cols)

    def push(r, c, to, out, inn):
        return pltpu.make_async_remote_copy(
            src_ref=x.at[r, c], dst_ref=x.at[r, c], send_sem=out, recv_sem=inn,
            device_id={"tp": to}, device_id_type=MESH)

    def send_own(j):
        push(rows(j), block(tp), right, out_sem.at[0], near_in.at[j]).start()
        push(rows(j), block(tp), left, out_sem.at[0], near_in.at[j]).start()

    def pass_near(j):
        push(half(j, 0), block(left), right, out_sem.at[1], far_in.at[j]).start()
        push(half(j, 1), block(right), left, out_sem.at[1], far_in.at[j]).start()
        push(rows(j), block(left), mate, out_sem.at[2], mate_near.at[j]).start()
        push(rows(j), block(right), mate, out_sem.at[2], mate_near.at[j]).start()

    def pass_far(j):
        push(rows(j), block(far), mate, out_sem.at[3], mate_far.at[j]).start()

    whole = pl.ds(0, n_chunk * B)

    def pair_own(owner):
        return push(whole, block(owner), mate, own_sem.at[0], own_sem.at[1])

    own_load.wait()
    pl.semaphore_wait(barrier, 7)

    pair_own(tp).start()
    tell(0, x_sides)
    for j in range(LEAD):
        send_own(j)

    kinds = (2, 3, 1)

    def own_part(c, carry):
        r = pl.ds(pl.multiple_of(c * 2 * B, 2 * B), 2 * B)
        xc = x[r, chip(tp)]
        for n, i in enumerate(kinds):
            part[n, r, :] = nn(xc, w[i, chip(tp), :])
        return carry

    def near_part(c):
        r = pl.ds(pl.multiple_of(c * B, B), 2 * B)
        xl, xr = x[r, chip(left)], x[r, chip(right)]
        for n, i in enumerate(kinds):
            part[n, r, :] += nn(xl, w[i, chip(left), :]) + nn(xr, w[i, chip(right), :])

    loads[1].wait()
    for h in range(heads):
        ex = jnp.concatenate([extra[h:h + 1, c * B:(c + 1) * B] for c in range(n_chunk)], axis=0)
        e_hi, e_lo = split2(ex)
        for mask, sums in ((upper, cf), (lower, cb)):
            tri = jnp.where(mask, 1.0, 0.0).astype(BF16)
            down = (nn(e_hi, tri) + nn(e_lo, tri)).T
            for c in range(n_chunk):
                sums[c * B:(c + 1) * B, h * HD:(h + 1) * HD] = jnp.broadcast_to(down[:, c:c + 1], (B, HD))

    for load in (loads[0], *loads[2:5]):
        load.wait()
    pair_own(mate).wait_recv()
    lax.fori_loop(0, n_chunk // 2, own_part, 0)

    s_f[...] = jnp.zeros_like(s_f)
    s_b[...] = jnp.zeros_like(s_b)
    acc[...] = jnp.zeros_like(acc)

    def compute(c):
        r = rows(c)
        xc = x[r, chip(far)]
        far_w = chip(far)
        part[0, r, :] += nn(xc, w[2, far_w, :])
        part[1, r, :] += nn(xc, w[3, far_w, :])
        vc = (part[2, r, :] + nn(xc, w[1, far_w, :])).astype(BF16)
        vs[r, :] = vc
        for t in range(B // TILE):
            rt = pl.ds(pl.multiple_of(c * B + t * TILE, TILE), TILE)
            for d, keys in ((0, kf_s), (1, kb_s)):
                key = room[d:d + 1, :] / (1.0 + jnp.exp(part[d, rt, :]))
                keys[rt, :] = key
                lg[d, t * TILE:(t + 1) * TILE], lg[d, B + t * TILE:B + (t + 1) * TILE] = split2(log_one_minus(key))
        for d, (mask, sums) in enumerate(((lower, cf), (upper, cb))):
            tri = jnp.where(mask, 1.0, 0.0).astype(BF16)
            sums[r, :] += nn(jnp.concatenate([tri, tri], axis=1), lg[d])
        for h in range(heads):
            hs = slice(h * HD, (h + 1) * HD)
            wf_h, wb_h = cf[r, hs], cb[r, hs]
            end_f, end_b = wf_h[B - 1:B, :], wb_h[0:1, :]
            f_hi, f_lo = split2(kf_s[r, hs] * jnp.exp(end_f - wf_h))
            b_hi, b_lo = split2(kb_s[r, hs] * jnp.exp(end_b - wb_h))
            keys = jnp.concatenate([jnp.concatenate([f_hi, b_hi], axis=1), jnp.concatenate([f_lo, b_lo], axis=1)], axis=0)
            vh = vc[:, hs]
            add = tn(jnp.concatenate([vh, vh], axis=0), keys)
            add_f, add_b = add[:, 0:HD], add[:, HD:2 * HD]
            a_f[c, h] = add_f
            a_b[c, h] = add_b
            e_f[c, h] = jnp.broadcast_to(jnp.exp(end_f), (8, HD))
            e_b[c, h] = jnp.broadcast_to(jnp.exp(end_b), (8, HD))
            s_f[h] = s_f[h] * jnp.exp(end_f) + add_f
            s_b[h] = s_b[h] + jnp.exp(acc[1, h, 0:1, :]) * add_b
            acc[0, h] = acc[0, h] + end_f
            acc[1, h] = acc[1, h] + end_b

    def step(j, carry):
        @pl.when(j < n_chunk)
        def _():
            push(rows(j), chip(left), left, out_sem.at[0], near_in.at[j]).wait_recv()
            pass_near(j)

        @pl.when(j + LEAD < n_chunk)
        def _():
            send_own(j + LEAD)

        @pl.when((j >= 1) & (j <= rounds))
        def _():
            pl.semaphore_wait(word.at[j - 1], 2)

        @pl.when((j >= 1) & (j < rounds))
        def _():
            tell(j, z_sides)

        @pl.when((j >= 1) & (j <= n_chunk))
        def _():
            c = j - 1
            push(rows(c), chip(left), mate, out_sem.at[2], mate_near.at[c]).wait_recv()

        @pl.when((j >= 2) & (j <= n_chunk) & (lax.rem(j, 2) == 0))
        def _():
            near_part(j - 2)

        @pl.when((j >= LAG) & (j < n_chunk + LAG))
        def _():
            c = j - LAG
            push(rows(c), block(far), left, out_sem.at[1], far_in.at[c]).wait_recv()
            pass_far(c)

        @pl.when(j >= LAG + 1)
        def _():
            c = j - LAG - 1
            push(rows(c), block(far), mate, out_sem.at[3], mate_far.at[c]).wait_recv()
            compute(c)

        return carry

    lax.fori_loop(0, n_chunk + LAG + 1, step, 0)

    per = n_sp // heads
    r_id = lax.broadcasted_iota(jnp.int32, (2, HD), 0)
    for h in range(heads):
        at = slice(h * per, (h + 1) * per)
        stage_f[at], stage_l[at] = split2(s_f[h].reshape(per, 8, HD))
        stage_b[at] = s_b[h].reshape(per, 8, HD).astype(BF16)
        both = jnp.where(r_id == 0, acc[0, h, 0:2], acc[1, h, 0:2])
        stage_d[at] = jnp.broadcast_to(both[None], (per, 2, HD))
    got_f[sp] = stage_f[sp]
    got_b[sp] = stage_b[sp]
    got_l[sp] = stage_l[sp]
    got_d[sp] = stage_d[sp]

    def outward(n):
        return [n // 2 + ((i + 1) // 2) * (1 - 2 * (i % 2)) for i in range(n)]

    z_at = {d: lax.rem(my_z + d, nz) * NX for d in range(nz)}
    x_at = {d: lax.rem(my_x + d, NX) for d in range(NX)}
    others = [z_at[dz] + x_at[dx] for dz in outward(nz) for dx in outward(NX) if dz or dx]

    def exchange(stages, gots, sends, recvs, whole=False):
        def copies(to, frm):
            return [pltpu.make_async_remote_copy(
                src_ref=st.at[sp] if whole else st.at[to], dst_ref=gt.at[frm], send_sem=sends.at[n],
                recv_sem=recvs.at[n], device_id={"sp": to}, device_id_type=MESH)
                for n, (st, gt) in enumerate(zip(stages, gots))]

        def spread():
            for to in others:
                for copy in copies(to, sp):
                    copy.start()

        every = [pltpu.make_async_remote_copy(
            src_ref=st.at[pl.ds(0, n_sp - 1)], dst_ref=gt.at[pl.ds(0, n_sp - 1)], send_sem=sends.at[n],
            recv_sem=recvs.at[n], device_id={"sp": others[0]}, device_id_type=MESH)
            for n, (st, gt) in enumerate(zip(stages, gots))]

        def collect():
            for copy in every:
                copy.wait_recv()

        def drain():
            for copy in every:
                copy.wait_send()

        return spread, collect, drain

    spread1, collect1, drain1 = exchange((stage_d, stage_f), (got_d, got_f), p1_send, p1_recv)
    spread5, collect5, drain5 = exchange((stage_b,), (got_b,), p5_send, p5_recv)
    spread2, collect2, drain2 = exchange((out_f,), (in_f,), p2_send, p2_recv)
    spread6, collect6, drain6 = exchange((out_b,), (in_b,), p6_send, p6_recv)
    spread4, collect4, drain4 = exchange((stage_l,), (got_l,), p4_send, p4_recv)
    spread3, collect3, drain3 = exchange((fin,), (fin,), p3_send, p3_recv, whole=True)

    spread1()
    spread5()
    spread4()

    def queries(c, carry):
        r = rows(c)
        xc = x[r, :]
        qs[r, :] = nn(xc, w[0]).astype(BF16)
        gs[r, :] = silu_gain(nn(xc, w[4]))
        return carry

    def scores(c, carry):
        r = rows(c)
        for h in range(heads):
            hs = slice(h * HD, (h + 1) * HD)
            wfh = cf[r, hs]
            wbh = cb[r, hs]
            mid_f = wfh[B // 2:B // 2 + 1, :]
            mid_b = wbh[B // 2 - 1:B // 2, :]
            q = qs[r, hs].astype(F32)
            qi_f = (q * jnp.exp(wfh - mid_f)).astype(BF16)
            qi_b = (q * jnp.exp(wbh - mid_b)).astype(BF16)
            ki_f = (kf_s[r, hs] * jnp.exp(mid_f - wfh)).astype(BF16)
            ki_b = (kb_s[r, hs] * jnp.exp(mid_b - wbh)).astype(BF16)
            sc = jnp.where(lower, nt(qi_f, ki_f), 0.0) + jnp.where(upper, nt(qi_b, ki_b), 0.0)
            inside[r, hs] = nn(sc.astype(BF16), vs[r, hs])
            qc[h, c, 0:B, 0:HD], qc[h, c, B:2 * B, 0:HD] = split2(q * jnp.exp(wfh))
            qc[h, c, 0:B, HD:2 * HD], qc[h, c, B:2 * B, HD:2 * HD] = split2(q * jnp.exp(wbh))
        return carry

    def inner(c, carry):
        queries(c, 0)
        return scores(c, 0)

    for load in loads[5:]:
        load.wait()
    early = n_chunk // 2
    lax.fori_loop(0, early, inner, 0)
    collect1()

    def decay(q, at):
        return jnp.exp(got_d[q, at:at + 1, :])

    run = jnp.zeros((8, HD), F32)
    for q in range(n_sp):
        out_f[q] = run
        run = run * decay(q, 0) + got_f[q].astype(F32)
    in_f[sp] = out_f[sp]
    spread2()
    collect5()
    run = jnp.zeros((8, HD), F32)
    for q in reversed(range(n_sp)):
        out_b[q] = run
        run = run * decay(q, 1) + got_b[q].astype(F32)
    in_b[sp] = out_b[sp]
    spread6()
    inner(early, 0)
    collect4()
    run = jnp.zeros((8, HD), F32)
    for q in range(n_sp):
        run = run * decay(q, 0) + (got_f[q].astype(F32) + got_l[q].astype(F32))
    fin[sp] = run.astype(BF16)
    spread3()
    lax.fori_loop(early + 1, n_chunk, inner, 0)
    new = nx[...]
    nqf = nn(new, w[0]).astype(BF16).astype(F32)
    nv[...] = nn(new, w[1]).astype(BF16)
    nf = room[0:1, :] / (1.0 + jnp.exp(nn(new, w[2])))
    nb = room[1:2, :] / (1.0 + jnp.exp(nn(new, w[3])))
    ngate[...] = silu_gain(nn(new, w[4]))
    nq_hi[...], nq_lo[...] = split2(nqf * (1.0 - nf))
    nown[...] = nqf * (nf + nb)


    push(whole, chip(tp), left, out_sem.at[0], near_in.at[0]).wait_send()
    push(whole, block(tp), left, out_sem.at[1], near_in.at[0]).wait_send()
    push(whole, chip(tp), left, out_sem.at[2], near_in.at[0]).wait_send()
    push(whole, block(tp), left, out_sem.at[3], near_in.at[0]).wait_send()
    pair_own(tp).wait_send()
    drain1()
    drain5()
    drain4()
    collect2()

    for h in range(heads):
        run = in_f[h * per:(h + 1) * per].reshape(HD, HD)
        for c in range(n_chunk):
            st[h, c, 0:HD, 0:HD], st[h, c, HD:2 * HD, 0:HD] = split2(run)
            run = run * e_f[c, h, 0:1, :] + a_f[c, h]
    collect6()
    for h in range(heads):
        run = in_b[h * per:(h + 1) * per].reshape(HD, HD)
        for c in reversed(range(n_chunk)):
            st[h, c, 0:HD, HD:2 * HD], st[h, c, HD:2 * HD, HD:2 * HD] = split2(run)
            run = run * e_b[c, h, 0:1, :] + a_b[c, h]

    def norm(mix, scale):
        return (mix * lax.rsqrt(jnp.mean(mix * mix, axis=-1, keepdims=True) + EPS) * scale).astype(BF16)

    def finish(c, carry):
        r = rows(c)
        for h in range(heads):
            hs = slice(h * HD, (h + 1) * HD)
            carried = nt(qc[h, c], st[h, c])
            carried = carried[0:B] + carried[B:2 * B]
            mix = inside[r, hs] + (carried[:, HD:2 * HD] + carried[:, 0:HD])
            mixed_out[r, hs] = norm(mix, gs[r, hs])
        return carry

    lax.fori_loop(0, n_chunk, finish, 0, unroll=8)

    collect3()
    for h in range(heads):
        hs = slice(h * HD, (h + 1) * HD)
        last = fin[h * per:(h + 1) * per].astype(F32).reshape(HD, HD)
        cached = last.astype(BF16)
        cache_out[h] = last.T.astype(BF16)
        own = jnp.sum(nown[:, hs], axis=-1, keepdims=True) * nv[:, hs].astype(F32)
        read_out[:, hs] = norm(nt(nq_lo[:, hs], cached) + nt(nq_hi[:, hs], cached) + own, ngate[:, hs])

    drain2()
    drain6()
    drain3()


def solution(mesh):
    n_sp, n_tp = mesh.shape["sp"], mesh.shape["tp"]

    def per_device(inputs, w_query, w_value, w_forget, w_gate, gate_room, extra_decay, out_gain, new_inputs):
        tokens, cols = inputs.shape
        depth = w_query.shape[0]
        heads = extra_decay.shape[0]
        fresh = new_inputs.shape[0]
        chunks = tokens // B
        hbm = pl.BlockSpec(memory_space=pltpu.HBM)
        vmem = pl.BlockSpec(memory_space=pltpu.VMEM)

        def kernel(*refs):
            body(n_sp, n_tp, chunks, heads, *refs)

        dma = pltpu.SemaphoreType.DMA
        done = pl.pallas_call(
            kernel,
            out_shape=(jax.ShapeDtypeStruct((tokens, cols), BF16),
                       jax.ShapeDtypeStruct((heads, HD, HD), BF16),
                       jax.ShapeDtypeStruct((fresh, cols), BF16)),
            in_specs=[hbm] * 9,
            out_specs=(vmem, vmem, vmem),
            scratch_shapes=[
                pltpu.VMEM((tokens, depth), BF16),
                pltpu.VMEM((5, depth, cols), BF16),
                pltpu.VMEM((fresh, depth), BF16),
                pltpu.VMEM((3, tokens, cols), F32),
                pltpu.VMEM((2, 2 * B, cols), BF16),
                pltpu.VMEM((2, cols), F32),
                pltpu.VMEM((heads, tokens), F32),
                pltpu.VMEM((1, cols), F32),
                pltpu.VMEM((tokens, cols), BF16),
                pltpu.VMEM((tokens, cols), BF16),
                pltpu.VMEM((tokens, cols), F32),
                pltpu.VMEM((tokens, cols), F32),
                pltpu.VMEM((tokens, cols), F32),
                pltpu.VMEM((tokens, cols), F32),
                pltpu.VMEM((tokens, cols), F32),
                pltpu.VMEM((chunks, heads, HD, HD), F32),
                pltpu.VMEM((chunks, heads, HD, HD), F32),
                pltpu.VMEM((chunks, heads, 8, HD), F32),
                pltpu.VMEM((chunks, heads, 8, HD), F32),
                pltpu.VMEM((heads, HD, HD), F32),
                pltpu.VMEM((heads, HD, HD), F32),
                pltpu.VMEM((2, heads, 8, HD), F32),
                pltpu.VMEM((tokens, cols), F32),
                pltpu.VMEM((heads, chunks, 2 * B, 2 * HD), BF16),
                pltpu.VMEM((heads, chunks, 2 * HD, 2 * HD), BF16),
                pltpu.VMEM((n_sp, 8, HD), BF16),
                pltpu.VMEM((n_sp, 8, HD), BF16),
                pltpu.VMEM((n_sp, 8, HD), BF16),
                pltpu.VMEM((n_sp, 2, HD), F32),
                pltpu.VMEM((n_sp, 8, HD), BF16),
                pltpu.VMEM((n_sp, 8, HD), BF16),
                pltpu.VMEM((n_sp, 8, HD), BF16),
                pltpu.VMEM((n_sp, 2, HD), F32),
                pltpu.VMEM((n_sp, 8, HD), F32),
                pltpu.VMEM((n_sp, 8, HD), F32),
                pltpu.VMEM((n_sp, 8, HD), F32),
                pltpu.VMEM((n_sp, 8, HD), F32),
                pltpu.VMEM((n_sp, 8, HD), BF16),
                pltpu.VMEM((fresh, cols), BF16),
                pltpu.VMEM((fresh, cols), BF16),
                pltpu.VMEM((fresh, cols), BF16),
                pltpu.VMEM((fresh, cols), F32),
                pltpu.VMEM((fresh, cols), F32),
                dma((10,)), dma((2,)),
                dma((4,)), dma((chunks,)), dma((chunks,)), dma((chunks,)), dma((chunks,)),
                pltpu.SemaphoreType.REGULAR((1 + n_sp // NX // 2,)),
                dma((2,)), dma((2,)), dma((1,)), dma((1,)), dma((1,)), dma((1,)), dma((1,)), dma((1,)),
                dma((1,)), dma((1,)), dma((1,)), dma((1,)),
            ],
            compiler_params=pltpu.CompilerParams(collective_id=0, has_side_effects=True,
                                                 vmem_limit_bytes=VM1 * 1024 * 1024),
        )(*(pltpu.with_memory_space_constraint(a, pltpu.HBM) for a in (
            inputs, w_query, w_value, w_forget, w_gate, new_inputs, gate_room, extra_decay, out_gain.reshape(1, cols))))

        def put(a, b, c, a_out, b_out, c_out, sems):
            copies = [pltpu.make_async_copy(s, d, sems.at[i])
                      for i, (s, d) in enumerate(((a, a_out), (b, b_out), (c, c_out)))]
            for copy in copies:
                copy.start()
            for copy in copies:
                copy.wait()

        return pl.pallas_call(
            put,
            out_shape=tuple(jax.ShapeDtypeStruct(d.shape, d.dtype) for d in done),
            in_specs=[vmem] * 3,
            out_specs=(hbm,) * 3,
            scratch_shapes=[dma((3,))],
            compiler_params=pltpu.CompilerParams(vmem_limit_bytes=4 * 1024 * 1024),
        )(*done)

    return jax.shard_map(
        per_device,
        mesh=mesh,
        in_specs=(P("sp", "tp"), P(None, "tp"), P(None, "tp"), P(None, None, "tp"), P(None, "tp"),
                  P(None, "tp"), P("tp", "sp"), P("tp"), P()),
        out_specs=(P("sp", "tp"), P("tp", None, None), P(None, "tp")),
        check_vma=False,
    )
```
